256 devices in a mesh: sp: 32 (over z, y), fs: 4 (over x), tp: 2 (over core).
Axes of the slice: x: 4, y: 4, z: 8, core: 2. Of those that a mesh axis runs over, the one named last changes fastest.
Arguments:
- tokens: bfloat16 [4, 24576, 2048], P('fs', 'sp', 'tp'), may hold values from -6 to 6
- in_gain: float32 [2048], replicated, may hold values from 0.1 to 1.9
- ret_query: bfloat16 [2048, 768], P(None, 'tp'), may hold values from -0.125 to 0.125
- ret_key: bfloat16 [2048, 768], P(None, 'tp'), may hold values from -0.125 to 0.125
- ret_value: bfloat16 [2048, 768], P(None, 'tp'), may hold values from -0.125 to 0.125
- att_query: bfloat16 [2048, 768], P(None, 'tp'), may hold values from -8 to 8
- att_key: bfloat16 [2048, 256], P(None, 'tp'), may hold values from -8 to 8
- att_value: bfloat16 [2048, 256], P(None, 'tp'), may hold values from -0.125 to 0.125
- log_decay: float32 [4, 12, 24576], P('fs', 'tp', 'sp'), may hold values from -1.5 to 0
- ret_gain: float32 [768], P('tp'), may hold values from 0.1 to 1.9
- sink_logit: float32 [12], P('tp'), may hold values from 1 to 5
- retentive_exit_matrix: bfloat16 [768, 2048], P('tp'), may hold values from -0.15625 to 0.15625
- out_att: bfloat16 [768, 2048], P('tp'), may hold values from -0.875 to 0.875
Outputs:
- mixed: bfloat16 [4, 24576, 2048], P('fs', ('sp', 'tp'))
The draws below stay inside these ranges and needn't reach their ends.
All inputs are finite; a program needn't handle non-finite values.
Results may differ from the reference program's by a relative error of at most 0.0085.
Values may be sent and summed in bfloat16 or wider, within the bound.
No kernel may reach another device: no remote copies, remote signals or barrier semaphores. Data moves between devices by JAX's collectives and lax.ppermute only.
A program may use at most 128 MiB of HBM per device.

```python
import jax
import jax.numpy as jnp
from jax import lax

D = 2048
HEAD_DIM = 64
RET_HEADS = 12
ATT_HEADS = 12
KV_HEADS = 4
WINDOW = 128
TOK_DEV = 768
SEQ = 24576
BATCH = 4


def paired_heads(key):
    keys = jax.random.split(jax.random.fold_in(key, 5), 2)
    key_weight = jax.random.normal(keys[0], (D, KV_HEADS * HEAD_DIM), jnp.float32) * D ** (-0.5)
    query_weight = jax.random.normal(keys[1], (D, ATT_HEADS * HEAD_DIM), jnp.float32) * D ** (-0.5)
    return (jnp.clip(query_weight, -8.0, 8.0), jnp.clip(key_weight, -8.0, 8.0))


def draw_att_query(key, part):
    return paired_heads(key)[0].astype(jnp.bfloat16)


def draw_att_key(key, part):
    return paired_heads(key)[1].astype(jnp.bfloat16)


def draw_log_decay(key, part):
    keys = jax.random.split(jax.random.fold_in(key, 11), 5)
    keep_share = 0.5
    slow = jax.random.uniform(keys[0], (BATCH, RET_HEADS, 1), jnp.float32) < keep_share
    span = 30.0 * jnp.exp(jax.random.uniform(keys[1], (BATCH, RET_HEADS, 1), jnp.float32) * jnp.log(100.0 / 30.0))
    starting_shift_amount = jnp.where(slow, -jnp.log(10.0) / (4.0 * SEQ), -1.0 / span)
    blocks = SEQ // TOK_DEV
    fading_multiplier = jnp.exp(jax.random.uniform(keys[2], (BATCH, 1, blocks), jnp.float32) * jnp.log(3.0))
    fading_multiplier = jnp.repeat(fading_multiplier, TOK_DEV, axis=2)
    location_numbers = jax.random.randint(keys[3], (BATCH, 3, 1), 0, SEQ)
    objective_numbers = jnp.log(1.0 - jax.random.uniform(keys[4], (BATCH, 3, 1), jnp.float32, 0.2, 0.5))
    element_locations = jnp.arange(SEQ)[None, None, :]
    cluster_sets = jnp.sum(jnp.where(element_locations == location_numbers, objective_numbers, 0.0), axis=1, keepdims=True)
    return (starting_shift_amount * fading_multiplier + cluster_sets).astype(jnp.float32)


def block_scale(key, dims, cuts, least, largest):
    def one(axis_at, shards_of):
        heights = jax.random.uniform(jax.random.fold_in(jax.random.fold_in(key, 6), axis_at), (shards_of,), jnp.float32, least / len(cuts), largest / len(cuts))
        return jnp.repeat(jnp.exp(heights), dims[axis_at] // shards_of).reshape((-1,) + (1,) * (len(dims) - axis_at - 1))

    level = one(*cuts[0])
    for cut in cuts[1:]:
        level = level * one(*cut)
    return level


def gaussian(key, dims, width, reach, pieces=(), held_as=jnp.bfloat16):
    array = jax.random.normal(key, dims, jnp.float32) * width
    if len(pieces) > 0:
        array = block_scale(key, dims, pieces, -0.22, 0.18) * array
    return jnp.clip(array, min=-reach, max=reach).astype(held_as)


def setup_inputs(seed: int = 0) -> dict:
    arg_keys = jax.random.split(jax.random.key(seed), 14)
    tokens = gaussian(arg_keys[0], (BATCH, SEQ, D), 1.0, 6.0, ((0, 4), (1, 32), (2, 2)))
    in_gain = jnp.clip(1.0 + 0.18 * jax.random.normal(arg_keys[1], (D,), jnp.float32), 0.1, 1.9)
    ret_query = gaussian(arg_keys[2], (D, RET_HEADS * HEAD_DIM), D ** -0.5, 0.125, ((1, 2),))
    ret_key = gaussian(arg_keys[3], (D, RET_HEADS * HEAD_DIM), D ** -0.5, 0.125, ((1, 2),))
    ret_value = gaussian(arg_keys[4], (D, RET_HEADS * HEAD_DIM), D ** -0.5, 0.125, ((1, 2),))
    att_query = draw_att_query(jax.random.fold_in(arg_keys[13], 71), 0)
    att_key = draw_att_key(jax.random.fold_in(arg_keys[13], 71), 0)
    att_value = gaussian(arg_keys[7], (D, KV_HEADS * HEAD_DIM), D ** -0.5, 0.125, ((1, 2),))
    log_decay = draw_log_decay(jax.random.fold_in(arg_keys[13], 71), 0)
    ret_gain = jnp.clip(1.0 + 0.18 * jax.random.normal(arg_keys[9], (RET_HEADS * HEAD_DIM,), jnp.float32), 0.1, 1.9)
    sink_logit = jnp.clip(1.0 + 4.0 * jax.random.uniform(arg_keys[10], (ATT_HEADS,), jnp.float32) ** block_scale(arg_keys[10], (ATT_HEADS,), ((0, 2),), -0.2, 0.2), 1.0, 5.0)
    retentive_exit_matrix = gaussian(arg_keys[11], (RET_HEADS * HEAD_DIM, D), (2 * RET_HEADS * HEAD_DIM) ** -0.5, 0.15625, ((0, 2),))
    out_att = gaussian(arg_keys[12], (ATT_HEADS * HEAD_DIM, D), (ATT_HEADS * HEAD_DIM // 16) ** -0.5, 0.875, ((0, 2),))
    return dict(tokens=tokens, in_gain=in_gain, ret_query=ret_query, ret_key=ret_key, ret_value=ret_value, att_query=att_query, att_key=att_key, att_value=att_value, log_decay=log_decay, ret_gain=ret_gain, sink_logit=sink_logit, retentive_exit_matrix=retentive_exit_matrix, out_att=out_att)


EPS = 1e-06

def retention_sequence(query_rows, key_rows, value_rows, log_rates, gain):
    heads = log_rates.shape[0]
    blocks = query_rows.shape[0] // TOK_DEV
    fading_multiplier = HEAD_DIM ** (-0.5)
    shaped_q = query_rows.reshape(blocks, TOK_DEV, heads, HEAD_DIM)
    shaped_k = key_rows.reshape(blocks, TOK_DEV, heads, HEAD_DIM)
    shaped_v = value_rows.reshape(blocks, TOK_DEV, heads, HEAD_DIM)
    shaped_r = log_rates.reshape(heads, blocks, TOK_DEV).transpose(1, 0, 2)
    later = jnp.arange(TOK_DEV)[:, None] >= jnp.arange(TOK_DEV)[None, :]

    def advance(state, inputs):
        block_q, block_k, block_v, block_r = inputs
        cumulative = jnp.cumsum(block_r, axis=1)
        decay = jnp.exp(jnp.where(later[None], cumulative[:, :, None] - cumulative[:, None, :], -jnp.inf))
        query_f = block_q.astype(jnp.float32)
        key_f = block_k.astype(jnp.float32)
        value_f = block_v.astype(jnp.float32)
        weights = (jnp.einsum('thd,shd->hts', query_f, key_f) * fading_multiplier * decay).astype(jnp.bfloat16)
        inner = jnp.einsum('hts,shd->thd', weights.astype(jnp.float32), value_f)
        carried = jnp.einsum('thd,hde->the', query_f, state, precision=lax.Precision.HIGHEST)
        carried = carried * jnp.exp(cumulative).T[:, :, None]
        keyed = key_f * (jnp.exp(cumulative[:, -1:] - cumulative) * fading_multiplier).T[:, :, None]
        own_state = jnp.einsum('shd,she->hde', keyed, value_f, precision=lax.Precision.HIGHEST)
        state = jnp.exp(cumulative[:, -1])[:, None, None] * state + own_state
        return (state, inner + carried)
    start_state = jnp.zeros((heads, HEAD_DIM, HEAD_DIM), jnp.float32)
    _, outputs = lax.scan(advance, start_state, (shaped_q, shaped_k, shaped_v, shaped_r))
    outputs = outputs.reshape(-1, heads, HEAD_DIM)
    normed = outputs * lax.rsqrt(lax.optimization_barrier(jnp.mean(outputs * outputs, axis=-1, keepdims=True)) + EPS)
    return (normed.reshape(-1, heads * HEAD_DIM) * gain).astype(jnp.bfloat16)

def window_attention(query_rows, key_ext, value_ext, first_position, sinks):
    length = query_rows.shape[0]
    blocks = length // WINDOW
    heads_kv = key_ext.shape[1] // HEAD_DIM
    heads = query_rows.shape[1] // HEAD_DIM
    group = heads // heads_kv
    shaped_q = query_rows.astype(jnp.float32).reshape(blocks, WINDOW, heads_kv, group, HEAD_DIM)
    key_block_list = key_ext.astype(jnp.float32).reshape(blocks + 1, WINDOW, heads_kv, HEAD_DIM)
    value_blocks = value_ext.astype(jnp.float32).reshape(blocks + 1, WINDOW, heads_kv, HEAD_DIM)
    key_band = jnp.concatenate([key_block_list[:-1], key_block_list[1:]], axis=1)
    value_band = jnp.concatenate([value_blocks[:-1], value_blocks[1:]], axis=1)
    scores = jnp.einsum('nqhgd,nkhd->hgnqk', shaped_q, key_band) * HEAD_DIM ** (-0.5)
    distance = WINDOW + jnp.arange(WINDOW)[:, None] - jnp.arange(2 * WINDOW)[None, :]
    key_position = first_position - WINDOW + jnp.arange(blocks)[:, None] * WINDOW + jnp.arange(2 * WINDOW)[None, :]
    allowed = ((distance >= 0) & (distance < WINDOW))[None] & (key_position >= 0)[:, None, :]
    scores = jnp.where(allowed, scores, -jnp.inf)
    sink_part = sinks.reshape(heads_kv, group, 1, 1, 1)
    greatest_level = jnp.maximum(lax.optimization_barrier(jnp.max(scores, axis=-1, keepdims=True)), sink_part)
    raised = jnp.exp(scores - greatest_level)
    totals = lax.optimization_barrier(jnp.sum(raised, axis=-1, keepdims=True)) + jnp.exp(sink_part - greatest_level)
    weights = (raised / totals).astype(jnp.bfloat16)
    outputs = jnp.einsum('hgnqk,nkhd->nqhgd', weights.astype(jnp.float32), value_band)
    return outputs.reshape(length, heads * HEAD_DIM).astype(jnp.bfloat16)

def reference(tokens, in_gain, ret_query, ret_key, ret_value, att_query, att_key, att_value, log_decay, ret_gain, sink_logit, retentive_exit_matrix, out_att):
    results = []
    for sequence in range(tokens.shape[0]):
        wide = tokens[sequence].astype(jnp.float32)
        inverse = lax.rsqrt(lax.optimization_barrier(jnp.mean(wide * wide, axis=-1, keepdims=True)) + EPS)
        scaled = (wide * in_gain).astype(jnp.bfloat16)

        def project(weight):
            return (jnp.dot(scaled, weight, preferred_element_type=jnp.float32) * inverse).astype(jnp.bfloat16)
        ret_q = project(ret_query)
        ret_k = project(ret_key)
        ret_v = project(ret_value)
        att_q = project(att_query)
        att_k = project(att_key)
        att_v = project(att_value)
        ret_out = retention_sequence(ret_q, ret_k, ret_v, log_decay[sequence], ret_gain)
        padding = jnp.zeros((WINDOW, att_k.shape[1]), jnp.bfloat16)
        att_out = window_attention(att_q, jnp.concatenate([padding, att_k], axis=0), jnp.concatenate([padding, att_v], axis=0), 0, sink_logit)
        summed = jnp.dot(ret_out, retentive_exit_matrix, preferred_element_type=jnp.float32) + jnp.dot(att_out, out_att, preferred_element_type=jnp.float32)
        results.append(summed.astype(jnp.bfloat16))
    return jnp.stack(results)
```

```python
import functools

import jax
import jax.numpy as jnp
from jax import lax
from jax.experimental import pallas as pl
from jax.experimental.pallas import tpu as pltpu
from jax.sharding import Mesh
from jax.sharding import PartitionSpec as P

HEAD_DIM = 64
WINDOW = 128
EPS = 1e-06
SP = ("sp_0", "sp_1")
SP_TP = ("sp_0", "sp_1", "tp")
F32 = jnp.float32
BF16 = jnp.bfloat16
CHUNK = 256
STATE_ROWS = 192
LOG_ROWS = 16
PAY_ROWS = STATE_ROWS + LOG_ROWS
PAIRS = 3
LANES = 128
CONTRACT_ROWS = (((0,), (0,)), ((), ()))
CONTRACT_LANES = (((1,), (1,)), ((), ()))


def dot(a, b):
    return jnp.dot(a, b, preferred_element_type=F32)


def lane_ids(shape):
    return lax.broadcasted_iota(jnp.int32, shape, len(shape) - 1)


def row_ids(shape):
    return lax.broadcasted_iota(jnp.int32, shape, 0)


def half_mask(half, dtype):
    lanes = lane_ids((1, LANES))
    inside = (lanes < HEAD_DIM) if half == 0 else (lanes >= HEAD_DIM)
    return jnp.where(inside, 1.0, 0.0).astype(dtype)


def diagonal_mask():
    return (row_ids((LANES, LANES)) < HEAD_DIM) == (lane_ids((LANES, LANES)) < HEAD_DIM)


def split3(x):
    high = x.astype(BF16).astype(F32)
    rest = x - high
    middle = rest.astype(BF16).astype(F32)
    return high, middle, rest - middle


def call(body, grid, in_specs, out_specs, out_shape, scratch, scalars, flops, name):
    return pl.pallas_call(
        body,
        out_shape=out_shape,
        grid_spec=pltpu.PrefetchScalarGridSpec(
            num_scalar_prefetch=scalars,
            grid=grid,
            in_specs=in_specs,
            out_specs=out_specs,
            scratch_shapes=scratch,
        ),
        compiler_params=pltpu.CompilerParams(
            dimension_semantics=("arbitrary",) * len(grid), vmem_limit_bytes=48 * 2**20
        ),
        cost_estimate=pl.CostEstimate(flops=flops, transcendentals=0, bytes_accessed=1 << 20),
        name=name,
    )


def whole(shape):
    return pl.BlockSpec(shape, lambda *_: (0,) * len(shape))


def decay_body(rates_ref, row_ref, col_ref):
    heads, rows = rates_ref.shape
    row_ref[...] = jnp.zeros_like(row_ref)
    row_ref[0:heads, :] = rates_ref[...]
    total = row_ref[...]
    lanes = lane_ids(total.shape)
    step = 1
    while step < rows:
        total = total + jnp.where(lanes >= step, pltpu.roll(total, step, 1), 0.0)
        step *= 2
    row_ref[...] = total
    parts = jnp.concatenate(split3(total) + (jnp.zeros_like(total),), axis=0).astype(BF16)
    shape = (32, heads * HEAD_DIM)
    picks = (row_ids(shape) % 8 == lane_ids(shape) // HEAD_DIM).astype(F32).astype(BF16)
    col_ref[...] = lax.dot_general(parts, picks, CONTRACT_ROWS, preferred_element_type=F32)


def decays(rates):
    heads, rows = rates.shape
    return call(
        decay_body,
        (1,),
        [whole(rates.shape)],
        [whole((8, rows)), whole((rows, heads * HEAD_DIM))],
        [
            jax.ShapeDtypeStruct((8, rows), F32),
            jax.ShapeDtypeStruct((rows, heads * HEAD_DIM), F32),
        ],
        [],
        0,
        2**28,
        "decays",
    )(rates)


def scaled_block(x_ref, gain_ref):
    wide = x_ref[...].astype(F32)
    return wide, (wide * gain_ref[...]).astype(BF16)


def squares_of(wide):
    squares = wide * wide
    total = squares[:, 0:LANES]
    for start in range(LANES, wide.shape[1], LANES):
        total = total + squares[:, start : start + LANES]
    return total


def key_value_body(tp, own, peer, gain, wk, wv, col, k_out, v_out, inv_out, pay_out, acc, sq):
    step = pl.program_id(0)
    width = wk.shape[1]

    def add(x_ref):
        wide, scaled = scaled_block(x_ref, gain)
        part = squares_of(wide)
        left, right = dot(scaled, wk[...]), dot(scaled, wv[...])

        @pl.when(step == 0)
        def _():
            sq[...] = part
            acc[:, 0:width] = left
            acc[:, width:] = right

        @pl.when(step > 0)
        def _():
            sq[...] += part
            acc[:, 0:width] += left
            acc[:, width:] += right

    @pl.when(step < 2)
    def _():
        add(own)

    @pl.when(step >= 2)
    def _():
        add(peer)

    @pl.when(step == 3)
    def _():
        model_width = 4 * gain.shape[1]
        mean = jnp.sum(sq[...], axis=1, keepdims=True) / model_width
        inverse = lax.rsqrt(mean + EPS)
        inv_out[...] = jnp.broadcast_to(inverse, inv_out.shape)
        keys = (acc[:, 0:width] * inverse).astype(BF16) * jnp.asarray(HEAD_DIM**-0.5, BF16)
        values = (acc[:, width:] * inverse).astype(BF16)
        k_out[...] = keys
        v_out[...] = values
        rows = keys.shape[0]
        logs = jnp.zeros((LOG_ROWS, LANES), F32)
        places = row_ids((LOG_ROWS, LANES))
        low = lane_ids((HEAD_DIM, LANES)) < HEAD_DIM
        for p in range(PAIRS):
            lanes = slice(p * LANES, (p + 1) * LANES)
            cum = col[:, lanes]
            last = col[rows - 1 : rows, lanes]
            faded = (keys[:, lanes].astype(F32) * jnp.exp(last - cum)).astype(BF16)
            state = lax.dot_general(
                faded, values[:, lanes], CONTRACT_ROWS, preferred_element_type=F32
            )
            packed = jnp.where(low, state[0:HEAD_DIM], state[HEAD_DIM:])
            pay_out[p * HEAD_DIM : (p + 1) * HEAD_DIM, :] = packed.astype(BF16)
            for i, part in enumerate(split3(last)):
                logs = logs + jnp.where(places == 3 * p + i, part, 0.0)
        pay_out[STATE_ROWS:, :] = logs.astype(BF16)


def token_specs(rows):
    block = (rows, 512)
    return [
        pl.BlockSpec(block, lambda k, tp: (0, jnp.minimum(k, 1))),
        pl.BlockSpec(block, lambda k, tp: (0, jnp.maximum(k - 2, 0))),
        pl.BlockSpec((1, 512), lambda k, tp: (0, (2 * tp[0] + k) % 4)),
    ]


def weight_spec(width):
    return pl.BlockSpec((512, width), lambda k, tp: ((2 * tp[0] + k) % 4, 0))


def key_value(tp, own, peer, gain, wk, wv, col):
    rows, width = own.shape[0], wk.shape[1]
    return call(
        key_value_body,
        (4,),
        token_specs(rows) + [weight_spec(width), weight_spec(width), whole(col.shape)],
        [
            whole((rows, width)),
            whole((rows, width)),
            whole((rows, LANES)),
            whole((PAY_ROWS, LANES)),
        ],
        [
            jax.ShapeDtypeStruct((rows, width), BF16),
            jax.ShapeDtypeStruct((rows, width), BF16),
            jax.ShapeDtypeStruct((rows, LANES), F32),
            jax.ShapeDtypeStruct((PAY_ROWS, LANES), BF16),
        ],
        [pltpu.VMEM((rows, 2 * width), F32), pltpu.VMEM((rows, LANES), F32)],
        1,
        4 * rows * 2048 * width,
        "key_value",
    )(tp, own, peer, gain, wk, wv, col)


def rest_body(tp, own, peer, gain, w0, w1, w2, w3, inv, q_out, aq_out, akv_out, acc):
    step = pl.program_id(0)
    weights = (w0, w1, w2, w3)

    def add(x_ref):
        _, scaled = scaled_block(x_ref, gain)
        start = 0
        for w in weights:
            stop = start + w.shape[1]
            part = dot(scaled, w[...])
            lanes = slice(start, stop)

            @pl.when(step == 0)
            def _():
                acc[:, lanes] = part

            @pl.when(step > 0)
            def _():
                acc[:, lanes] += part

            start = stop

    @pl.when(step < 2)
    def _():
        add(own)

    @pl.when(step >= 2)
    def _():
        add(peer)

    @pl.when(step == 3)
    def _():
        inverse = inv[:, 0:1]
        a, b = w0.shape[1], w0.shape[1] + w1.shape[1]
        q_out[...] = (acc[:, 0:a] * inverse).astype(BF16)
        aq_out[...] = (acc[:, a:b] * inverse).astype(BF16) * jnp.asarray(HEAD_DIM**-0.5, BF16)
        akv_out[...] = (acc[:, b:] * inverse).astype(BF16)


def rest(tp, own, peer, gain, weights, inv):
    rows = own.shape[0]
    widths = [w.shape[1] for w in weights]
    shapes = [(rows, widths[0]), (rows, widths[1]), (rows, widths[2] + widths[3])]
    return call(
        rest_body,
        (4,),
        token_specs(rows) + [weight_spec(w) for w in widths] + [whole(inv.shape)],
        [whole(s) for s in shapes],
        [jax.ShapeDtypeStruct(s, BF16) for s in shapes],
        [pltpu.VMEM((rows, sum(widths)), F32)],
        1,
        2 * rows * 2048 * sum(widths),
        "rest",
    )(tp, own, peer, gain, *weights, inv)


def inner_body(q_ref, k_ref, v_ref, row_ref, col_ref, out_ref):
    pair = pl.program_id(0)
    rows = q_ref.shape[0]
    later = row_ids((CHUNK, CHUNK)) >= lane_ids((CHUNK, CHUNK))
    low = lane_ids((CHUNK, LANES)) < HEAD_DIM
    diagonal = diagonal_mask()
    masks = [half_mask(0, BF16), half_mask(1, BF16)]
    state = None
    start = None
    for begin in range(0, rows, CHUNK):
        here = slice(begin, begin + CHUNK)
        q, k, v, cum = q_ref[here, :], k_ref[here, :], v_ref[here, :], col_ref[here, :]
        parts = []
        for half in range(2):
            scores = lax.dot_general(
                q * masks[half], k, CONTRACT_LANES, preferred_element_type=F32
            )
            over = cum[:, half * HEAD_DIM : half * HEAD_DIM + 1]
            keyed = row_ref[pl.ds(2 * pair + half, 1), here]
            fade = jnp.exp(jnp.where(later, over - keyed, -jnp.inf))
            parts.append(dot((scores * fade).astype(BF16), v))
        out = jnp.where(low, parts[0], parts[1])
        end = col_ref[begin + CHUNK - 1 : begin + CHUNK, :]
        if state is not None:
            faded = (q.astype(F32) * jnp.exp(cum - start)).astype(BF16)
            out = out + dot(faded, state.astype(BF16))
        out_ref[here, :] = out
        if begin + CHUNK < rows:
            keyed = (k.astype(F32) * jnp.exp(end - cum)).astype(BF16)
            added = lax.dot_general(keyed, v, CONTRACT_ROWS, preferred_element_type=F32)
            added = jnp.where(diagonal, added, 0.0)
            state = added if state is None else state * jnp.exp(end - start) + added
            start = end


def inner(q, k, v, row, col):
    rows = q.shape[0]
    spec = pl.BlockSpec((rows, LANES), lambda p: (0, p))
    return call(
        inner_body,
        (PAIRS,),
        [spec, spec, spec, whole(row.shape), spec],
        spec,
        jax.ShapeDtypeStruct(q.shape, F32),
        [],
        0,
        3 * 2**30,
        "inner",
    )(q, k, v, row, col)


def logs_of(tile, p):
    return tile[3 * p : 3 * p + 1] + tile[3 * p + 1 : 3 * p + 2] + tile[3 * p + 2 : 3 * p + 3]


def state_of(ref, p):
    return ref[p * HEAD_DIM : (p + 1) * HEAD_DIM, :].astype(F32)


def log_tile(ref):
    return ref[STATE_ROWS:, :].astype(F32)


def row_in_tile(shape, p, row):
    return jnp.where(row_ids(shape) == p, row, 0.0)


def packed_logs(rows):
    places = row_ids((LOG_ROWS, LANES))
    logs = jnp.zeros((LOG_ROWS, LANES), F32)
    for p, row in enumerate(rows):
        for i, part in enumerate(split3(row)):
            logs = logs + jnp.where(places == 3 * p + i, part, 0.0)
    return logs.astype(BF16)


def line_body(where, own, one, two, three, before_out, log_out, pay_out):
    y = where[0]
    refs = (own, one, two, three)
    tiles = [log_tile(r) for r in refs]
    place = [(y - k + 4) % 4 for k in range(4)]
    lead = jnp.zeros((8, LANES), F32)
    totals = []
    for p in range(PAIRS):
        logs = [logs_of(t, p) for t in tiles]
        states = [state_of(r, p) for r in refs]
        total = jnp.zeros((HEAD_DIM, LANES), F32)
        before = jnp.zeros((HEAD_DIM, LANES), F32)
        between = jnp.zeros((1, LANES), F32)
        for k in range(4):
            after = jnp.zeros((1, LANES), F32)
            for j in range(4):
                if j != k:
                    after = after + jnp.where(place[j] > place[k], logs[j], 0.0)
            total = total + states[k] * jnp.exp(after)
            if k > 0:
                before = before + jnp.where(k <= y, states[k] * jnp.exp(between), 0.0)
                between = between + jnp.where(k <= y, logs[k], 0.0)
        here = slice(p * HEAD_DIM, (p + 1) * HEAD_DIM)
        before_out[here, :] = before
        lead = lead + row_in_tile((8, LANES), p, between)
        pay_out[here, :] = total.astype(BF16)
        totals.append(logs[0] + logs[1] + logs[2] + logs[3])
    log_out[...] = lead
    pay_out[STATE_ROWS:, :] = packed_logs(totals)


def column_body(where, own, one, two, before_out, log_out, pay_out):
    z = where[0]
    tiles = [log_tile(r) for r in (own, one, two)]
    lead = jnp.zeros((8, LANES), F32)
    totals = []
    for p in range(PAIRS):
        log0, log1, log2 = [logs_of(t, p) for t in tiles]
        log1 = jnp.where(z >= 1, log1, 0.0)
        log2 = jnp.where(z >= 2, log2, 0.0)
        before = jnp.where(z >= 1, state_of(one, p), 0.0)
        before = before + jnp.exp(log1) * jnp.where(z >= 2, state_of(two, p), 0.0)
        here = slice(p * HEAD_DIM, (p + 1) * HEAD_DIM)
        before_out[here, :] = before
        lead = lead + row_in_tile((8, LANES), p, log1 + log2)
        pay_out[here, :] = (state_of(own, p) + jnp.exp(log0) * before).astype(BF16)
        totals.append(log0 + log1 + log2)
    log_out[...] = lead
    pay_out[STATE_ROWS:, :] = packed_logs(totals)


def combine(body, where, payloads, name):
    return call(
        body,
        (1,),
        [whole((PAY_ROWS, LANES)) for _ in payloads],
        [whole((STATE_ROWS, LANES)), whole((8, LANES)), whole((PAY_ROWS, LANES))],
        [
            jax.ShapeDtypeStruct((STATE_ROWS, LANES), F32),
            jax.ShapeDtypeStruct((8, LANES), F32),
            jax.ShapeDtypeStruct((PAY_ROWS, LANES), BF16),
        ],
        [],
        1,
        2**26,
        name,
    )(where, *payloads)


def finish_body(
    where, q_ref, in_ref, col_ref, gain, line, line_log, column, column_log, three, six, out_ref
):
    z = where[1]
    tile3, tile6 = log_tile(three), log_tile(six)
    diagonal = diagonal_mask()
    ones = jnp.where(diagonal, 1.0, 0.0).astype(BF16)
    for p in range(PAIRS):
        here = slice(p * HEAD_DIM, (p + 1) * HEAD_DIM)
        lanes = slice(p * LANES, (p + 1) * LANES)
        far = jnp.where(z >= 3, state_of(three, p), 0.0)
        log3 = jnp.where(z >= 3, logs_of(tile3, p), 0.0)
        far = far + jnp.exp(log3) * jnp.where(z >= 6, state_of(six, p), 0.0)
        before = column[here, :] + jnp.exp(column_log[p : p + 1, :]) * far
        before = line[here, :] + jnp.exp(line_log[p : p + 1, :]) * before
        state = jnp.where(diagonal, jnp.concatenate([before, before], axis=0), 0.0).astype(BF16)
        carried = dot(q_ref[:, lanes], state) * jnp.exp(col_ref[:, lanes])
        retained = in_ref[:, lanes] + carried
        squares = retained * retained
        high = squares.astype(BF16)
        low = (squares - high.astype(F32)).astype(BF16)
        mean = (dot(high, ones) + dot(low, ones)) / HEAD_DIM
        out_ref[:, lanes] = (retained * lax.rsqrt(mean + EPS) * gain[:, lanes]).astype(BF16)


def finish(where, q, inside, col, gain, line, line_log, column, column_log, three, six):
    rows, width = q.shape
    spec = pl.BlockSpec((rows // 2, width), lambda i, w: (w[0], 0))
    small = [line, line_log, column, column_log, three, six]
    return call(
        finish_body,
        (1,),
        [spec, spec, spec, whole(gain.shape)] + [whole(s.shape) for s in small],
        whole((rows // 2, width)),
        jax.ShapeDtypeStruct((rows // 2, width), BF16),
        [],
        1,
        2**29,
        "finish",
    )(where, q, inside, col, gain, *small)


def window_body(where, q_ref, kv_ref, halo_ref, sink_ref, out_ref, ext):
    half, first = where[0], where[1]
    rows = q_ref.shape[0]
    begin = pl.multiple_of(half * rows, WINDOW)

    @pl.when(half == 0)
    def _():
        ext[0:WINDOW, :] = halo_ref[...]

    @pl.when(half == 1)
    def _():
        ext[0:WINDOW, :] = kv_ref[rows - WINDOW : rows, :]

    ext[WINDOW:, :] = kv_ref[pl.ds(begin, rows), :]
    masks = [half_mask(0, BF16), half_mask(1, BF16)]
    band = (WINDOW, 2 * WINDOW)
    distance = WINDOW + row_ids(band) - lane_ids(band)
    near = (distance >= 0) & (distance < WINDOW)
    low = lane_ids((WINDOW, LANES)) < HEAD_DIM
    heads = q_ref.shape[1] // HEAD_DIM
    group = heads // 2
    for block in range(rows // WINDOW):
        span = slice(block * WINDOW, (block + 2) * WINDOW)
        keys = ext[span, 0:LANES].astype(F32)
        values = ext[span, LANES:].astype(F32)
        keys = [keys.astype(BF16), pltpu.roll(keys, HEAD_DIM, 1).astype(BF16)]
        values = [values.astype(BF16), pltpu.roll(values, HEAD_DIM, 1).astype(BF16)]
        allowed = near
        if block == 0:
            behind = jnp.where((half == 0) & (first == 0), WINDOW, 0)
            allowed = near & (lane_ids(band) >= behind)
        here = slice(block * WINDOW, (block + 1) * WINDOW)
        outs = []
        for h in range(heads):
            lanes = slice(h // 2 * LANES, (h // 2 + 1) * LANES)
            turned = (h % 2) != (h // group)
            q = q_ref[here, lanes] * masks[h % 2]
            scores = lax.dot_general(
                q, keys[turned], CONTRACT_LANES, preferred_element_type=F32
            )
            scores = jnp.where(allowed, scores, -jnp.inf)
            sink = sink_ref[h]
            highest = jnp.maximum(jnp.max(scores, axis=1, keepdims=True), sink)
            raised = jnp.exp(scores - highest)
            total = jnp.sum(raised, axis=1, keepdims=True) + jnp.exp(sink - highest)
            weights = (raised * (1.0 / total)).astype(BF16)
            outs.append(dot(weights, values[turned]))
        for p in range(heads // 2):
            lanes = slice(p * LANES, (p + 1) * LANES)
            out_ref[here, lanes] = jnp.where(low, outs[2 * p], outs[2 * p + 1]).astype(BF16)


def window(where, q, kv, halo, sinks):
    rows, width = q.shape
    return call(
        window_body,
        (1,),
        [
            pl.BlockSpec((rows // 2, width), lambda i, w: (w[0], 0)),
            whole(kv.shape),
            whole(halo.shape),
            pl.BlockSpec(memory_space=pltpu.SMEM),
        ],
        whole((rows // 2, width)),
        jax.ShapeDtypeStruct((rows // 2, width), BF16),
        [pltpu.VMEM((rows // 2 + WINDOW, kv.shape[1]), BF16)],
        1,
        2**30,
        "window",
    )(where, q, kv, halo, sinks)


def first_exit_body(a, b, wa, wb, out):
    out[...] = dot(a[...], wa[...]) + dot(b[...], wb[...])


def last_exit_body(a, b, wa, wb, more, out):
    out[...] = (more[...] + dot(a[...], wa[...]) + dot(b[...], wb[...])).astype(BF16)


def exit_product(body, a, b, wa, wb, more, dtype, name):
    rows, width = a.shape[0], wa.shape[1]
    tile = 512
    columns = lambda n: pl.BlockSpec((n, tile), lambda j: (0, j))
    args = [a, b, wa, wb] + more
    specs = [whole(a.shape), whole(b.shape), columns(wa.shape[0]), columns(wb.shape[0])]
    return call(
        body,
        (width // tile,),
        specs + [columns(rows) for _ in more],
        columns(rows),
        jax.ShapeDtypeStruct((rows, width), dtype),
        [],
        0,
        4 * rows * a.shape[1] * width,
        name,
    )(*args)


def turned(value, axis, by):
    peers = lax.axis_size(axis)
    return lax.ppermute(value, axis, [(i, (i + by) % peers) for i in range(peers)])


def shards(
    tokens,
    in_gain,
    ret_query,
    ret_key,
    ret_value,
    att_query,
    att_key,
    att_value,
    log_decay,
    ret_gain,
    sink_logit,
    retentive_exit_matrix,
    out_att,
):
    tp = lax.axis_index("tp").astype(jnp.int32)
    y = lax.axis_index("sp_1").astype(jnp.int32)
    z = lax.axis_index("sp_0").astype(jnp.int32)
    own = tokens[0]
    gain = in_gain[None]
    peer = turned(own, "tp", 1)
    row, col = decays(log_decay[0])
    side = jnp.stack([tp])
    ret_k, ret_v, inv, payload = key_value(side, own, peer, gain, ret_key, ret_value, col)
    line_in = [payload] + [turned(payload, "sp_1", k) for k in (1, 2, 3)]
    ret_q, att_q, att_kv = rest(
        side, own, peer, gain, (ret_query, att_query, att_key, att_value), inv
    )
    peers = lax.axis_size(SP)
    halo = lax.ppermute(
        att_kv[att_kv.shape[0] - WINDOW :], SP, [(i, i + 1) for i in range(peers - 1)]
    )
    line, line_log, line_pay = combine(line_body, jnp.stack([y]), line_in, "line")
    column_in = [line_pay] + [turned(line_pay, "sp_0", k) for k in (1, 2)]
    inside = inner(ret_q, ret_k, ret_v, row, col)
    column, column_log, column_pay = combine(column_body, jnp.stack([z]), column_in, "column")
    three, six = turned(column_pay, "sp_0", 3), turned(column_pay, "sp_0", 6)
    first = z * lax.axis_size("sp_1") + y
    theirs = window(jnp.stack([1 - tp, first]), att_q, att_kv, halo, sink_logit)
    att_got = turned(theirs, "tp", 1)
    att_mine = window(jnp.stack([tp, first]), att_q, att_kv, halo, sink_logit)
    out_att_peer = turned(out_att, "tp", 1)
    exit_peer = turned(retentive_exit_matrix, "tp", 1)
    partial = exit_product(
        first_exit_body, att_mine, att_got, out_att, out_att_peer, [], F32, "att_exit"
    )
    args = (ret_q, inside, col, ret_gain[None], line, line_log, column, column_log, three, six)
    ret_got = turned(finish(jnp.stack([1 - tp, z]), *args), "tp", 1)
    ret_mine = finish(jnp.stack([tp, z]), *args)
    mixed = exit_product(
        last_exit_body,
        ret_mine,
        ret_got,
        retentive_exit_matrix,
        exit_peer,
        [partial],
        BF16,
        "ret_exit",
    )
    return mixed[None]


def solution(mesh):
    finer = Mesh(
        mesh.devices.reshape(8, 4, mesh.shape["fs"], mesh.shape["tp"]), ("sp_0", "sp_1", "fs", "tp")
    )
    placed = (
        P("fs", SP, "tp"),
        P(),
        P(None, "tp"),
        P(None, "tp"),
        P(None, "tp"),
        P(None, "tp"),
        P(None, "tp"),
        P(None, "tp"),
        P("fs", "tp", SP),
        P("tp"),
        P("tp"),
        P("tp", None),
        P("tp", None),
    )
    return jax.shard_map(
        shards, mesh=finer, in_specs=placed, out_specs=P("fs", SP_TP, None), check_vma=False
    )
```

```python
import functools

import jax
import jax.numpy as jnp
from jax import lax
from jax.experimental import pallas as pl
from jax.experimental.pallas import tpu as pltpu
from jax.sharding import Mesh
from jax.sharding import PartitionSpec as P

HEAD_DIM = 64
WINDOW = 128
EPS = 1e-06
SP = ("sp_0", "sp_1")
SP_TP = ("sp_0", "sp_1", "tp")
F32 = jnp.float32
BF16 = jnp.bfloat16
CHUNK = 256
STATE_ROWS = 192
LOG_ROWS = 16
PAY_ROWS = STATE_ROWS + LOG_ROWS
PAIRS = 3
LANES = 128
CONTRACT_ROWS = (((0,), (0,)), ((), ()))
CONTRACT_LANES = (((1,), (1,)), ((), ()))


def dot(a, b):
    return jnp.dot(a, b, preferred_element_type=F32)


def lane_ids(shape):
    return lax.broadcasted_iota(jnp.int32, shape, len(shape) - 1)


def row_ids(shape):
    return lax.broadcasted_iota(jnp.int32, shape, 0)


def half_mask(half, dtype):
    lanes = lane_ids((1, LANES))
    inside = (lanes < HEAD_DIM) if half == 0 else (lanes >= HEAD_DIM)
    return jnp.where(inside, 1.0, 0.0).astype(dtype)


def diagonal_mask():
    return (row_ids((LANES, LANES)) < HEAD_DIM) == (lane_ids((LANES, LANES)) < HEAD_DIM)


def split3(x):
    high = x.astype(BF16).astype(F32)
    rest = x - high
    middle = rest.astype(BF16).astype(F32)
    return high, middle, rest - middle


def call(body, in_specs, out_specs, out_shape, scratch, scalars, flops, mib, name, grid=(1,)):
    return pl.pallas_call(
        body,
        out_shape=out_shape,
        grid_spec=pltpu.PrefetchScalarGridSpec(
            num_scalar_prefetch=scalars,
            grid=grid,
            in_specs=in_specs,
            out_specs=out_specs,
            scratch_shapes=scratch,
        ),
        compiler_params=pltpu.CompilerParams(
            dimension_semantics=("arbitrary",) * len(grid), vmem_limit_bytes=mib * 2**20
        ),
        cost_estimate=pl.CostEstimate(flops=flops, transcendentals=0, bytes_accessed=1 << 20),
        name=name,
    )


def whole(shape):
    return pl.BlockSpec(shape, lambda *_: (0,) * len(shape))


IN_HBM = pl.BlockSpec(memory_space=pltpu.HBM)
SCALE = HEAD_DIM**-0.5


def in_hbm(x):
    return pltpu.with_memory_space_constraint(x, pltpu.HBM)


def fetch_weights(weights, buffer, sems, begin):
    copies, start = [], 0
    depth = buffer.shape[0]
    for i, w in enumerate(weights):
        stop = start + w.shape[1]
        copy = pltpu.make_async_copy(
            w.at[pl.ds(begin, depth), :], buffer.at[:, start:stop], sems.at[i]
        )
        copy.start()
        copies.append(copy)
        start = stop
    return copies


def weight_columns(weights, begin, depth, start):
    pieces, left = [], 0
    for w in weights:
        for n in range(0, w.shape[1], LANES):
            if start <= left + n < start + CHUNK:
                pieces.append(w[pl.ds(begin, depth), n : n + LANES])
        left += w.shape[1]
    return jnp.concatenate(pieces, axis=1)


def squares_of(wide):
    squares = wide * wide
    total = squares[:, 0:LANES]
    for start in range(LANES, wide.shape[1], LANES):
        total = total + squares[:, start : start + LANES]
    return total


def decays(rates_ref, row_ref, col_ref):
    heads, _, rows = rates_ref.shape
    row_ref[...] = jnp.zeros_like(row_ref)
    for h in range(heads):
        row_ref[h : h + 1, :] = rates_ref[h]
    total = row_ref[...]
    lanes = lane_ids(total.shape)
    step = 1
    while step < rows:
        total = total + jnp.where(lanes >= step, pltpu.roll(total, step, 1), 0.0)
        step *= 2
    row_ref[...] = total
    parts = jnp.concatenate(split3(total) + (jnp.zeros_like(total),), axis=0).astype(BF16)
    shape = (32, heads * HEAD_DIM)
    picks = (row_ids(shape) % 8 == lane_ids(shape) // HEAD_DIM).astype(F32).astype(BF16)
    col_ref[...] = lax.dot_general(parts, picks, CONTRACT_ROWS, preferred_element_type=F32)


def own_body(tp, x_hbm, gain_hbm, rates_hbm, *refs):
    weights = refs[:6]
    first, second, sq, row, col, xbuf, gain, rates, wbuf, sbuf, sems = refs[6:]
    rows, depth = xbuf.shape
    small = pltpu.make_async_copy(rates_hbm, rates, sems.at[8])
    small.start()
    load = pltpu.make_async_copy(x_hbm, xbuf, sems.at[6])
    load.start()
    gains = pltpu.make_async_copy(gain_hbm, gain, sems.at[7])
    gains.start()
    begin = pl.multiple_of(tp[0] * depth, depth)
    copies = fetch_weights(weights, wbuf, sems, begin)
    small.wait()
    decays(rates, row, col)
    gains.wait()
    load.wait()
    scale = gain[:, pl.ds(begin, depth)]
    for m in range(0, rows, CHUNK):
        wide = xbuf[m : m + CHUNK, :].astype(F32)
        sbuf[m : m + CHUNK, :] = (wide * scale).astype(BF16)
        sq[m : m + CHUNK, :] = squares_of(wide)
    split = first.shape[1]
    groups = ((first, 0, split, copies[:4]), (second, split, wbuf.shape[1], copies[4:]))
    for out, start, stop, waits in groups:
        for copy in waits:
            copy.wait()
        for n in range(start, stop, CHUNK):
            for m in range(0, rows, CHUNK):
                out[m : m + CHUNK, n - start : n - start + CHUNK] = dot(
                    sbuf[m : m + CHUNK, :], wbuf[:, n : n + CHUNK]
                )


def own_half(tp, own, gain, rates, weights):
    rows, depth = own.shape
    widths = [w.shape[1] for w in weights]
    shapes = [
        ((rows, sum(widths[:4])), F32),
        ((rows, sum(widths[4:])), F32),
        ((rows, LANES), F32),
        ((8, rows), F32),
        ((rows, widths[0]), F32),
    ]
    return call(
        own_body,
        [IN_HBM] * 9,
        [whole(s) for s, _ in shapes],
        [jax.ShapeDtypeStruct(s, t) for s, t in shapes],
        [
            pltpu.VMEM((rows, depth), BF16),
            pltpu.VMEM(gain.shape, F32),
            pltpu.VMEM(rates.shape, F32),
            pltpu.VMEM((depth, sum(widths)), BF16),
            pltpu.VMEM((rows, depth), BF16),
            pltpu.SemaphoreType.DMA((9,)),
        ],
        1,
        2 * rows * depth * sum(widths),
        24,
        "own_half",
    )(tp, *[in_hbm(a) for a in (own, gain, rates) + weights])


def keys_body(tp, x, gain, part, sq, col, *refs):
    weights = refs[:4]
    k_out, v_out, akv_out, inv_out, scaled_out, pay_out, more_out = refs[4:]
    rows, depth = x.shape
    width = k_out.shape[1]
    begin = pl.multiple_of((1 - tp[0]) * depth, depth)
    scale = gain[:, pl.ds(begin, depth)]
    low = lane_ids((HEAD_DIM, LANES)) < HEAD_DIM
    for m in range(0, rows, CHUNK):
        here = slice(m, m + CHUNK)
        wide = x[here, :].astype(F32)
        scaled_out[here, :] = (wide * scale).astype(BF16)
        mean = jnp.sum(sq[here, :] + squares_of(wide), axis=1, keepdims=True) / (2 * depth)
        inv_out[here, :] = jnp.broadcast_to(lax.rsqrt(mean + EPS), (CHUNK, LANES))
    for m in range(0, rows, CHUNK):
        here = slice(m, m + CHUNK)
        inverse = inv_out[here, 0:1]
        scaled = scaled_out[here, :]
        for n in range(0, part.shape[1], CHUNK):
            columns = weight_columns(weights, begin, depth, n)
            total = part[here, n : n + CHUNK] + dot(scaled, columns)
            value = (total * inverse).astype(BF16)
            for j in range(n, n + CHUNK, LANES):
                piece = value[:, j - n : j - n + LANES]
                if j < width:
                    k_out[here, j : j + LANES] = piece * jnp.asarray(SCALE, BF16)
                elif j < 2 * width:
                    v_out[here, j - width : j - width + LANES] = piece
                else:
                    akv_out[here, j - 2 * width : j - 2 * width + LANES] = piece
    logs = jnp.zeros((LOG_ROWS, LANES), F32)
    places = row_ids((LOG_ROWS, LANES))
    for p in range(PAIRS):
        lanes = slice(p * LANES, (p + 1) * LANES)
        last = col[rows - 1 : rows, lanes]
        faded = (k_out[:, lanes].astype(F32) * jnp.exp(last - col[:, lanes])).astype(BF16)
        state = lax.dot_general(faded, v_out[:, lanes], CONTRACT_ROWS, preferred_element_type=F32)
        packed = jnp.where(low, state[0:HEAD_DIM], state[HEAD_DIM:]).astype(BF16)
        pay_out[p * HEAD_DIM : (p + 1) * HEAD_DIM, :] = packed
        more_out[p * HEAD_DIM : (p + 1) * HEAD_DIM, :] = packed
        for i, part3 in enumerate(split3(last)):
            logs = logs + jnp.where(places == 3 * p + i, part3, 0.0)
    pay_out[STATE_ROWS:, :] = logs.astype(BF16)
    more_out[STATE_ROWS:PAY_ROWS, :] = logs.astype(BF16)
    tail = slice(rows - WINDOW, rows)
    more_out[PAY_ROWS : PAY_ROWS + WINDOW, :] = akv_out[tail, 0:LANES]
    more_out[PAY_ROWS + WINDOW :, :] = akv_out[tail, LANES:]


def keys_half(tp, peer, gain, part, sq, col, weights):
    rows, depth = peer.shape
    widths = [w.shape[1] for w in weights]
    shapes = [
        ((rows, widths[0]), BF16),
        ((rows, widths[1]), BF16),
        ((rows, widths[2] + widths[3]), BF16),
        ((rows, LANES), F32),
        ((rows, depth), BF16),
        ((PAY_ROWS, LANES), BF16),
        ((PAY_ROWS + 2 * WINDOW, LANES), BF16),
    ]
    return call(
        keys_body,
        [whole(a.shape) for a in (peer, gain, part, sq, col) + weights],
        [whole(s) for s, _ in shapes],
        [jax.ShapeDtypeStruct(s, t) for s, t in shapes],
        [],
        1,
        2 * rows * depth * sum(widths),
        20,
        "keys_half",
    )(tp, peer, gain, part, sq, col, *weights)


def queries_body(tp, scaled, part, inv, w0, w1, q_out, aq_out):
    rows, depth = scaled.shape
    width = q_out.shape[1]
    begin = pl.multiple_of((1 - tp[0]) * depth, depth)
    for m in range(0, rows, CHUNK):
        here = slice(m, m + CHUNK)
        inverse = inv[here, 0:1]
        for n in range(0, part.shape[1], CHUNK):
            columns = weight_columns((w0, w1), begin, depth, n)
            total = part[here, n : n + CHUNK] + dot(scaled[here, :], columns)
            value = (total * inverse).astype(BF16)
            for j in range(n, n + CHUNK, LANES):
                piece = value[:, j - n : j - n + LANES]
                if j < width:
                    q_out[here, j : j + LANES] = piece
                else:
                    aq_out[here, j - width : j - width + LANES] = piece * jnp.asarray(SCALE, BF16)


def queries_half(tp, scaled, part, inv, w0, w1):
    rows, depth = scaled.shape
    shapes = [(rows, w0.shape[1]), (rows, w1.shape[1])]
    return call(
        queries_body,
        [whole(a.shape) for a in (scaled, part, inv, w0, w1)],
        [whole(s) for s in shapes],
        [jax.ShapeDtypeStruct(s, BF16) for s in shapes],
        [],
        1,
        2 * rows * depth * part.shape[1],
        16,
        "queries_half",
    )(tp, scaled, part, inv, w0, w1)


def inner_body(q_ref, k_ref, v_ref, row_ref, col_ref, out_ref):
    rows = q_ref.shape[0]
    later = row_ids((CHUNK, CHUNK)) >= lane_ids((CHUNK, CHUNK))
    low = lane_ids((CHUNK, LANES)) < HEAD_DIM
    diagonal = diagonal_mask()
    masks = [half_mask(0, BF16), half_mask(1, BF16)]
    for pair in range(PAIRS):
        lanes = slice(pair * LANES, (pair + 1) * LANES)
        state = start = None
        for begin in range(0, rows, CHUNK):
            here = slice(begin, begin + CHUNK)
            q, k, v = q_ref[here, lanes], k_ref[here, lanes], v_ref[here, lanes]
            cum = col_ref[here, lanes]
            parts = []
            for half in range(2):
                scores = lax.dot_general(
                    q * masks[half], k, CONTRACT_LANES, preferred_element_type=F32
                )
                over = cum[:, half * HEAD_DIM : half * HEAD_DIM + 1]
                keyed = row_ref[2 * pair + half : 2 * pair + half + 1, here]
                fade = jnp.exp(jnp.where(later, over - keyed, -jnp.inf))
                parts.append(dot((scores * fade).astype(BF16), v))
            out = jnp.where(low, parts[0], parts[1])
            end = col_ref[begin + CHUNK - 1 : begin + CHUNK, lanes]
            if state is not None:
                faded = (q.astype(F32) * jnp.exp(cum - start)).astype(BF16)
                out = out + dot(faded, state.astype(BF16))
            out_ref[here, lanes] = out
            if begin + CHUNK < rows:
                keyed = (k.astype(F32) * jnp.exp(end - cum)).astype(BF16)
                added = lax.dot_general(keyed, v, CONTRACT_ROWS, preferred_element_type=F32)
                added = jnp.where(diagonal, added, 0.0)
                state = added if state is None else state * jnp.exp(end - start) + added
                start = end


def inner(q, k, v, row, col):
    args = (q, k, v, row, col)
    return call(
        inner_body,
        [whole(a.shape) for a in args],
        whole(q.shape),
        jax.ShapeDtypeStruct(q.shape, F32),
        [],
        0,
        3 * 2**30,
        12,
        "inner",
    )(*args)


def logs_of(tile, p):
    return tile[3 * p : 3 * p + 1] + tile[3 * p + 1 : 3 * p + 2] + tile[3 * p + 2 : 3 * p + 3]


def state_of(ref, p):
    return ref[p * HEAD_DIM : (p + 1) * HEAD_DIM, :].astype(F32)


def log_tile(ref):
    return ref[STATE_ROWS:PAY_ROWS, :].astype(F32)


def behind(index, shifts, refs, tiles, p):
    state, log = None, None
    for shift, ref, tile in reversed(list(zip(shifts, refs, tiles))):
        here = jnp.where(index >= shift, state_of(ref, p), 0.0)
        rate = jnp.where(index >= shift, logs_of(tile, p), 0.0)
        state = here if state is None else here + jnp.exp(rate) * state
        log = rate if log is None else rate + log
    return state, log


def scan_body(shifts, where, own, *refs):
    known = len(shifts) == 2
    if known:
        near, near_log = refs[:2]
        refs = refs[2:]
    sources, (near_out, log_out, pay_out) = refs[: len(shifts)], refs[len(shifts) :]
    tiles = [log_tile(r) for r in sources]
    own_tile = log_tile(own)
    lead = jnp.zeros((8, LANES), F32)
    logs = jnp.zeros((LOG_ROWS, LANES), F32)
    places = row_ids((LOG_ROWS, LANES))
    for p in range(PAIRS):
        here = slice(p * HEAD_DIM, (p + 1) * HEAD_DIM)
        before, log = behind(where[0], shifts, sources, tiles, p)
        if known:
            before = near[here, :] + jnp.exp(near_log[p : p + 1, :]) * before
            log = near_log[p : p + 1, :] + log
        own_log = logs_of(own_tile, p)
        near_out[here, :] = before
        lead = lead + jnp.where(row_ids((8, LANES)) == p, log, 0.0)
        pay_out[here, :] = (state_of(own, p) + jnp.exp(own_log) * before).astype(BF16)
        for i, part in enumerate(split3(own_log + log)):
            logs = logs + jnp.where(places == 3 * p + i, part, 0.0)
    log_out[...] = lead
    pay_out[STATE_ROWS:, :] = logs.astype(BF16)


def scan_step(shifts, where, own, near, sources, name):
    args = [own] + near + sources
    return call(
        functools.partial(scan_body, shifts),
        [whole(a.shape) for a in args],
        [whole((STATE_ROWS, LANES)), whole((8, LANES)), whole((PAY_ROWS, LANES))],
        [
            jax.ShapeDtypeStruct((STATE_ROWS, LANES), F32),
            jax.ShapeDtypeStruct((8, LANES), F32),
            jax.ShapeDtypeStruct((PAY_ROWS, LANES), BF16),
        ],
        [],
        1,
        2**26,
        4,
        name,
    )(where, *args)


def finish_body(shifts, side, spot, q_ref, in_ref, col_ref, gain, near, near_log, *refs):
    sources, out_ref = refs[:-1], refs[-1]
    tiles = [log_tile(r) for r in sources]
    diagonal = diagonal_mask()
    ones = jnp.where(diagonal, 1.0, 0.0).astype(BF16)
    for p in range(PAIRS):
        here = slice(p * HEAD_DIM, (p + 1) * HEAD_DIM)
        lanes = slice(p * LANES, (p + 1) * LANES)
        far, _ = behind(spot[0], shifts, sources, tiles, p)
        before = near[here, :] + jnp.exp(near_log[p : p + 1, :]) * far
        state = jnp.where(diagonal, jnp.concatenate([before, before], axis=0), 0.0).astype(BF16)
        carried = dot(q_ref[:, lanes], state) * jnp.exp(col_ref[:, lanes])
        retained = in_ref[:, lanes] + carried
        squares = retained * retained
        high = squares.astype(BF16)
        rest = (squares - high.astype(F32)).astype(BF16)
        mean = (dot(high, ones) + dot(rest, ones)) / HEAD_DIM
        out_ref[:, lanes] = (retained * lax.rsqrt(mean + EPS) * gain[:, lanes]).astype(BF16)


def finish(shifts, mine, side, spot, q, inside, col, gain, near, near_log, sources):
    rows, width = q.shape
    spec = pl.BlockSpec((rows // 2, width), lambda i, t, f: (half_of(t, mine), 0))
    small = [near, near_log] + sources
    return call(
        functools.partial(finish_body, shifts),
        [spec, spec, spec, whole(gain.shape)] + [whole(s.shape) for s in small],
        whole((rows // 2, width)),
        jax.ShapeDtypeStruct((rows // 2, width), BF16),
        [],
        2,
        2**29,
        8,
        "finish",
    )(side, spot, q, inside, col, gain, *small)


def half_of(side, mine):
    return side[0] if mine else 1 - side[0]


def window_body(mine, side, spot, q_ref, kv_ref, halo_ref, sink_ref, out_ref, ext):
    half, first = half_of(side, mine), spot[0]
    rows = q_ref.shape[0]
    begin = pl.multiple_of(half * rows, WINDOW)

    @pl.when(half == 0)
    def _():
        ext[0:WINDOW, 0:LANES] = halo_ref[PAY_ROWS : PAY_ROWS + WINDOW, :]
        ext[0:WINDOW, LANES:] = halo_ref[PAY_ROWS + WINDOW :, :]

    @pl.when(half == 1)
    def _():
        ext[0:WINDOW, :] = kv_ref[rows - WINDOW : rows, :]

    ext[WINDOW:, :] = kv_ref[pl.ds(begin, rows), :]
    masks = [half_mask(0, BF16), half_mask(1, BF16)]
    heads = q_ref.shape[1] // HEAD_DIM
    group = heads // 2
    band = (2 * WINDOW, group * WINDOW)
    place = lane_ids(band) % WINDOW
    distance = WINDOW + place - row_ids(band)
    near = (distance >= 0) & (distance < WINDOW)
    spot = lane_ids((1, group * WINDOW)) // WINDOW
    for block in range(rows // WINDOW):
        span = slice(block * WINDOW, (block + 2) * WINDOW)
        keys, values = ext[span, 0:LANES], ext[span, LANES:]
        allowed = near
        if block == 0:
            behind_rows = jnp.where((half == 0) & (first == 0), WINDOW, 0)
            allowed = near & (row_ids(band) >= behind_rows)
        here = slice(block * WINDOW, (block + 1) * WINDOW)
        outs = []
        for g in range(2):
            stack = []
            sink = jnp.zeros((1, group * WINDOW), F32)
            for j in range(group):
                h = g * group + j
                q = q_ref[here, h // 2 * LANES : (h // 2 + 1) * LANES]
                if h % 2 != g:
                    q = pltpu.roll(q.astype(F32), HEAD_DIM, 1).astype(BF16)
                stack.append(q * masks[g])
                sink = sink + jnp.where(spot == j, sink_ref[h], 0.0)
            scores = lax.dot_general(
                keys, jnp.concatenate(stack, axis=0), CONTRACT_LANES, preferred_element_type=F32
            )
            scores = jnp.where(allowed, scores, -jnp.inf)
            highest = jnp.maximum(jnp.max(scores, axis=0, keepdims=True), sink)
            raised = jnp.exp(scores - highest)
            total = jnp.sum(raised, axis=0, keepdims=True) + jnp.exp(sink - highest)
            weights = (raised * (1.0 / total)).astype(BF16)
            out = lax.dot_general(values, weights, CONTRACT_ROWS, preferred_element_type=F32)
            out = out[g * HEAD_DIM : (g + 1) * HEAD_DIM]
            outs += [out[:, j * WINDOW : (j + 1) * WINDOW] for j in range(group)]
        for p in range(heads // 2):
            both = jnp.concatenate([outs[2 * p], outs[2 * p + 1]], axis=0)
            out_ref[here, p * LANES : (p + 1) * LANES] = both.T.astype(BF16)


def window(mine, side, spot, q, kv, halo, sinks):
    rows, width = q.shape
    return call(
        functools.partial(window_body, mine),
        [
            pl.BlockSpec((rows // 2, width), lambda i, t, f: (half_of(t, mine), 0)),
            whole(kv.shape),
            whole(halo.shape),
            pl.BlockSpec(memory_space=pltpu.SMEM),
        ],
        whole((rows // 2, width)),
        jax.ShapeDtypeStruct((rows // 2, width), BF16),
        [pltpu.VMEM((rows // 2 + WINDOW, kv.shape[1]), BF16)],
        2,
        2**30,
        8,
        "window",
    )(side, spot, q, kv, halo, sinks)


def first_exit_body(a, b, wa, wb, out):
    rows = jnp.concatenate([a[...], b[...]], axis=1)
    for n in range(0, out.shape[1], CHUNK):
        here = slice(n, n + CHUNK)
        out[:, here] = dot(rows, jnp.concatenate([wa[:, here], wb[:, here]], axis=0))


def last_exit_body(a, b, wa, wb, more, out, buffer, sems):
    rows = jnp.concatenate([a[...], b[...]], axis=1)
    copies = []
    for i, n in enumerate(range(0, out.shape[1], 2 * CHUNK)):
        for m in (n, n + CHUNK):
            here = slice(m, m + CHUNK)
            part = dot(rows, jnp.concatenate([wa[:, here], wb[:, here]], axis=0))
            buffer[:, here] = (more[:, here] + part).astype(BF16)
        copy = pltpu.make_async_copy(
            buffer.at[:, n : n + 2 * CHUNK], out.at[:, n : n + 2 * CHUNK], sems.at[i]
        )
        copy.start()
        copies.append(copy)
    for copy in copies:
        copy.wait()


def first_exit(a, b, wa, wb):
    args = (a, b, wa, wb)
    shape = (a.shape[0], wa.shape[1])
    return call(
        first_exit_body,
        [whole(x.shape) for x in args],
        whole(shape),
        jax.ShapeDtypeStruct(shape, F32),
        [],
        0,
        4 * a.shape[0] * a.shape[1] * wa.shape[1],
        12,
        "first_exit",
    )(*args)


def last_exit(a, b, wa, wb, more):
    args = (a, b, wa, wb, more)
    shape = (a.shape[0], wa.shape[1])
    return call(
        last_exit_body,
        [whole(x.shape) for x in args],
        IN_HBM,
        jax.ShapeDtypeStruct(shape, BF16),
        [pltpu.VMEM(shape, BF16), pltpu.SemaphoreType.DMA((shape[1] // (2 * CHUNK),))],
        0,
        4 * a.shape[0] * a.shape[1] * wa.shape[1],
        16,
        "last_exit",
    )(*args)


def turned(value, axis, by):
    peers = lax.axis_size(axis)
    return lax.ppermute(value, axis, [(i, (i + by) % peers) for i in range(peers)])


def shards(
    tokens,
    in_gain,
    ret_query,
    ret_key,
    ret_value,
    att_query,
    att_key,
    att_value,
    log_decay,
    ret_gain,
    sink_logit,
    retentive_exit_matrix,
    out_att,
):
    tp = lax.axis_index("tp").astype(jnp.int32)
    place = lax.axis_index(SP).astype(jnp.int32)
    own = tokens[0]
    gain = in_gain[None]
    side, spot = tp.reshape(1), place.reshape(1)
    peer = turned(own, "tp", 1)
    early = (ret_key, ret_value, att_key, att_value)
    rates = log_decay.reshape(log_decay.shape[1], 1, log_decay.shape[2])
    first, second, squares, row, col = own_half(
        side, own, gain, rates, early + (ret_query, att_query)
    )
    ret_k, ret_v, att_kv, inv, scaled, payload, more = keys_half(
        side, peer, gain, first, squares, col, early
    )
    sources = [turned(more, SP, 1), turned(payload, SP, 2), turned(payload, SP, 3)]
    ret_q, att_q = queries_half(side, scaled, second, inv, ret_query, att_query)
    inside = inner(ret_q, ret_k, ret_v, row, col)
    sources, inside = lax.optimization_barrier((sources, inside))
    halo = sources[0]
    near, near_log, span = scan_step((1, 2, 3), spot, payload, [], sources, "scan_one")
    sources = [turned(span, "sp_0", 1), turned(span, "sp_0", 2)]
    theirs = window(False, side, spot, att_q, att_kv, halo, sink_logit)
    att_got = turned(theirs, "tp", 1)
    sources, theirs = lax.optimization_barrier((sources, theirs))
    att_mine = window(True, side, spot, att_q, att_kv, halo, sink_logit)
    near, near_log, span = scan_step(
        (4, 8), spot, payload, [near, near_log], sources, "scan_two"
    )
    sources = [turned(span, "sp_0", 3), turned(span, "sp_0", 6)]
    out_att_peer = turned(out_att, "tp", 1)
    exit_peer = turned(retentive_exit_matrix, "tp", 1)
    partial = first_exit(att_mine, att_got, out_att, out_att_peer)
    sources, partial = lax.optimization_barrier((sources, partial))
    args = (ret_q, inside, col, ret_gain[None], near, near_log, sources)
    ret_got = turned(finish((12, 24), False, side, spot, *args), "tp", 1)
    ret_mine = finish((12, 24), True, side, spot, *args)
    mixed = last_exit(ret_mine, ret_got, retentive_exit_matrix, exit_peer, partial)
    return mixed[None]


def solution(mesh):
    finer = Mesh(
        mesh.devices.reshape(8, 4, mesh.shape["fs"], mesh.shape["tp"]), ("sp_0", "sp_1", "fs", "tp")
    )
    placed = (
        P("fs", SP, "tp"),
        P(),
        P(None, "tp"),
        P(None, "tp"),
        P(None, "tp"),
        P(None, "tp"),
        P(None, "tp"),
        P(None, "tp"),
        P("fs", "tp", SP),
        P("tp"),
        P("tp"),
        P("tp", None),
        P("tp", None),
    )
    return jax.shard_map(
        shards, mesh=finer, in_specs=placed, out_specs=P("fs", SP_TP, None), check_vma=False
    )
```

```python
import functools

import jax
import jax.numpy as jnp
from jax import lax
from jax.experimental import pallas as pl
from jax.experimental.pallas import tpu as pltpu
from jax.sharding import Mesh
from jax.sharding import PartitionSpec as P


HEAD_DIM = 64
WINDOW = 128
EPS = 1e-06
SP = ("sp_0", "sp_1")
SP_TP = ("sp_0", "sp_1", "tp")
F32 = jnp.float32
BF16 = jnp.bfloat16
CHUNK = 256
STATE_ROWS = 192
LOG_ROWS = 16
PAY_ROWS = STATE_ROWS + LOG_ROWS
PAIRS = 3
LANES = 128
CONTRACT_ROWS = (((0,), (0,)), ((), ()))
CONTRACT_LANES = (((1,), (1,)), ((), ()))


def dot(a, b):
    return jnp.dot(a, b, preferred_element_type=F32)


def lane_ids(shape):
    return lax.broadcasted_iota(jnp.int32, shape, len(shape) - 1)


def row_ids(shape):
    return lax.broadcasted_iota(jnp.int32, shape, 0)


def half_mask(half, dtype):
    lanes = lane_ids((1, LANES))
    inside = (lanes < HEAD_DIM) if half == 0 else (lanes >= HEAD_DIM)
    return jnp.where(inside, 1.0, 0.0).astype(dtype)


def diagonal_mask():
    return (row_ids((LANES, LANES)) < HEAD_DIM) == (lane_ids((LANES, LANES)) < HEAD_DIM)


def split3(x):
    high = x.astype(BF16).astype(F32)
    rest = x - high
    middle = rest.astype(BF16).astype(F32)
    return high, middle, rest - middle


def call(body, in_specs, out_specs, out_shape, scratch, scalars, flops, mib, name, grid=(1,)):
    return pl.pallas_call(
        body,
        out_shape=out_shape,
        grid_spec=pltpu.PrefetchScalarGridSpec(
            num_scalar_prefetch=scalars,
            grid=grid,
            in_specs=in_specs,
            out_specs=out_specs,
            scratch_shapes=scratch,
        ),
        compiler_params=pltpu.CompilerParams(
            dimension_semantics=("arbitrary",) * len(grid), vmem_limit_bytes=mib * 2**20
        ),
        cost_estimate=pl.CostEstimate(flops=flops, transcendentals=0, bytes_accessed=1 << 20),
        name=name,
    )


def whole(shape):
    return pl.BlockSpec(shape, lambda *_: (0,) * len(shape))


IN_HBM = pl.BlockSpec(memory_space=pltpu.HBM)
SCALE = HEAD_DIM**-0.5


def in_hbm(x):
    return pltpu.with_memory_space_constraint(x, pltpu.HBM)


def fetch_weights(weights, buffer, sems, begin):
    copies, start = [], 0
    depth = buffer.shape[0]
    for i, w in enumerate(weights):
        stop = start + w.shape[1]
        copy = pltpu.make_async_copy(
            w.at[pl.ds(begin, depth), :], buffer.at[:, start:stop], sems.at[i]
        )
        copy.start()
        copies.append(copy)
        start = stop
    return copies


def weight_columns(weights, begin, depth, start):
    pieces, left = [], 0
    for w in weights:
        for n in range(0, w.shape[1], LANES):
            if start <= left + n < start + CHUNK:
                pieces.append(w[pl.ds(begin, depth), n : n + LANES])
        left += w.shape[1]
    return jnp.concatenate(pieces, axis=1)


def squares_of(wide):
    squares = wide * wide
    total = squares[:, 0:LANES]
    for start in range(LANES, wide.shape[1], LANES):
        total = total + squares[:, start : start + LANES]
    return total


def decays(rates_ref, row_ref, col_ref):
    heads, _, rows = rates_ref.shape
    row_ref[...] = jnp.zeros_like(row_ref)
    for h in range(heads):
        row_ref[h : h + 1, :] = rates_ref[h]
    total = row_ref[...]
    lanes = lane_ids(total.shape)
    step = 1
    while step < rows:
        total = total + jnp.where(lanes >= step, pltpu.roll(total, step, 1), 0.0)
        step *= 2
    row_ref[...] = total
    parts = jnp.concatenate(split3(total) + (jnp.zeros_like(total),), axis=0).astype(BF16)
    shape = (32, heads * HEAD_DIM)
    picks = (row_ids(shape) % 8 == lane_ids(shape) // HEAD_DIM).astype(F32).astype(BF16)
    col_ref[...] = lax.dot_general(parts, picks, CONTRACT_ROWS, preferred_element_type=F32)


def own_body(tp, x_hbm, gain_hbm, rates_hbm, *refs):
    weights = refs[:4]
    first, scaled, sq, row, col, xbuf, gain, rates, wbuf, sems = refs[4:]
    rows, depth = xbuf.shape
    small = pltpu.make_async_copy(rates_hbm, rates, sems.at[8])
    small.start()
    load = pltpu.make_async_copy(x_hbm, xbuf, sems.at[6])
    load.start()
    gains = pltpu.make_async_copy(gain_hbm, gain, sems.at[7])
    gains.start()
    begin = pl.multiple_of(tp[0] * depth, depth)
    copies = fetch_weights(weights, wbuf, sems, begin)
    small.wait()
    decays(rates, row, col)
    gains.wait()
    load.wait()
    scale = gain[:, pl.ds(begin, depth)]
    for m in range(0, rows, CHUNK):
        wide = xbuf[m : m + CHUNK, :].astype(F32)
        scaled[m : m + CHUNK, :] = (wide * scale).astype(BF16)
        sq[m : m + CHUNK, :] = squares_of(wide)
    for copy in copies:
        copy.wait()
    for n in range(0, first.shape[1], CHUNK):
        for m in range(0, rows, CHUNK):
            here = slice(m, m + CHUNK)
            first[here, n : n + CHUNK] = dot(scaled[here, :], wbuf[:, n : n + CHUNK])


def own_half(tp, own, gain, rates, weights):
    rows, depth = own.shape
    widths = [w.shape[1] for w in weights]
    shapes = [
        ((rows, sum(widths)), F32),
        ((rows, depth), BF16),
        ((rows, LANES), F32),
        ((8, rows), F32),
        ((rows, widths[0]), F32),
    ]
    return call(
        own_body,
        [IN_HBM] * 7,
        [whole(s) for s, _ in shapes],
        [jax.ShapeDtypeStruct(s, t) for s, t in shapes],
        [
            pltpu.VMEM((rows, depth), BF16),
            pltpu.VMEM(gain.shape, F32),
            pltpu.VMEM(rates.shape, F32),
            pltpu.VMEM((depth, sum(widths)), BF16),
            pltpu.SemaphoreType.DMA((9,)),
        ],
        1,
        2 * rows * depth * sum(widths),
        24,
        "own_half",
    )(tp, *[in_hbm(a) for a in (own, gain, rates) + weights])


def keys_body(tp, x, gain, part, sq, col, *refs):
    weights = refs[:4]
    k_out, v_out, akv_out, inv_out, scaled_out, pay_out, tail_out = refs[4:]
    rows, depth = x.shape
    width = k_out.shape[1]
    begin = pl.multiple_of((1 - tp[0]) * depth, depth)
    scale = gain[:, pl.ds(begin, depth)]
    low = lane_ids((HEAD_DIM, LANES)) < HEAD_DIM
    for m in range(0, rows, CHUNK):
        here = slice(m, m + CHUNK)
        wide = x[here, :].astype(F32)
        scaled_out[here, :] = (wide * scale).astype(BF16)
        mean = jnp.sum(sq[here, :] + squares_of(wide), axis=1, keepdims=True) / (2 * depth)
        inv_out[here, :] = jnp.broadcast_to(lax.rsqrt(mean + EPS), (CHUNK, LANES))
    for m in range(0, rows, CHUNK):
        here = slice(m, m + CHUNK)
        inverse = inv_out[here, 0:1]
        scaled = scaled_out[here, :]
        for n in range(0, part.shape[1], CHUNK):
            columns = weight_columns(weights, begin, depth, n)
            total = part[here, n : n + CHUNK] + dot(scaled, columns)
            value = (total * inverse).astype(BF16)
            for j in range(n, n + CHUNK, LANES):
                piece = value[:, j - n : j - n + LANES]
                if j < width:
                    k_out[here, j : j + LANES] = piece * jnp.asarray(SCALE, BF16)
                elif j < 2 * width:
                    v_out[here, j - width : j - width + LANES] = piece
                else:
                    akv_out[here, j - 2 * width : j - 2 * width + LANES] = piece
    logs = jnp.zeros((LOG_ROWS, LANES), F32)
    places = row_ids((LOG_ROWS, LANES))
    for p in range(PAIRS):
        lanes = slice(p * LANES, (p + 1) * LANES)
        last = col[rows - 1 : rows, lanes]
        faded = (k_out[:, lanes].astype(F32) * jnp.exp(last - col[:, lanes])).astype(BF16)
        state = lax.dot_general(faded, v_out[:, lanes], CONTRACT_ROWS, preferred_element_type=F32)
        packed = jnp.where(low, state[0:HEAD_DIM], state[HEAD_DIM:]).astype(BF16)
        pay_out[p * HEAD_DIM : (p + 1) * HEAD_DIM, :] = packed
        for i, part3 in enumerate(split3(last)):
            logs = logs + jnp.where(places == 3 * p + i, part3, 0.0)
    pay_out[STATE_ROWS:, :] = logs.astype(BF16)
    tail_out[...] = akv_out[rows - WINDOW : rows, :]


def keys_half(tp, peer, gain, part, sq, col, weights):
    rows, depth = peer.shape
    widths = [w.shape[1] for w in weights]
    shapes = [
        ((rows, widths[0]), BF16),
        ((rows, widths[1]), BF16),
        ((rows, widths[2] + widths[3]), BF16),
        ((rows, LANES), F32),
        ((rows, depth), BF16),
        ((PAY_ROWS, LANES), BF16),
        ((WINDOW, widths[2] + widths[3]), BF16),
    ]
    return call(
        keys_body,
        [whole(a.shape) for a in (peer, gain, part, sq, col) + weights],
        [whole(s) for s, _ in shapes],
        [jax.ShapeDtypeStruct(s, t) for s, t in shapes],
        [],
        1,
        2 * rows * depth * sum(widths),
        20,
        "keys_half",
    )(tp, peer, gain, part, sq, col, *weights)


def queries_body(tp, own, peer, inv, w0, w1, q_out, aq_out):
    rows, depth = own.shape
    width = q_out.shape[1]
    begin = pl.multiple_of(tp[0] * depth, depth)
    other = pl.multiple_of((1 - tp[0]) * depth, depth)
    weights = (w0, w1)
    for m in range(0, rows, CHUNK):
        here = slice(m, m + CHUNK)
        inverse = inv[here, 0:1]
        for n in range(0, 2 * width, CHUNK):
            total = dot(own[here, :], weight_columns(weights, begin, depth, n))
            total = total + dot(peer[here, :], weight_columns(weights, other, depth, n))
            value = (total * inverse).astype(BF16)
            for j in range(n, n + CHUNK, LANES):
                piece = value[:, j - n : j - n + LANES]
                if j < width:
                    q_out[here, j : j + LANES] = piece
                else:
                    aq_out[here, j - width : j - width + LANES] = piece * jnp.asarray(SCALE, BF16)


def queries(tp, own, peer, inv, w0, w1):
    rows, depth = own.shape
    shapes = [(rows, w0.shape[1]), (rows, w1.shape[1])]
    return call(
        queries_body,
        [whole(a.shape) for a in (own, peer, inv, w0, w1)],
        [whole(s) for s in shapes],
        [jax.ShapeDtypeStruct(s, BF16) for s in shapes],
        [],
        1,
        8 * rows * depth * w0.shape[1],
        20,
        "queries",
    )(tp, own, peer, inv, w0, w1)


def inner_body(q_ref, k_ref, v_ref, row_ref, col_ref, out_ref):
    rows = q_ref.shape[0]
    later = row_ids((CHUNK, CHUNK)) >= lane_ids((CHUNK, CHUNK))
    low = lane_ids((CHUNK, LANES)) < HEAD_DIM
    diagonal = diagonal_mask()
    masks = [half_mask(0, BF16), half_mask(1, BF16)]
    for pair in range(PAIRS):
        lanes = slice(pair * LANES, (pair + 1) * LANES)
        state = start = None
        for begin in range(0, rows, CHUNK):
            here = slice(begin, begin + CHUNK)
            q, k, v = q_ref[here, lanes], k_ref[here, lanes], v_ref[here, lanes]
            cum = col_ref[here, lanes]
            parts = []
            for half in range(2):
                scores = lax.dot_general(
                    q * masks[half], k, CONTRACT_LANES, preferred_element_type=F32
                )
                over = cum[:, half * HEAD_DIM : half * HEAD_DIM + 1]
                keyed = row_ref[2 * pair + half : 2 * pair + half + 1, here]
                fade = jnp.exp(jnp.where(later, over - keyed, -jnp.inf))
                parts.append(dot((scores * fade).astype(BF16), v))
            out = jnp.where(low, parts[0], parts[1])
            end = col_ref[begin + CHUNK - 1 : begin + CHUNK, lanes]
            if state is not None:
                faded = (q.astype(F32) * jnp.exp(cum - start)).astype(BF16)
                out = out + dot(faded, state.astype(BF16))
            out_ref[here, lanes] = out
            if begin + CHUNK < rows:
                keyed = (k.astype(F32) * jnp.exp(end - cum)).astype(BF16)
                added = lax.dot_general(keyed, v, CONTRACT_ROWS, preferred_element_type=F32)
                added = jnp.where(diagonal, added, 0.0)
                state = added if state is None else state * jnp.exp(end - start) + added
                start = end


def inner(q, k, v, row, col):
    args = (q, k, v, row, col)
    return call(
        inner_body,
        [whole(a.shape) for a in args],
        whole(q.shape),
        jax.ShapeDtypeStruct(q.shape, F32),
        [],
        0,
        3 * 2**30,
        12,
        "inner",
    )(*args)


def logs_of(tile, p):
    return tile[3 * p : 3 * p + 1] + tile[3 * p + 1 : 3 * p + 2] + tile[3 * p + 2 : 3 * p + 3]


def state_of(ref, p):
    return ref[p * HEAD_DIM : (p + 1) * HEAD_DIM, :].astype(F32)


def log_tile(ref):
    return ref[STATE_ROWS:PAY_ROWS, :].astype(F32)


def write_logs(pay_out, rows):
    places = row_ids((LOG_ROWS, LANES))
    logs = jnp.zeros((LOG_ROWS, LANES), F32)
    for p, row in enumerate(rows):
        for i, part in enumerate(split3(row)):
            logs = logs + jnp.where(places == 3 * p + i, part, 0.0)
    pay_out[STATE_ROWS:, :] = logs.astype(BF16)


def line_body(place, *refs):
    y = place[0]
    sources, (before_out, log_out, pay_out) = refs[:4], refs[4:]
    tiles = [log_tile(r) for r in sources]
    spots = [(y - k + 4) % 4 for k in range(4)]
    lead = jnp.zeros((8, LANES), F32)
    totals = []
    for p in range(PAIRS):
        here = slice(p * HEAD_DIM, (p + 1) * HEAD_DIM)
        logs = [logs_of(t, p) for t in tiles]
        states = [state_of(r, p) for r in sources]
        total = before = between = None
        for k in range(4):
            after = jnp.zeros((1, LANES), F32)
            for j in range(4):
                if j != k:
                    after = after + jnp.where(spots[j] > spots[k], logs[j], 0.0)
            part = states[k] * jnp.exp(after)
            total = part if total is None else total + part
            if k > 0:
                part = jnp.where(k <= y, states[k], 0.0)
                part = part if between is None else part * jnp.exp(between)
                before = part if before is None else before + part
                rate = jnp.where(k <= y, logs[k], 0.0)
                between = rate if between is None else between + rate
        before_out[here, :] = before
        lead = lead + jnp.where(row_ids((8, LANES)) == p, between, 0.0)
        pay_out[here, :] = total.astype(BF16)
        totals.append(logs[0] + logs[1] + logs[2] + logs[3])
    log_out[...] = lead
    write_logs(pay_out, totals)


def column_body(place, own, back, ahead, before_out, log_out, pay_out):
    z = place[0]
    last = z == 7
    tiles = [log_tile(r) for r in (own, back, ahead)]
    lead = jnp.zeros((8, LANES), F32)
    totals = []
    for p in range(PAIRS):
        here = slice(p * HEAD_DIM, (p + 1) * HEAD_DIM)
        log, log_back, log_ahead = [logs_of(t, p) for t in tiles]
        before = jnp.where(z >= 1, state_of(back, p), 0.0)
        rate = jnp.where(z >= 1, log_back, 0.0)
        before_out[here, :] = before
        lead = lead + jnp.where(row_ids((8, LANES)) == p, rate, 0.0)
        inner_part = jnp.where(last, 0.0, state_of(own, p) + jnp.exp(log) * before)
        pay_out[here, :] = (state_of(ahead, p) + jnp.exp(log_ahead) * inner_part).astype(BF16)
        totals.append(log_ahead + jnp.where(last, 0.0, log + rate))
    log_out[...] = lead
    write_logs(pay_out, totals)


def scan_step(body, place, sources, name):
    return call(
        body,
        [whole(a.shape) for a in sources],
        [whole((STATE_ROWS, LANES)), whole((8, LANES)), whole((PAY_ROWS, LANES))],
        [
            jax.ShapeDtypeStruct((STATE_ROWS, LANES), F32),
            jax.ShapeDtypeStruct((8, LANES), F32),
            jax.ShapeDtypeStruct((PAY_ROWS, LANES), BF16),
        ],
        [],
        1,
        2**26,
        4,
        name,
    )(place, *sources)


def finish_body(side, row, q_ref, in_ref, col_ref, gain, *refs):
    line, line_log, column, column_log, three, six, out_ref = refs
    z = row[0]
    tile3, tile6 = log_tile(three), log_tile(six)
    diagonal = diagonal_mask()
    ones = jnp.where(diagonal, 1.0, 0.0).astype(BF16)
    for p in range(PAIRS):
        here = slice(p * HEAD_DIM, (p + 1) * HEAD_DIM)
        lanes = slice(p * LANES, (p + 1) * LANES)
        far = jnp.where(z >= 2, state_of(three, p), 0.0)
        rate = jnp.where(z >= 2, logs_of(tile3, p), 0.0)
        far = far + jnp.exp(rate) * jnp.where(z >= 5, state_of(six, p), 0.0)
        before = column[here, :] + jnp.exp(column_log[p : p + 1, :]) * far
        before = line[here, :] + jnp.exp(line_log[p : p + 1, :]) * before
        state = jnp.where(diagonal, jnp.concatenate([before, before], axis=0), 0.0).astype(BF16)
        carried = dot(q_ref[:, lanes], state) * jnp.exp(col_ref[:, lanes])
        retained = in_ref[:, lanes] + carried
        squares = retained * retained
        high = squares.astype(BF16)
        rest = (squares - high.astype(F32)).astype(BF16)
        mean = (dot(high, ones) + dot(rest, ones)) / HEAD_DIM
        out_ref[:, lanes] = (
            retained * lax.rsqrt(mean + EPS) * gain[lanes].reshape(1, LANES)
        ).astype(BF16)


def finish(mine, side, row, q, inside, col, gain, small):
    rows, width = q.shape
    spec = pl.BlockSpec((rows // 2, width), lambda i, t, z: (half_of(t, mine), 0))
    return call(
        finish_body,
        [spec, spec, spec, whole(gain.shape)] + [whole(s.shape) for s in small],
        whole((rows // 2, width)),
        jax.ShapeDtypeStruct((rows // 2, width), BF16),
        [],
        2,
        2**29,
        8,
        "finish",
    )(side, row, q, inside, col, gain, *small)


def half_of(side, mine):
    return side[0] if mine else 1 - side[0]


def window_body(mine, side, spot, q_ref, kv_ref, halo_ref, sink_ref, out_ref, ext):
    half, first = half_of(side, mine), spot[0]
    rows = q_ref.shape[0]
    begin = pl.multiple_of(half * rows, WINDOW)

    @pl.when(half == 0)
    def _():
        ext[0:WINDOW, :] = halo_ref[...]

    @pl.when(half == 1)
    def _():
        ext[0:WINDOW, :] = kv_ref[rows - WINDOW : rows, :]

    ext[WINDOW:, :] = kv_ref[pl.ds(begin, rows), :]
    masks = [half_mask(0, BF16), half_mask(1, BF16)]
    heads = q_ref.shape[1] // HEAD_DIM
    group = heads // 2
    band = (2 * WINDOW, group * WINDOW)
    place = lane_ids(band) % WINDOW
    distance = WINDOW + place - row_ids(band)
    near = (distance >= 0) & (distance < WINDOW)
    spot = lane_ids((1, group * WINDOW)) // WINDOW
    for block in range(rows // WINDOW):
        span = slice(block * WINDOW, (block + 2) * WINDOW)
        keys, values = ext[span, 0:LANES], ext[span, LANES:]
        allowed = near
        if block == 0:
            behind_rows = jnp.where((half == 0) & (first == 0), WINDOW, 0)
            allowed = near & (row_ids(band) >= behind_rows)
        here = slice(block * WINDOW, (block + 1) * WINDOW)
        outs = []
        for g in range(2):
            stack = []
            sink = jnp.zeros((1, group * WINDOW), F32)
            for j in range(group):
                h = g * group + j
                q = q_ref[here, h // 2 * LANES : (h // 2 + 1) * LANES]
                if h % 2 != g:
                    q = pltpu.roll(q.astype(F32), HEAD_DIM, 1).astype(BF16)
                stack.append(q * masks[g])
                sink = sink + jnp.where(spot == j, sink_ref[h], 0.0)
            scores = lax.dot_general(
                keys, jnp.concatenate(stack, axis=0), CONTRACT_LANES, preferred_element_type=F32
            )
            scores = jnp.where(allowed, scores, -jnp.inf)
            highest = jnp.maximum(jnp.max(scores, axis=0, keepdims=True), sink)
            raised = jnp.exp(scores - highest)
            total = jnp.sum(raised, axis=0, keepdims=True) + jnp.exp(sink - highest)
            weights = (raised * (1.0 / total)).astype(BF16)
            out = lax.dot_general(values, weights, CONTRACT_ROWS, preferred_element_type=F32)
            out = out[g * HEAD_DIM : (g + 1) * HEAD_DIM]
            outs += [out[:, j * WINDOW : (j + 1) * WINDOW] for j in range(group)]
        for p in range(heads // 2):
            both = jnp.concatenate([outs[2 * p], outs[2 * p + 1]], axis=0)
            out_ref[here, p * LANES : (p + 1) * LANES] = both.T.astype(BF16)


def window(mine, side, spot, q, kv, halo, sinks):
    rows, width = q.shape
    return call(
        functools.partial(window_body, mine),
        [
            pl.BlockSpec((rows // 2, width), lambda i, t, f: (half_of(t, mine), 0)),
            whole(kv.shape),
            whole(halo.shape),
            pl.BlockSpec(memory_space=pltpu.SMEM),
        ],
        whole((rows // 2, width)),
        jax.ShapeDtypeStruct((rows // 2, width), BF16),
        [pltpu.VMEM((rows // 2 + WINDOW, kv.shape[1]), BF16)],
        2,
        2**30,
        8,
        "window",
    )(side, spot, q, kv, halo, sinks)


def first_exit_body(a, b, wa, wb, out):
    rows = jnp.concatenate([a[...], b[...]], axis=1)
    for n in range(0, out.shape[1], CHUNK):
        here = slice(n, n + CHUNK)
        out[:, here] = dot(rows, jnp.concatenate([wa[:, here], wb[:, here]], axis=0))


def own_exit_body(a, w, more, out):
    for n in range(0, out.shape[1], CHUNK):
        here = slice(n, n + CHUNK)
        out[:, here] = more[:, here] + dot(a[...], w[:, here])


def last_exit_body(a, w, more, out, buffer, sems):
    copies = []
    for i, n in enumerate(range(0, out.shape[1], CHUNK)):
        here = slice(n, n + CHUNK)
        buffer[:, here] = (more[:, here] + dot(a[...], w[:, here])).astype(BF16)
        copy = pltpu.make_async_copy(buffer.at[:, here], out.at[:, here], sems.at[i])
        copy.start()
        copies.append(copy)
    for copy in copies:
        copy.wait()


def first_exit(a, b, wa, wb):
    args = (a, b, wa, wb)
    shape = (a.shape[0], wa.shape[1])
    return call(
        first_exit_body,
        [whole(x.shape) for x in args],
        whole(shape),
        jax.ShapeDtypeStruct(shape, F32),
        [],
        0,
        4 * a.shape[0] * a.shape[1] * wa.shape[1],
        12,
        "first_exit",
    )(*args)


def own_exit(a, w, more):
    args = (a, w, more)
    return call(
        own_exit_body,
        [whole(x.shape) for x in args],
        whole(more.shape),
        jax.ShapeDtypeStruct(more.shape, F32),
        [],
        0,
        2 * a.shape[0] * a.shape[1] * w.shape[1],
        12,
        "own_exit",
    )(*args)


def last_exit(a, w, more):
    args = (a, w, more)
    shape = (a.shape[0], w.shape[1])
    return call(
        last_exit_body,
        [whole(x.shape) for x in args],
        IN_HBM,
        jax.ShapeDtypeStruct(shape, BF16),
        [pltpu.VMEM(shape, BF16), pltpu.SemaphoreType.DMA((shape[1] // CHUNK,))],
        0,
        2 * a.shape[0] * a.shape[1] * w.shape[1],
        14,
        "last_exit",
    )(*args)


def turned(value, axis, by):
    peers = lax.axis_size(axis)
    return lax.ppermute(value, axis, [(i, (i + by) % peers) for i in range(peers)])


def shards(
    tokens,
    in_gain,
    ret_query,
    ret_key,
    ret_value,
    att_query,
    att_key,
    att_value,
    log_decay,
    ret_gain,
    sink_logit,
    retentive_exit_matrix,
    out_att,
):
    tp = lax.axis_index("tp").astype(jnp.int32)
    y = lax.axis_index("sp_1").astype(jnp.int32)
    z = lax.axis_index("sp_0").astype(jnp.int32)
    side, spot, row = tp.reshape(1), lax.axis_index(SP).astype(jnp.int32).reshape(1), z.reshape(1)
    side, spot, row, line_spot = lax.optimization_barrier((side, spot, row, y.reshape(1)))
    own = tokens[0]
    gain = in_gain[None]
    peer = turned(own, "tp", 1)
    early = (ret_key, ret_value, att_key, att_value)
    rates = log_decay.reshape(log_decay.shape[1], 1, log_decay.shape[2])
    first, scaled_own, squares, row_cum, col = own_half(side, own, gain, rates, early)
    ret_k, ret_v, att_kv, inv, scaled, payload, tail = keys_half(
        side, peer, gain, first, squares, col, early
    )
    sources = [payload] + [turned(payload, "sp_1", k) for k in (1, 2, 3)]
    peers = lax.axis_size(SP)
    halo = lax.ppermute(tail, SP, [(i, (i + 1) % peers) for i in range(peers)])
    ret_q, att_q = queries(side, scaled_own, scaled, inv, ret_query, att_query)
    exit_own, out_own = retentive_exit_matrix, out_att
    out_peer = turned(out_own, "tp", 1)
    exit_peer = turned(exit_own, "tp", 1)
    inside = inner(ret_q, ret_k, ret_v, row_cum, col)
    sources, inside = lax.optimization_barrier((sources, inside))
    line, line_log, span = scan_step(line_body, line_spot, sources, "line")
    sources = [span, turned(span, "sp_0", 1), turned(span, "sp_0", 7)]
    side, span = lax.optimization_barrier((side, span))
    theirs = window(False, side, spot, att_q, att_kv, halo, sink_logit)
    sources, theirs = lax.optimization_barrier((sources, theirs))
    att_got = turned(theirs, "tp", 1)
    column, column_log, span = scan_step(column_body, row, sources, "column")
    sources = [turned(span, "sp_0", 3), turned(span, "sp_0", 6)]
    side, span = lax.optimization_barrier((side, span))
    att_mine = window(True, side, spot, att_q, att_kv, halo, sink_logit)
    partial = first_exit(att_mine, att_got, out_att, out_peer)
    sources, partial = lax.optimization_barrier((sources, partial))
    small = [line, line_log, column, column_log] + sources
    args = (side, row, ret_q, inside, col, ret_gain, small)
    ret_got = turned(finish(False, *args), "tp", 1)
    ret_mine = finish(True, *args)
    partial = own_exit(ret_mine, retentive_exit_matrix, partial)
    mixed = last_exit(ret_got, exit_peer, partial)
    return mixed[None]


def solution(mesh):
    finer = Mesh(
        mesh.devices.reshape(8, 4, mesh.shape["fs"], mesh.shape["tp"]), ("sp_0", "sp_1", "fs", "tp")
    )
    placed = (
        P("fs", SP, "tp"),
        P(),
        P(None, "tp"),
        P(None, "tp"),
        P(None, "tp"),
        P(None, "tp"),
        P(None, "tp"),
        P(None, "tp"),
        P("fs", "tp", SP),
        P("tp"),
        P("tp"),
        P("tp", None),
        P("tp", None),
    )
    return jax.shard_map(
        shards, mesh=finer, in_specs=placed, out_specs=P("fs", SP_TP, None), check_vma=False
    )
```

```python
import functools

import jax
import jax.numpy as jnp
from jax import lax
from jax.experimental import pallas as pl
from jax.experimental.pallas import tpu as pltpu
from jax.sharding import Mesh
from jax.sharding import PartitionSpec as P


HEAD_DIM = 64
WINDOW = 128
EPS = 1e-06
SP = ("sp_0", "sp_1")
SP_TP = ("sp_0", "sp_1", "tp")
F32 = jnp.float32
BF16 = jnp.bfloat16
CHUNK = 256
STATE_ROWS = 192
LOG_ROWS = 16
PAY_ROWS = STATE_ROWS + LOG_ROWS
PAIRS = 3
LANES = 128
CONTRACT_ROWS = (((0,), (0,)), ((), ()))
CONTRACT_LANES = (((1,), (1,)), ((), ()))


def dot(a, b):
    return jnp.dot(a, b, preferred_element_type=F32)


def lane_ids(shape):
    return lax.broadcasted_iota(jnp.int32, shape, len(shape) - 1)


def row_ids(shape):
    return lax.broadcasted_iota(jnp.int32, shape, 0)


def half_mask(half, dtype):
    lanes = lane_ids((1, LANES))
    inside = (lanes < HEAD_DIM) if half == 0 else (lanes >= HEAD_DIM)
    return jnp.where(inside, 1.0, 0.0).astype(dtype)


def diagonal_mask():
    return (row_ids((LANES, LANES)) < HEAD_DIM) == (lane_ids((LANES, LANES)) < HEAD_DIM)


def split3(x):
    high = x.astype(BF16).astype(F32)
    rest = x - high
    middle = rest.astype(BF16).astype(F32)
    return high, middle, rest - middle


def call(body, in_specs, out_specs, out_shape, scratch, scalars, flops, mib, grid=(1,)):
    return pl.pallas_call(
        body,
        out_shape=out_shape,
        grid_spec=pltpu.PrefetchScalarGridSpec(
            num_scalar_prefetch=scalars,
            grid=grid,
            in_specs=in_specs,
            out_specs=out_specs,
            scratch_shapes=scratch,
        ),
        compiler_params=pltpu.CompilerParams(
            dimension_semantics=("arbitrary",) * len(grid), vmem_limit_bytes=mib * 2**20
        ),
        cost_estimate=pl.CostEstimate(flops=flops, transcendentals=0, bytes_accessed=1 << 20),
    )


def whole(shape):
    return pl.BlockSpec(shape, lambda *_: (0,) * len(shape))


IN_HBM = pl.BlockSpec(memory_space=pltpu.HBM)
SCALE = HEAD_DIM**-0.5


def in_hbm(x):
    return pltpu.with_memory_space_constraint(x, pltpu.HBM)


def fetch_weights(weights, buffer, sems, begin):
    copies, start = [], 0
    depth = buffer.shape[0]
    for i, w in enumerate(weights):
        stop = start + w.shape[1]
        copy = pltpu.make_async_copy(
            w.at[pl.ds(begin, depth), :], buffer.at[:, start:stop], sems.at[i]
        )
        copy.start()
        copies.append(copy)
        start = stop
    return copies


def weight_columns(weights, begin, depth, start):
    pieces, left = [], 0
    for w in weights:
        for n in range(0, w.shape[1], LANES):
            if start <= left + n < start + CHUNK:
                pieces.append(w[pl.ds(begin, depth), n : n + LANES])
        left += w.shape[1]
    return jnp.concatenate(pieces, axis=1)


def squares_of(wide):
    squares = wide * wide
    total = squares[:, 0:LANES]
    for start in range(LANES, wide.shape[1], LANES):
        total = total + squares[:, start : start + LANES]
    return total


def decays(rates_ref, row_ref, col_ref):
    heads, _, rows = rates_ref.shape
    row_ref[...] = jnp.zeros_like(row_ref)
    for h in range(heads):
        row_ref[h : h + 1, :] = rates_ref[h]
    total = row_ref[...]
    lanes = lane_ids(total.shape)
    step = 1
    while step < rows:
        total = total + jnp.where(lanes >= step, pltpu.roll(total, step, 1), 0.0)
        step *= 2
    row_ref[...] = total
    parts = jnp.concatenate(split3(total) + (jnp.zeros_like(total),), axis=0).astype(BF16)
    shape = (32, heads * HEAD_DIM)
    picks = (row_ids(shape) % 8 == lane_ids(shape) // HEAD_DIM).astype(F32).astype(BF16)
    col_ref[...] = lax.dot_general(parts, picks, CONTRACT_ROWS, preferred_element_type=F32)


def own_body(tp, x_hbm, gain_hbm, rates_hbm, *refs):
    weights = refs[:4]
    first, scaled, sq, row, col, xbuf, gain, rates, wbuf, sems = refs[4:]
    rows, depth = xbuf.shape
    small = pltpu.make_async_copy(rates_hbm, rates, sems.at[8])
    small.start()
    load = pltpu.make_async_copy(x_hbm, xbuf, sems.at[6])
    load.start()
    gains = pltpu.make_async_copy(gain_hbm, gain, sems.at[7])
    gains.start()
    begin = pl.multiple_of(tp[0] * depth, depth)
    copies = fetch_weights(weights, wbuf, sems, begin)
    small.wait()
    decays(rates, row, col)
    gains.wait()
    load.wait()
    for copy in copies:
        copy.wait()
    scale = gain[:, pl.ds(begin, depth)]
    for m in range(0, rows, CHUNK):
        here = slice(m, m + CHUNK)
        wide = xbuf[here, :].astype(F32)
        part = (wide * scale).astype(BF16)
        scaled[here, :] = part
        sq[here, :] = squares_of(wide)
        for n in range(0, first.shape[1], CHUNK):
            first[here, n : n + CHUNK] = dot(part, wbuf[:, n : n + CHUNK])


def own_half(tp, own, gain, rates, weights):
    rows, depth = own.shape
    widths = [w.shape[1] for w in weights]
    shapes = [
        ((rows, sum(widths)), F32),
        ((rows, depth), BF16),
        ((rows, LANES), F32),
        ((8, rows), F32),
        ((rows, widths[0]), F32),
    ]
    return call(
        own_body,
        [IN_HBM] * 7,
        [whole(s) for s, _ in shapes],
        [jax.ShapeDtypeStruct(s, t) for s, t in shapes],
        [
            pltpu.VMEM((rows, depth), BF16),
            pltpu.VMEM(gain.shape, F32),
            pltpu.VMEM(rates.shape, F32),
            pltpu.VMEM((depth, sum(widths)), BF16),
            pltpu.SemaphoreType.DMA((9,)),
        ],
        1,
        2 * rows * depth * sum(widths),
        24,
    )(tp, *[in_hbm(a) for a in (own, gain, rates) + weights])


def keys_body(tp, x, gain, part, sq, col, *refs):
    weights = refs[:4]
    k_out, v_out, akv_out, inv_out, scaled_out, pay_out, tail_out = refs[4:]
    rows, depth = x.shape
    width = k_out.shape[1]
    begin = pl.multiple_of((1 - tp[0]) * depth, depth)
    scale = gain[:, pl.ds(begin, depth)]
    low = lane_ids((HEAD_DIM, LANES)) < HEAD_DIM
    for m in range(0, rows, CHUNK):
        here = slice(m, m + CHUNK)
        wide = x[here, :].astype(F32)
        scaled = (wide * scale).astype(BF16)
        scaled_out[here, :] = scaled
        mean = jnp.sum(sq[here, :] + squares_of(wide), axis=1, keepdims=True) / (2 * depth)
        inverse = lax.rsqrt(mean + EPS)
        inv_out[here, :] = jnp.broadcast_to(inverse, (CHUNK, LANES))
        for n in range(0, part.shape[1], CHUNK):
            columns = weight_columns(weights, begin, depth, n)
            total = part[here, n : n + CHUNK] + dot(scaled, columns)
            value = (total * inverse).astype(BF16)
            for j in range(n, n + CHUNK, LANES):
                piece = value[:, j - n : j - n + LANES]
                if j < width:
                    k_out[here, j : j + LANES] = piece * jnp.asarray(SCALE, BF16)
                elif j < 2 * width:
                    v_out[here, j - width : j - width + LANES] = piece
                else:
                    akv_out[here, j - 2 * width : j - 2 * width + LANES] = piece
    logs = jnp.zeros((LOG_ROWS, LANES), F32)
    places = row_ids((LOG_ROWS, LANES))
    for p in range(PAIRS):
        lanes = slice(p * LANES, (p + 1) * LANES)
        last = col[rows - 1 : rows, lanes]
        faded = (k_out[:, lanes].astype(F32) * jnp.exp(last - col[:, lanes])).astype(BF16)
        state = lax.dot_general(faded, v_out[:, lanes], CONTRACT_ROWS, preferred_element_type=F32)
        packed = jnp.where(low, state[0:HEAD_DIM], state[HEAD_DIM:]).astype(BF16)
        pay_out[p * HEAD_DIM : (p + 1) * HEAD_DIM, :] = packed
        for i, part3 in enumerate(split3(last)):
            logs = logs + jnp.where(places == 3 * p + i, part3, 0.0)
    pay_out[STATE_ROWS:, :] = logs.astype(BF16)
    tail_out[...] = akv_out[rows - WINDOW : rows, :]


def keys_half(tp, peer, gain, part, sq, col, weights):
    rows, depth = peer.shape
    widths = [w.shape[1] for w in weights]
    shapes = [
        ((rows, widths[0]), BF16),
        ((rows, widths[1]), BF16),
        ((rows, widths[2] + widths[3]), BF16),
        ((rows, LANES), F32),
        ((rows, depth), BF16),
        ((PAY_ROWS, LANES), BF16),
        ((WINDOW, widths[2] + widths[3]), BF16),
    ]
    return call(
        keys_body,
        [whole(a.shape) for a in (peer, gain, part, sq, col) + weights],
        [whole(s) for s, _ in shapes],
        [jax.ShapeDtypeStruct(s, t) for s, t in shapes],
        [],
        1,
        2 * rows * depth * sum(widths),
        20,
    )(tp, peer, gain, part, sq, col, *weights)


def queries_body(tp, own, peer, inv, w0, w1, q_out, aq_out):
    rows, depth = own.shape
    width = q_out.shape[1]
    begin = pl.multiple_of(tp[0] * depth, depth)
    other = pl.multiple_of((1 - tp[0]) * depth, depth)
    weights = (w0, w1)
    for m in range(0, rows, CHUNK):
        here = slice(m, m + CHUNK)
        inverse = inv[here, 0:1]
        for n in range(0, 2 * width, CHUNK):
            total = dot(own[here, :], weight_columns(weights, begin, depth, n))
            total = total + dot(peer[here, :], weight_columns(weights, other, depth, n))
            value = (total * inverse).astype(BF16)
            for j in range(n, n + CHUNK, LANES):
                piece = value[:, j - n : j - n + LANES]
                if j < width:
                    q_out[here, j : j + LANES] = piece
                else:
                    aq_out[here, j - width : j - width + LANES] = piece * jnp.asarray(SCALE, BF16)


def queries(tp, own, peer, inv, w0, w1):
    rows, depth = own.shape
    shapes = [(rows, w0.shape[1]), (rows, w1.shape[1])]
    return call(
        queries_body,
        [whole(a.shape) for a in (own, peer, inv, w0, w1)],
        [whole(s) for s in shapes],
        [jax.ShapeDtypeStruct(s, BF16) for s in shapes],
        [],
        1,
        8 * rows * depth * w0.shape[1],
        20,
    )(tp, own, peer, inv, w0, w1)


def inner_body(q_ref, k_ref, v_ref, row_ref, col_ref, out_ref):
    rows = q_ref.shape[0]
    later = row_ids((CHUNK, CHUNK)) >= lane_ids((CHUNK, CHUNK))
    low = lane_ids((CHUNK, LANES)) < HEAD_DIM
    diagonal = diagonal_mask()
    masks = [half_mask(0, BF16), half_mask(1, BF16)]
    for pair in range(PAIRS):
        lanes = slice(pair * LANES, (pair + 1) * LANES)
        state = start = None
        for begin in range(0, rows, CHUNK):
            here = slice(begin, begin + CHUNK)
            q, k, v = q_ref[here, lanes], k_ref[here, lanes], v_ref[here, lanes]
            cum = col_ref[here, lanes]
            parts = []
            for half in range(2):
                scores = lax.dot_general(
                    q * masks[half], k, CONTRACT_LANES, preferred_element_type=F32
                )
                over = cum[:, half * HEAD_DIM : half * HEAD_DIM + 1]
                keyed = row_ref[2 * pair + half : 2 * pair + half + 1, here]
                fade = jnp.exp(jnp.where(later, over - keyed, -jnp.inf))
                parts.append(dot((scores * fade).astype(BF16), v))
            out = jnp.where(low, parts[0], parts[1])
            end = col_ref[begin + CHUNK - 1 : begin + CHUNK, lanes]
            if state is not None:
                faded = (q.astype(F32) * jnp.exp(cum - start)).astype(BF16)
                out = out + dot(faded, state.astype(BF16))
            out_ref[here, lanes] = out
            if begin + CHUNK < rows:
                keyed = (k.astype(F32) * jnp.exp(end - cum)).astype(BF16)
                added = lax.dot_general(keyed, v, CONTRACT_ROWS, preferred_element_type=F32)
                added = jnp.where(diagonal, added, 0.0)
                state = added if state is None else state * jnp.exp(end - start) + added
                start = end


def inner(q, k, v, row, col):
    args = (q, k, v, row, col)
    return call(
        inner_body,
        [whole(a.shape) for a in args],
        whole(q.shape),
        jax.ShapeDtypeStruct(q.shape, F32),
        [],
        0,
        3 * 2**30,
        12,
    )(*args)


def logs_of(tile, p):
    return tile[3 * p : 3 * p + 1] + tile[3 * p + 1 : 3 * p + 2] + tile[3 * p + 2 : 3 * p + 3]


def state_of(ref, p):
    return ref[p * HEAD_DIM : (p + 1) * HEAD_DIM, :].astype(F32)


def log_tile(ref):
    return ref[STATE_ROWS:PAY_ROWS, :].astype(F32)


def write_logs(pay_out, rows):
    places = row_ids((LOG_ROWS, LANES))
    logs = jnp.zeros((LOG_ROWS, LANES), F32)
    for p, row in enumerate(rows):
        for i, part in enumerate(split3(row)):
            logs = logs + jnp.where(places == 3 * p + i, part, 0.0)
    pay_out[STATE_ROWS:, :] = logs.astype(BF16)


def line_body(place, *refs):
    y = place[0]
    sources, (before_out, log_out, pay_out) = refs[:4], refs[4:]
    tiles = [log_tile(r) for r in sources]
    spots = [(y - k + 4) % 4 for k in range(4)]
    lead = jnp.zeros((8, LANES), F32)
    totals = []
    for p in range(PAIRS):
        here = slice(p * HEAD_DIM, (p + 1) * HEAD_DIM)
        logs = [logs_of(t, p) for t in tiles]
        states = [state_of(r, p) for r in sources]
        total = before = between = None
        for k in range(4):
            after = jnp.zeros((1, LANES), F32)
            for j in range(4):
                if j != k:
                    after = after + jnp.where(spots[j] > spots[k], logs[j], 0.0)
            part = states[k] * jnp.exp(after)
            total = part if total is None else total + part
            if k > 0:
                part = jnp.where(k <= y, states[k], 0.0)
                part = part if between is None else part * jnp.exp(between)
                before = part if before is None else before + part
                rate = jnp.where(k <= y, logs[k], 0.0)
                between = rate if between is None else between + rate
        before_out[here, :] = before
        lead = lead + jnp.where(row_ids((8, LANES)) == p, between, 0.0)
        pay_out[here, :] = total.astype(BF16)
        totals.append(logs[0] + logs[1] + logs[2] + logs[3])
    log_out[...] = lead
    write_logs(pay_out, totals)


def column_body(place, own, back, ahead, before_out, log_out, pay_out):
    z = place[0]
    last = z == 7
    tiles = [log_tile(r) for r in (own, back, ahead)]
    lead = jnp.zeros((8, LANES), F32)
    totals = []
    for p in range(PAIRS):
        here = slice(p * HEAD_DIM, (p + 1) * HEAD_DIM)
        log, log_back, log_ahead = [logs_of(t, p) for t in tiles]
        before = jnp.where(z >= 1, state_of(back, p), 0.0)
        rate = jnp.where(z >= 1, log_back, 0.0)
        before_out[here, :] = before
        lead = lead + jnp.where(row_ids((8, LANES)) == p, rate, 0.0)
        inner_part = jnp.where(last, 0.0, state_of(own, p) + jnp.exp(log) * before)
        pay_out[here, :] = (state_of(ahead, p) + jnp.exp(log_ahead) * inner_part).astype(BF16)
        totals.append(log_ahead + jnp.where(last, 0.0, log + rate))
    log_out[...] = lead
    write_logs(pay_out, totals)


def scan_step(body, place, sources):
    return call(
        body,
        [whole(a.shape) for a in sources],
        [whole((STATE_ROWS, LANES)), whole((8, LANES)), whole((PAY_ROWS, LANES))],
        [
            jax.ShapeDtypeStruct((STATE_ROWS, LANES), F32),
            jax.ShapeDtypeStruct((8, LANES), F32),
            jax.ShapeDtypeStruct((PAY_ROWS, LANES), BF16),
        ],
        [],
        1,
        2**26,
        4,
    )(place, *sources)


def finish_body(side, row, q_ref, in_ref, col_ref, gain, *refs):
    line, line_log, column, column_log, three, six, out_ref = refs
    z = row[0]
    tile3, tile6 = log_tile(three), log_tile(six)
    diagonal = diagonal_mask()
    ones = jnp.where(diagonal, 1.0, 0.0).astype(BF16)
    for p in range(PAIRS):
        here = slice(p * HEAD_DIM, (p + 1) * HEAD_DIM)
        lanes = slice(p * LANES, (p + 1) * LANES)
        far = jnp.where(z >= 2, state_of(three, p), 0.0)
        rate = jnp.where(z >= 2, logs_of(tile3, p), 0.0)
        far = far + jnp.exp(rate) * jnp.where(z >= 5, state_of(six, p), 0.0)
        before = column[here, :] + jnp.exp(column_log[p : p + 1, :]) * far
        before = line[here, :] + jnp.exp(line_log[p : p + 1, :]) * before
        state = jnp.where(diagonal, jnp.concatenate([before, before], axis=0), 0.0).astype(BF16)
        carried = dot(q_ref[:, lanes], state) * jnp.exp(col_ref[:, lanes])
        retained = in_ref[:, lanes] + carried
        squares = retained * retained
        high = squares.astype(BF16)
        rest = (squares - high.astype(F32)).astype(BF16)
        mean = (dot(high, ones) + dot(rest, ones)) / HEAD_DIM
        out_ref[:, lanes] = (
            retained * lax.rsqrt(mean + EPS) * gain[lanes].reshape(1, LANES)
        ).astype(BF16)


def finish(mine, side, row, q, inside, col, gain, small):
    rows, width = q.shape
    spec = pl.BlockSpec((rows // 2, width), lambda i, t, z: (half_of(t, mine), 0))
    return call(
        finish_body,
        [spec, spec, spec, whole(gain.shape)] + [whole(s.shape) for s in small],
        whole((rows // 2, width)),
        jax.ShapeDtypeStruct((rows // 2, width), BF16),
        [],
        2,
        2**29,
        8,
    )(side, row, q, inside, col, gain, *small)


def half_of(side, mine):
    return side[0] if mine else 1 - side[0]


def window_body(mine, side, spot, q_ref, kv_ref, halo_ref, sink_ref, out_ref, ext):
    half, first = half_of(side, mine), spot[0]
    rows = q_ref.shape[0]
    begin = pl.multiple_of(half * rows, WINDOW)

    @pl.when(half == 0)
    def _():
        ext[0:WINDOW, :] = halo_ref[...]

    @pl.when(half == 1)
    def _():
        ext[0:WINDOW, :] = kv_ref[rows - WINDOW : rows, :]

    ext[WINDOW:, :] = kv_ref[pl.ds(begin, rows), :]
    masks = [half_mask(0, BF16), half_mask(1, BF16)]
    heads = q_ref.shape[1] // HEAD_DIM
    group = heads // 2
    band = (2 * WINDOW, group * WINDOW)
    place = lane_ids(band) % WINDOW
    distance = WINDOW + place - row_ids(band)
    near = (distance >= 0) & (distance < WINDOW)
    spot = lane_ids((1, group * WINDOW)) // WINDOW
    for block in range(rows // WINDOW):
        span = slice(block * WINDOW, (block + 2) * WINDOW)
        keys, values = ext[span, 0:LANES], ext[span, LANES:]
        allowed = near
        if block == 0:
            behind_rows = jnp.where((half == 0) & (first == 0), WINDOW, 0)
            allowed = near & (row_ids(band) >= behind_rows)
        here = slice(block * WINDOW, (block + 1) * WINDOW)
        outs = []
        for g in range(2):
            stack = []
            sink = jnp.zeros((1, group * WINDOW), F32)
            for j in range(group):
                h = g * group + j
                q = q_ref[here, h // 2 * LANES : (h // 2 + 1) * LANES]
                if h % 2 != g:
                    q = pltpu.roll(q.astype(F32), HEAD_DIM, 1).astype(BF16)
                stack.append(q * masks[g])
                sink = sink + jnp.where(spot == j, sink_ref[h], 0.0)
            scores = lax.dot_general(
                keys, jnp.concatenate(stack, axis=0), CONTRACT_LANES, preferred_element_type=F32
            )
            scores = jnp.where(allowed, scores, -jnp.inf)
            highest = jnp.maximum(jnp.max(scores, axis=0, keepdims=True), sink)
            raised = jnp.exp(scores - highest)
            total = jnp.sum(raised, axis=0, keepdims=True) + jnp.exp(sink - highest)
            weights = (raised * (1.0 / total)).astype(BF16)
            out = lax.dot_general(values, weights, CONTRACT_ROWS, preferred_element_type=F32)
            out = out[g * HEAD_DIM : (g + 1) * HEAD_DIM]
            outs += [out[:, j * WINDOW : (j + 1) * WINDOW] for j in range(group)]
        for p in range(heads // 2):
            both = jnp.concatenate([outs[2 * p], outs[2 * p + 1]], axis=0)
            out_ref[here, p * LANES : (p + 1) * LANES] = both.T.astype(BF16)


def window(mine, side, spot, q, kv, halo, sinks):
    rows, width = q.shape
    return call(
        functools.partial(window_body, mine),
        [
            pl.BlockSpec((rows // 2, width), lambda i, t, f: (half_of(t, mine), 0)),
            whole(kv.shape),
            whole(halo.shape),
            pl.BlockSpec(memory_space=pltpu.SMEM),
        ],
        whole((rows // 2, width)),
        jax.ShapeDtypeStruct((rows // 2, width), BF16),
        [pltpu.VMEM((rows // 2 + WINDOW, kv.shape[1]), BF16)],
        2,
        2**30,
        8,
    )(side, spot, q, kv, halo, sinks)


def first_exit_body(a, b, wa, wb, out):
    rows = jnp.concatenate([a[...], b[...]], axis=1)
    for n in range(0, out.shape[1], CHUNK):
        here = slice(n, n + CHUNK)
        out[:, here] = dot(rows, jnp.concatenate([wa[:, here], wb[:, here]], axis=0))


def own_exit_body(a, w, more, out):
    for n in range(0, out.shape[1], CHUNK):
        here = slice(n, n + CHUNK)
        out[:, here] = more[:, here] + dot(a[...], w[:, here])


def last_exit_body(a, w, more, out, buffer, sems):
    copies = []
    for i, n in enumerate(range(0, out.shape[1], CHUNK)):
        here = slice(n, n + CHUNK)
        buffer[:, here] = (more[:, here] + dot(a[...], w[:, here])).astype(BF16)
        copy = pltpu.make_async_copy(buffer.at[:, here], out.at[:, here], sems.at[i])
        copy.start()
        copies.append(copy)
    for copy in copies:
        copy.wait()


def first_exit(a, b, wa, wb):
    args = (a, b, wa, wb)
    shape = (a.shape[0], wa.shape[1])
    return call(
        first_exit_body,
        [whole(x.shape) for x in args],
        whole(shape),
        jax.ShapeDtypeStruct(shape, F32),
        [],
        0,
        4 * a.shape[0] * a.shape[1] * wa.shape[1],
        12,
    )(*args)


def own_exit(a, w, more):
    args = (a, w, more)
    return call(
        own_exit_body,
        [whole(x.shape) for x in args],
        whole(more.shape),
        jax.ShapeDtypeStruct(more.shape, F32),
        [],
        0,
        2 * a.shape[0] * a.shape[1] * w.shape[1],
        12,
    )(*args)


def last_exit(a, w, more):
    args = (a, w, more)
    shape = (a.shape[0], w.shape[1])
    return call(
        last_exit_body,
        [whole(x.shape) for x in args],
        IN_HBM,
        jax.ShapeDtypeStruct(shape, BF16),
        [pltpu.VMEM(shape, BF16), pltpu.SemaphoreType.DMA((shape[1] // CHUNK,))],
        0,
        2 * a.shape[0] * a.shape[1] * w.shape[1],
        14,
    )(*args)


def turned(value, axis, by):
    peers = lax.axis_size(axis)
    return lax.ppermute(value, axis, [(i, (i + by) % peers) for i in range(peers)])


def shards(
    tokens,
    in_gain,
    ret_query,
    ret_key,
    ret_value,
    att_query,
    att_key,
    att_value,
    log_decay,
    ret_gain,
    sink_logit,
    retentive_exit_matrix,
    out_att,
):
    tp = lax.axis_index("tp").astype(jnp.int32)
    y = lax.axis_index("sp_1").astype(jnp.int32)
    z = lax.axis_index("sp_0").astype(jnp.int32)
    side, spot, row = tp.reshape(1), lax.axis_index(SP).astype(jnp.int32).reshape(1), z.reshape(1)
    side, spot, row, line_spot = lax.optimization_barrier((side, spot, row, y.reshape(1)))
    own = tokens[0]
    gain = in_gain[None]
    peer = turned(own, "tp", 1)
    early = (ret_key, ret_value, att_key, att_value)
    rates = log_decay.reshape(log_decay.shape[1], 1, log_decay.shape[2])
    first, scaled_own, squares, row_cum, col = own_half(side, own, gain, rates, early)
    ret_k, ret_v, att_kv, inv, scaled, payload, tail = keys_half(
        side, peer, gain, first, squares, col, early
    )
    sources = [payload] + [turned(payload, "sp_1", k) for k in (1, 2, 3)]
    peers = lax.axis_size(SP)
    halo = lax.ppermute(tail, SP, [(i, (i + 1) % peers) for i in range(peers)])
    ret_q, att_q = queries(side, scaled_own, scaled, inv, ret_query, att_query)
    sources, ret_q = lax.optimization_barrier((sources, ret_q))
    line, line_log, span = scan_step(line_body, line_spot, sources)
    sources = [span, turned(span, "sp_0", 1), turned(span, "sp_0", 7)]
    side, span = lax.optimization_barrier((side, span))
    theirs = window(False, side, spot, att_q, att_kv, halo, sink_logit)
    exit_own, out_own, sources[0] = lax.optimization_barrier(
        (retentive_exit_matrix, out_att, sources[0])
    )
    out_peer = turned(out_own, "tp", 1)
    exit_peer = turned(exit_own, "tp", 1)
    sources, theirs = lax.optimization_barrier((sources, theirs))
    att_got = turned(theirs, "tp", 1)
    column, column_log, span = scan_step(column_body, row, sources)
    sources = [turned(span, "sp_0", 3), turned(span, "sp_0", 6)]
    side, row, span = lax.optimization_barrier((side, row, span))
    att_mine = window(True, side, spot, att_q, att_kv, halo, sink_logit)
    ret_q, row = lax.optimization_barrier((ret_q, row))
    inside = inner(ret_q, ret_k, ret_v, row_cum, col)
    partial = first_exit(att_mine, att_got, out_att, out_peer)
    sources, partial, inside = lax.optimization_barrier((sources, partial, inside))
    small = [line, line_log, column, column_log] + sources
    args = (side, row, ret_q, inside, col, ret_gain, small)
    ret_got = turned(finish(False, *args), "tp", 1)
    ret_mine = finish(True, *args)
    partial = own_exit(ret_mine, retentive_exit_matrix, partial)
    mixed = last_exit(ret_got, exit_peer, partial)
    return mixed[None]


def solution(mesh):
    finer = Mesh(
        mesh.devices.reshape(8, 4, mesh.shape["fs"], mesh.shape["tp"]), ("sp_0", "sp_1", "fs", "tp")
    )
    placed = (
        P("fs", SP, "tp"),
        P(),
        P(None, "tp"),
        P(None, "tp"),
        P(None, "tp"),
        P(None, "tp"),
        P(None, "tp"),
        P(None, "tp"),
        P("fs", "tp", SP),
        P("tp"),
        P("tp"),
        P("tp", None),
        P("tp", None),
    )
    return jax.shard_map(
        shards, mesh=finer, in_specs=placed, out_specs=P("fs", SP_TP, None), check_vma=False
    )
```

```python
import functools

import jax
import jax.numpy as jnp
from jax import lax
from jax.experimental import pallas as pl
from jax.experimental.pallas import tpu as pltpu
from jax.sharding import Mesh
from jax.sharding import PartitionSpec as P


HEAD_DIM = 64
WINDOW = 128
EPS = 1e-06
SP = ("sp_0", "sp_1")
SP_TP = ("sp_0", "sp_1", "tp")
F32 = jnp.float32
BF16 = jnp.bfloat16
CHUNK = 256
STATE_ROWS = 192
LOG_ROWS = 16
PAY_ROWS = STATE_ROWS + LOG_ROWS
PAIRS = 3
LANES = 128
CONTRACT_ROWS = (((0,), (0,)), ((), ()))
CONTRACT_LANES = (((1,), (1,)), ((), ()))


def dot(a, b):
    return jnp.dot(a, b, preferred_element_type=F32)


def lane_ids(shape):
    return lax.broadcasted_iota(jnp.int32, shape, len(shape) - 1)


def row_ids(shape):
    return lax.broadcasted_iota(jnp.int32, shape, 0)


def half_mask(half, dtype):
    lanes = lane_ids((1, LANES))
    inside = (lanes < HEAD_DIM) if half == 0 else (lanes >= HEAD_DIM)
    return jnp.where(inside, 1.0, 0.0).astype(dtype)


def diagonal_mask():
    return (row_ids((LANES, LANES)) < HEAD_DIM) == (lane_ids((LANES, LANES)) < HEAD_DIM)


def split3(x):
    high = x.astype(BF16).astype(F32)
    rest = x - high
    middle = rest.astype(BF16).astype(F32)
    return high, middle, rest - middle


def call(body, in_specs, out_specs, out_shape, scratch, scalars, flops, mib, grid=(1,)):
    return pl.pallas_call(
        body,
        out_shape=out_shape,
        grid_spec=pltpu.PrefetchScalarGridSpec(
            num_scalar_prefetch=scalars,
            grid=grid,
            in_specs=in_specs,
            out_specs=out_specs,
            scratch_shapes=scratch,
        ),
        compiler_params=pltpu.CompilerParams(
            dimension_semantics=("arbitrary",) * len(grid), vmem_limit_bytes=mib * 2**20
        ),
        cost_estimate=pl.CostEstimate(flops=flops, transcendentals=0, bytes_accessed=1 << 20),
    )


def whole(shape):
    return pl.BlockSpec(shape, lambda *_: (0,) * len(shape))


IN_HBM = pl.BlockSpec(memory_space=pltpu.HBM)
SCALE = HEAD_DIM**-0.5


def in_hbm(x):
    return pltpu.with_memory_space_constraint(x, pltpu.HBM)


def fetch_weights(weights, buffer, sems, begin):
    copies, start = [], 0
    depth = buffer.shape[0]
    for i, w in enumerate(weights):
        stop = start + w.shape[1]
        copy = pltpu.make_async_copy(
            w.at[pl.ds(begin, depth), :], buffer.at[:, start:stop], sems.at[i]
        )
        copy.start()
        copies.append(copy)
        start = stop
    return copies


def weight_columns(weights, begin, depth, start):
    pieces, left = [], 0
    for w in weights:
        for n in range(0, w.shape[1], LANES):
            if start <= left + n < start + CHUNK:
                pieces.append(w[pl.ds(begin, depth), n : n + LANES])
        left += w.shape[1]
    return jnp.concatenate(pieces, axis=1)


def squares_of(wide):
    squares = wide * wide
    total = squares[:, 0:LANES]
    for start in range(LANES, wide.shape[1], LANES):
        total = total + squares[:, start : start + LANES]
    return total


def decays(rates_ref, row_ref, col_ref, wide_ref):
    heads, _, rows = rates_ref.shape
    row_ref[...] = jnp.zeros_like(row_ref)
    for h in range(heads):
        row_ref[h : h + 1, :] = rates_ref[h]
    total = row_ref[...]
    lanes = lane_ids(total.shape)
    step = 1
    while step < rows:
        total = total + jnp.where(lanes >= step, pltpu.roll(total, step, 1), 0.0)
        step *= 2
    row_ref[...] = total
    parts = jnp.concatenate(split3(total) + (jnp.zeros_like(total),), axis=0).astype(BF16)
    for ref, lanes in ((col_ref, HEAD_DIM), (wide_ref, LANES)):
        shape = (32, heads * lanes)
        picks = (row_ids(shape) % 8 == lane_ids(shape) // lanes).astype(F32).astype(BF16)
        ref[...] = lax.dot_general(parts, picks, CONTRACT_ROWS, preferred_element_type=F32)


def own_body(tp, x_hbm, gain_hbm, rates_hbm, *refs):
    weights = refs[:4]
    first, scaled, sq, row, col, wide_col, later, xbuf, gain, rates, wbuf, sems = refs[4:]
    rows, depth = xbuf.shape
    small = pltpu.make_async_copy(rates_hbm, rates, sems.at[8])
    small.start()
    load = pltpu.make_async_copy(x_hbm, xbuf, sems.at[6])
    load.start()
    gains = pltpu.make_async_copy(gain_hbm, gain, sems.at[7])
    gains.start()
    begin = pl.multiple_of(tp[0] * depth, depth)
    copies = fetch_weights(weights, wbuf, sems, begin)
    other = pl.multiple_of((1 - tp[0]) * depth, depth)
    more = fetch_weights(weights, later, sems.at[pl.ds(9, 4)], other)
    small.wait()
    decays(rates, row, col, wide_col)
    gains.wait()
    load.wait()
    for copy in copies:
        copy.wait()
    scale = gain[:, pl.ds(begin, depth)]
    for m in range(0, rows, CHUNK):
        here = slice(m, m + CHUNK)
        wide = xbuf[here, :].astype(F32)
        part = (wide * scale).astype(BF16)
        scaled[here, :] = part
        sq[here, :] = squares_of(wide)
        for n in range(0, first.shape[1], CHUNK):
            first[here, n : n + CHUNK] = dot(part, wbuf[:, n : n + CHUNK])
    for copy in more:
        copy.wait()


def own_half(tp, own, gain, rates, weights):
    rows, depth = own.shape
    widths = [w.shape[1] for w in weights]
    shapes = [
        ((rows, sum(widths)), F32),
        ((rows, depth), BF16),
        ((rows, LANES), F32),
        ((8, rows), F32),
        ((rows, widths[0]), F32),
        ((rows, 2 * widths[0]), F32),
        ((depth, sum(widths)), BF16),
    ]
    return call(
        own_body,
        [IN_HBM] * 7,
        [whole(s) for s, _ in shapes],
        [jax.ShapeDtypeStruct(s, t) for s, t in shapes],
        [
            pltpu.VMEM((rows, depth), BF16),
            pltpu.VMEM(gain.shape, F32),
            pltpu.VMEM(rates.shape, F32),
            pltpu.VMEM((depth, sum(widths)), BF16),
            pltpu.SemaphoreType.DMA((13,)),
        ],
        1,
        2 * rows * depth * sum(widths),
        24,
    )(tp, *[in_hbm(a) for a in (own, gain, rates) + weights])


def keys_body(tp, x, gain, part, sq, col, wbuf, *refs):
    k_out, v_out, akv_out, inv_out, scaled_out, pay_out, tail_out = refs
    rows, depth = x.shape
    width = k_out.shape[1]
    begin = pl.multiple_of((1 - tp[0]) * depth, depth)
    scale = gain[:, pl.ds(begin, depth)]
    low = lane_ids((HEAD_DIM, LANES)) < HEAD_DIM
    for m in range(0, rows, CHUNK):
        here = slice(m, m + CHUNK)
        wide = x[here, :].astype(F32)
        scaled = (wide * scale).astype(BF16)
        scaled_out[here, :] = scaled
        mean = jnp.sum(sq[here, :] + squares_of(wide), axis=1, keepdims=True) / (2 * depth)
        inverse = lax.rsqrt(mean + EPS)
        inv_out[here, :] = jnp.broadcast_to(inverse, (CHUNK, LANES))
        for n in range(0, part.shape[1], CHUNK):
            total = part[here, n : n + CHUNK] + dot(scaled, wbuf[:, n : n + CHUNK])
            value = (total * inverse).astype(BF16)
            for j in range(n, n + CHUNK, LANES):
                piece = value[:, j - n : j - n + LANES]
                if j < width:
                    k_out[here, j : j + LANES] = piece * jnp.asarray(SCALE, BF16)
                elif j < 2 * width:
                    v_out[here, j - width : j - width + LANES] = piece
                else:
                    akv_out[here, j - 2 * width : j - 2 * width + LANES] = piece
    logs = jnp.zeros((LOG_ROWS, LANES), F32)
    places = row_ids((LOG_ROWS, LANES))
    for p in range(PAIRS):
        lanes = slice(p * LANES, (p + 1) * LANES)
        last = col[rows - 1 : rows, lanes]
        faded = (k_out[:, lanes].astype(F32) * jnp.exp(last - col[:, lanes])).astype(BF16)
        state = lax.dot_general(faded, v_out[:, lanes], CONTRACT_ROWS, preferred_element_type=F32)
        packed = jnp.where(low, state[0:HEAD_DIM], state[HEAD_DIM:]).astype(BF16)
        pay_out[p * HEAD_DIM : (p + 1) * HEAD_DIM, :] = packed
        for i, part3 in enumerate(split3(last)):
            logs = logs + jnp.where(places == 3 * p + i, part3, 0.0)
    pay_out[STATE_ROWS:, :] = logs.astype(BF16)
    tail_out[...] = akv_out[rows - WINDOW : rows, :]


def keys_half(tp, peer, gain, part, sq, col, wbuf, width):
    rows, depth = peer.shape
    shapes = [
        ((rows, width), BF16),
        ((rows, width), BF16),
        ((rows, wbuf.shape[1] - 2 * width), BF16),
        ((rows, LANES), F32),
        ((rows, depth), BF16),
        ((PAY_ROWS, LANES), BF16),
        ((WINDOW, wbuf.shape[1] - 2 * width), BF16),
    ]
    return call(
        keys_body,
        [whole(a.shape) for a in (peer, gain, part, sq, col, wbuf)],
        [whole(s) for s, _ in shapes],
        [jax.ShapeDtypeStruct(s, t) for s, t in shapes],
        [],
        1,
        2 * rows * depth * wbuf.shape[1],
        20,
    )(tp, peer, gain, part, sq, col, wbuf)


def queries_body(tp, own, peer, inv, w0, w1, q_out, aq_out):
    rows, depth = own.shape
    width = q_out.shape[1]
    begin = pl.multiple_of(tp[0] * depth, depth)
    other = pl.multiple_of((1 - tp[0]) * depth, depth)
    weights = (w0, w1)
    for m in range(0, rows, CHUNK):
        here = slice(m, m + CHUNK)
        inverse = inv[here, 0:1]
        for n in range(0, 2 * width, CHUNK):
            total = dot(own[here, :], weight_columns(weights, begin, depth, n))
            total = total + dot(peer[here, :], weight_columns(weights, other, depth, n))
            value = (total * inverse).astype(BF16)
            for j in range(n, n + CHUNK, LANES):
                piece = value[:, j - n : j - n + LANES]
                if j < width:
                    q_out[here, j : j + LANES] = piece
                else:
                    aq_out[here, j - width : j - width + LANES] = piece * jnp.asarray(SCALE, BF16)


def queries(tp, own, peer, inv, w0, w1):
    rows, depth = own.shape
    shapes = [(rows, w0.shape[1]), (rows, w1.shape[1])]
    return call(
        queries_body,
        [whole(a.shape) for a in (own, peer, inv, w0, w1)],
        [whole(s) for s in shapes],
        [jax.ShapeDtypeStruct(s, BF16) for s in shapes],
        [],
        1,
        8 * rows * depth * w0.shape[1],
        20,
    )(tp, own, peer, inv, w0, w1)


def inner_body(q_ref, k_ref, v_ref, row_ref, col_ref, wide_ref, out_ref):
    rows = q_ref.shape[0]
    size = 256
    later = row_ids((size, size)) >= lane_ids((size, size))
    diagonal = diagonal_mask()
    masks = [half_mask(0, BF16), half_mask(1, BF16)]
    states = [None] * PAIRS
    for begin in range(0, rows, size):
        here = slice(begin, begin + size)
        last = slice(begin + size - 1, begin + size)
        for pair in range(PAIRS):
            lanes = slice(pair * LANES, (pair + 1) * LANES)
            q, k, v = q_ref[here, lanes], k_ref[here, lanes], v_ref[here, lanes]
            cum = col_ref[here, lanes]
            end = col_ref[last, lanes]
            start = col_ref[begin - 1 : begin, lanes] if begin else None
            both = jnp.concatenate([q * masks[0], q * masks[1]], axis=0)
            scores = lax.dot_general(both, k, CONTRACT_LANES, preferred_element_type=F32)
            weights = []
            for half in range(2):
                head = 2 * pair + half
                over = wide_ref[here, head * LANES : (head + 1) * LANES]
                over = jnp.concatenate([over] * (size // LANES), axis=1)
                fade = jnp.exp(jnp.where(later, over - row_ref[head : head + 1, here], -jnp.inf))
                part = scores[half * size : (half + 1) * size]
                weights.append((part * fade).astype(BF16))
            values = jnp.concatenate([v * masks[0], v * masks[1]], axis=0)
            out = dot(jnp.concatenate(weights, axis=1), values)
            if begin:
                faded = (q.astype(F32) * jnp.exp(cum - start)).astype(BF16)
                out = out + dot(faded, states[pair].astype(BF16))
            out_ref[here, lanes] = out
            if begin + size < rows:
                keyed = (k.astype(F32) * jnp.exp(end - cum)).astype(BF16)
                added = lax.dot_general(keyed, v, CONTRACT_ROWS, preferred_element_type=F32)
                added = jnp.where(diagonal, added, 0.0)
                states[pair] = states[pair] * jnp.exp(end - start) + added if begin else added


def inner(q, k, v, row, col, wide):
    args = (q, k, v, row, col, wide)
    return call(
        inner_body,
        [whole(a.shape) for a in args],
        whole(q.shape),
        jax.ShapeDtypeStruct(q.shape, F32),
        [],
        0,
        3 * 2**30,
        12,
    )(*args)


def logs_of(tile, p):
    return tile[3 * p : 3 * p + 1] + tile[3 * p + 1 : 3 * p + 2] + tile[3 * p + 2 : 3 * p + 3]


def state_of(ref, p):
    return ref[p * HEAD_DIM : (p + 1) * HEAD_DIM, :].astype(F32)


def log_tile(ref):
    return ref[STATE_ROWS:PAY_ROWS, :].astype(F32)


def write_logs(pay_out, rows):
    places = row_ids((LOG_ROWS, LANES))
    logs = jnp.zeros((LOG_ROWS, LANES), F32)
    for p, row in enumerate(rows):
        for i, part in enumerate(split3(row)):
            logs = logs + jnp.where(places == 3 * p + i, part, 0.0)
    pay_out[STATE_ROWS:, :] = logs.astype(BF16)


def line_body(place, *refs):
    y = place[0]
    sources, (before_out, log_out, pay_out) = refs[:4], refs[4:]
    tiles = [log_tile(r) for r in sources]
    spots = [(y - k + 4) % 4 for k in range(4)]
    lead = jnp.zeros((8, LANES), F32)
    totals = []
    for p in range(PAIRS):
        here = slice(p * HEAD_DIM, (p + 1) * HEAD_DIM)
        logs = [logs_of(t, p) for t in tiles]
        states = [state_of(r, p) for r in sources]
        total = before = between = None
        for k in range(4):
            after = jnp.zeros((1, LANES), F32)
            for j in range(4):
                if j != k:
                    after = after + jnp.where(spots[j] > spots[k], logs[j], 0.0)
            part = states[k] * jnp.exp(after)
            total = part if total is None else total + part
            if k > 0:
                part = jnp.where(k <= y, states[k], 0.0)
                part = part if between is None else part * jnp.exp(between)
                before = part if before is None else before + part
                rate = jnp.where(k <= y, logs[k], 0.0)
                between = rate if between is None else between + rate
        before_out[here, :] = before
        lead = lead + jnp.where(row_ids((8, LANES)) == p, between, 0.0)
        pay_out[here, :] = total.astype(BF16)
        totals.append(logs[0] + logs[1] + logs[2] + logs[3])
    log_out[...] = lead
    write_logs(pay_out, totals)


def column_body(place, own, back, ahead, before_out, log_out, pay_out):
    z = place[0]
    last = z == 7
    tiles = [log_tile(r) for r in (own, back, ahead)]
    lead = jnp.zeros((8, LANES), F32)
    totals = []
    for p in range(PAIRS):
        here = slice(p * HEAD_DIM, (p + 1) * HEAD_DIM)
        log, log_back, log_ahead = [logs_of(t, p) for t in tiles]
        before = jnp.where(z >= 1, state_of(back, p), 0.0)
        rate = jnp.where(z >= 1, log_back, 0.0)
        before_out[here, :] = before
        lead = lead + jnp.where(row_ids((8, LANES)) == p, rate, 0.0)
        inner_part = jnp.where(last, 0.0, state_of(own, p) + jnp.exp(log) * before)
        pay_out[here, :] = (state_of(ahead, p) + jnp.exp(log_ahead) * inner_part).astype(BF16)
        totals.append(log_ahead + jnp.where(last, 0.0, log + rate))
    log_out[...] = lead
    write_logs(pay_out, totals)


def scan_step(body, place, sources):
    return call(
        body,
        [whole(a.shape) for a in sources],
        [whole((STATE_ROWS, LANES)), whole((8, LANES)), whole((PAY_ROWS, LANES))],
        [
            jax.ShapeDtypeStruct((STATE_ROWS, LANES), F32),
            jax.ShapeDtypeStruct((8, LANES), F32),
            jax.ShapeDtypeStruct((PAY_ROWS, LANES), BF16),
        ],
        [],
        1,
        2**26,
        4,
    )(place, *sources)


def finish_body(side, row, q_ref, in_ref, col_ref, gain, *refs):
    line, line_log, column, column_log, three, six, out_ref = refs
    z = row[0]
    tile3, tile6 = log_tile(three), log_tile(six)
    diagonal = diagonal_mask()
    ones = jnp.where(diagonal, 1.0, 0.0).astype(BF16)
    for p in range(PAIRS):
        here = slice(p * HEAD_DIM, (p + 1) * HEAD_DIM)
        lanes = slice(p * LANES, (p + 1) * LANES)
        far = jnp.where(z >= 2, state_of(three, p), 0.0)
        rate = jnp.where(z >= 2, logs_of(tile3, p), 0.0)
        far = far + jnp.exp(rate) * jnp.where(z >= 5, state_of(six, p), 0.0)
        before = column[here, :] + jnp.exp(column_log[p : p + 1, :]) * far
        before = line[here, :] + jnp.exp(line_log[p : p + 1, :]) * before
        state = jnp.where(diagonal, jnp.concatenate([before, before], axis=0), 0.0).astype(BF16)
        carried = dot(q_ref[:, lanes], state) * jnp.exp(col_ref[:, lanes])
        retained = in_ref[:, lanes] + carried
        squares = retained * retained
        high = squares.astype(BF16)
        rest = (squares - high.astype(F32)).astype(BF16)
        mean = (dot(high, ones) + dot(rest, ones)) / HEAD_DIM
        out_ref[:, lanes] = (
            retained * lax.rsqrt(mean + EPS) * gain[lanes].reshape(1, LANES)
        ).astype(BF16)


def finish(mine, side, row, q, inside, col, gain, small):
    rows, width = q.shape
    spec = pl.BlockSpec((rows // 2, width), lambda i, t, z: (half_of(t, mine), 0))
    return call(
        finish_body,
        [spec, spec, spec, whole(gain.shape)] + [whole(s.shape) for s in small],
        whole((rows // 2, width)),
        jax.ShapeDtypeStruct((rows // 2, width), BF16),
        [],
        2,
        2**29,
        8,
    )(side, row, q, inside, col, gain, *small)


def half_of(side, mine):
    return side[0] if mine else 1 - side[0]


def window_body(mine, side, spot, q_ref, kv_ref, halo_ref, sink_ref, out_ref, ext):
    half, first = half_of(side, mine), spot[0]
    rows = q_ref.shape[0]
    begin = pl.multiple_of(half * rows, WINDOW)

    @pl.when(half == 0)
    def _():
        ext[0:WINDOW, :] = halo_ref[...]

    @pl.when(half == 1)
    def _():
        ext[0:WINDOW, :] = kv_ref[rows - WINDOW : rows, :]

    ext[WINDOW:, :] = kv_ref[pl.ds(begin, rows), :]
    masks = [half_mask(0, BF16), half_mask(1, BF16)]
    heads = q_ref.shape[1] // HEAD_DIM
    group = heads // 2
    band = (WINDOW, group * WINDOW)
    upper = row_ids(band) > lane_ids(band) % WINDOW
    empty = jnp.where((half == 0) & (first == 0), -jnp.inf, 0.0)
    spot = lane_ids((1, group * WINDOW)) // WINDOW
    for block in range(rows // WINDOW):
        span = slice(block * WINDOW, (block + 2) * WINDOW)
        keys, values = ext[span, 0:LANES], ext[span, LANES:]
        here = slice(block * WINDOW, (block + 1) * WINDOW)
        outs = []
        for g in range(2):
            stack = []
            sink = jnp.zeros((1, group * WINDOW), F32)
            for j in range(group):
                h = g * group + j
                q = q_ref[here, h // 2 * LANES : (h // 2 + 1) * LANES]
                if h % 2 != g:
                    q = pltpu.roll(q.astype(F32), HEAD_DIM, 1).astype(BF16)
                stack.append(q * masks[g])
                sink = sink + jnp.where(spot == j, sink_ref[h], 0.0)
            scores = lax.dot_general(
                keys, jnp.concatenate(stack, axis=0), CONTRACT_LANES, preferred_element_type=F32
            )
            back = scores[0:WINDOW] + empty if block == 0 else scores[0:WINDOW]
            scores = jnp.where(upper, back, scores[WINDOW:])
            highest = jnp.maximum(jnp.max(scores, axis=0, keepdims=True), sink)
            raised = jnp.exp(scores - highest)
            total = jnp.sum(raised, axis=0, keepdims=True) + jnp.exp(sink - highest)
            weights = jnp.concatenate(
                [jnp.where(upper, raised, 0.0), jnp.where(upper, 0.0, raised)], axis=0
            ).astype(BF16)
            out = lax.dot_general(values, weights, CONTRACT_ROWS, preferred_element_type=F32)
            out = out[g * HEAD_DIM : (g + 1) * HEAD_DIM] * (1.0 / total)
            outs += [out[:, j * WINDOW : (j + 1) * WINDOW] for j in range(group)]
        for p in range(heads // 2):
            both = jnp.concatenate([outs[2 * p], outs[2 * p + 1]], axis=0)
            out_ref[here, p * LANES : (p + 1) * LANES] = both.T.astype(BF16)


def window(mine, side, spot, q, kv, halo, sinks):
    rows, width = q.shape
    return call(
        functools.partial(window_body, mine),
        [
            pl.BlockSpec((rows // 2, width), lambda i, t, f: (half_of(t, mine), 0)),
            whole(kv.shape),
            whole(halo.shape),
            pl.BlockSpec(memory_space=pltpu.SMEM),
        ],
        whole((rows // 2, width)),
        jax.ShapeDtypeStruct((rows // 2, width), BF16),
        [pltpu.VMEM((rows // 2 + WINDOW, kv.shape[1]), BF16)],
        2,
        2**30,
        8,
    )(side, spot, q, kv, halo, sinks)


def first_exit_body(a, b, wa, wb, out):
    rows = jnp.concatenate([a[...], b[...]], axis=1)
    for n in range(0, out.shape[1], CHUNK):
        here = slice(n, n + CHUNK)
        out[:, here] = dot(rows, jnp.concatenate([wa[:, here], wb[:, here]], axis=0))


def own_exit_body(a, w, more, out):
    for n in range(0, out.shape[1], CHUNK):
        here = slice(n, n + CHUNK)
        out[:, here] = more[:, here] + dot(a[...], w[:, here])


def last_exit_body(a, w, more, out, buffer, sems):
    copies = []
    for i, n in enumerate(range(0, out.shape[1], CHUNK)):
        here = slice(n, n + CHUNK)
        buffer[:, here] = (more[:, here] + dot(a[...], w[:, here])).astype(BF16)
        copy = pltpu.make_async_copy(buffer.at[:, here], out.at[:, here], sems.at[i])
        copy.start()
        copies.append(copy)
    for copy in copies:
        copy.wait()


def first_exit(a, b, wa, wb):
    args = (a, b, wa, wb)
    shape = (a.shape[0], wa.shape[1])
    return call(
        first_exit_body,
        [whole(x.shape) for x in args],
        whole(shape),
        jax.ShapeDtypeStruct(shape, F32),
        [],
        0,
        4 * a.shape[0] * a.shape[1] * wa.shape[1],
        12,
    )(*args)


def own_exit(a, w, more):
    args = (a, w, more)
    return call(
        own_exit_body,
        [whole(x.shape) for x in args],
        whole(more.shape),
        jax.ShapeDtypeStruct(more.shape, F32),
        [],
        0,
        2 * a.shape[0] * a.shape[1] * w.shape[1],
        12,
    )(*args)


def last_exit(a, w, more):
    args = (a, w, more)
    shape = (a.shape[0], w.shape[1])
    return call(
        last_exit_body,
        [whole(x.shape) for x in args],
        IN_HBM,
        jax.ShapeDtypeStruct(shape, BF16),
        [pltpu.VMEM(shape, BF16), pltpu.SemaphoreType.DMA((shape[1] // CHUNK,))],
        0,
        2 * a.shape[0] * a.shape[1] * w.shape[1],
        14,
    )(*args)


def turned(value, axis, by):
    peers = lax.axis_size(axis)
    return lax.ppermute(value, axis, [(i, (i + by) % peers) for i in range(peers)])


def shards(
    tokens,
    in_gain,
    ret_query,
    ret_key,
    ret_value,
    att_query,
    att_key,
    att_value,
    log_decay,
    ret_gain,
    sink_logit,
    retentive_exit_matrix,
    out_att,
):
    tp = lax.axis_index("tp").astype(jnp.int32)
    y = lax.axis_index("sp_1").astype(jnp.int32)
    z = lax.axis_index("sp_0").astype(jnp.int32)
    side, spot, row = tp.reshape(1), lax.axis_index(SP).astype(jnp.int32).reshape(1), z.reshape(1)
    side, spot, row, line_spot = lax.optimization_barrier((side, spot, row, y.reshape(1)))
    own = tokens[0]
    gain = in_gain[None]
    peer = turned(own, "tp", 1)
    early = (ret_key, ret_value, att_key, att_value)
    rates = log_decay.reshape(log_decay.shape[1], 1, log_decay.shape[2])
    first, scaled_own, squares, row_cum, col, wide_col, late = own_half(
        side, own, gain, rates, early
    )
    ret_k, ret_v, att_kv, inv, scaled, payload, tail = keys_half(
        side, peer, gain, first, squares, col, late, ret_key.shape[1]
    )
    sources = [payload] + [turned(payload, "sp_1", k) for k in (1, 2, 3)]
    peers = lax.axis_size(SP)
    halo = lax.ppermute(tail, SP, [(i, (i + 1) % peers) for i in range(peers)])
    ret_q, att_q = queries(side, scaled_own, scaled, inv, ret_query, att_query)
    sources, ret_q = lax.optimization_barrier((sources, ret_q))
    line, line_log, span = scan_step(line_body, line_spot, sources)
    sources = [span, turned(span, "sp_0", 1), turned(span, "sp_0", 7)]
    side, span = lax.optimization_barrier((side, span))
    theirs = window(False, side, spot, att_q, att_kv, halo, sink_logit)
    exit_own, out_own, sources[0] = lax.optimization_barrier(
        (retentive_exit_matrix, out_att, sources[0])
    )
    out_peer = turned(out_own, "tp", 1)
    exit_peer = turned(exit_own, "tp", 1)
    sources, theirs = lax.optimization_barrier((sources, theirs))
    att_got = turned(theirs, "tp", 1)
    column, column_log, span = scan_step(column_body, row, sources)
    sources = [turned(span, "sp_0", 3), turned(span, "sp_0", 6)]
    side, row, span = lax.optimization_barrier((side, row, span))
    att_mine = window(True, side, spot, att_q, att_kv, halo, sink_logit)
    ret_q, row = lax.optimization_barrier((ret_q, row))
    inside = inner(ret_q, ret_k, ret_v, row_cum, col, wide_col)
    partial = first_exit(att_mine, att_got, out_att, out_peer)
    sources, partial, inside = lax.optimization_barrier((sources, partial, inside))
    small = [line, line_log, column, column_log] + sources
    args = (side, row, ret_q, inside, col, ret_gain, small)
    ret_got = turned(finish(False, *args), "tp", 1)
    ret_mine = finish(True, *args)
    partial = own_exit(ret_mine, retentive_exit_matrix, partial)
    mixed = last_exit(ret_got, exit_peer, partial)
    return mixed[None]


def solution(mesh):
    finer = Mesh(
        mesh.devices.reshape(8, 4, mesh.shape["fs"], mesh.shape["tp"]), ("sp_0", "sp_1", "fs", "tp")
    )
    placed = (
        P("fs", SP, "tp"),
        P(),
        P(None, "tp"),
        P(None, "tp"),
        P(None, "tp"),
        P(None, "tp"),
        P(None, "tp"),
        P(None, "tp"),
        P("fs", "tp", SP),
        P("tp"),
        P("tp"),
        P("tp", None),
        P("tp", None),
    )
    return jax.shard_map(
        shards, mesh=finer, in_specs=placed, out_specs=P("fs", SP_TP, None), check_vma=False
    )
```

```python
import functools

import jax
import jax.numpy as jnp
from jax import lax
from jax.experimental import pallas as pl
from jax.experimental.pallas import tpu as pltpu
from jax.sharding import Mesh
from jax.sharding import PartitionSpec as P


HEAD_DIM = 64
WINDOW = 128
EPS = 1e-06
SP = ("sp_0", "sp_1")
SP_TP = ("sp_0", "sp_1", "tp")
F32 = jnp.float32
BF16 = jnp.bfloat16
CHUNK = 256
STATE_ROWS = 192
LOG_ROWS = 16
PAY_ROWS = STATE_ROWS + LOG_ROWS
PAIRS = 3
LANES = 128
CONTRACT_ROWS = (((0,), (0,)), ((), ()))
CONTRACT_LANES = (((1,), (1,)), ((), ()))


def dot(a, b):
    return jnp.dot(a, b, preferred_element_type=F32)


def lane_ids(shape):
    return lax.broadcasted_iota(jnp.int32, shape, len(shape) - 1)


def row_ids(shape):
    return lax.broadcasted_iota(jnp.int32, shape, 0)


def half_mask(half, dtype):
    lanes = lane_ids((1, LANES))
    inside = (lanes < HEAD_DIM) if half == 0 else (lanes >= HEAD_DIM)
    return jnp.where(inside, 1.0, 0.0).astype(dtype)


def diagonal_mask():
    return (row_ids((LANES, LANES)) < HEAD_DIM) == (lane_ids((LANES, LANES)) < HEAD_DIM)


def split3(x):
    high = x.astype(BF16).astype(F32)
    rest = x - high
    middle = rest.astype(BF16).astype(F32)
    return high, middle, rest - middle


def call(body, in_specs, out_specs, out_shape, scratch, scalars, flops, mib, grid=(1,)):
    return pl.pallas_call(
        body,
        out_shape=out_shape,
        grid_spec=pltpu.PrefetchScalarGridSpec(
            num_scalar_prefetch=scalars,
            grid=grid,
            in_specs=in_specs,
            out_specs=out_specs,
            scratch_shapes=scratch,
        ),
        compiler_params=pltpu.CompilerParams(
            dimension_semantics=("arbitrary",) * len(grid), vmem_limit_bytes=mib * 2**20
        ),
        cost_estimate=pl.CostEstimate(flops=flops, transcendentals=0, bytes_accessed=1 << 20),
    )


def whole(shape):
    return pl.BlockSpec(shape, lambda *_: (0,) * len(shape))


IN_HBM = pl.BlockSpec(memory_space=pltpu.HBM)
SCALE = HEAD_DIM**-0.5


def in_hbm(x):
    return pltpu.with_memory_space_constraint(x, pltpu.HBM)


def fetch_weights(weights, buffer, sems, begin):
    copies, start = [], 0
    depth = buffer.shape[0]
    for i, w in enumerate(weights):
        stop = start + w.shape[1]
        copy = pltpu.make_async_copy(
            w.at[pl.ds(begin, depth), :], buffer.at[:, start:stop], sems.at[i]
        )
        copy.start()
        copies.append(copy)
        start = stop
    return copies


def weight_columns(weights, begin, depth, start):
    pieces, left = [], 0
    for w in weights:
        for n in range(0, w.shape[1], LANES):
            if start <= left + n < start + CHUNK:
                pieces.append(w[pl.ds(begin, depth), n : n + LANES])
        left += w.shape[1]
    return jnp.concatenate(pieces, axis=1)


def squares_of(wide):
    squares = wide * wide
    total = squares[:, 0:LANES]
    for start in range(LANES, wide.shape[1], LANES):
        total = total + squares[:, start : start + LANES]
    return total


def decays(rates_ref, row_ref, col_ref, wide_ref):
    heads, _, rows = rates_ref.shape
    row_ref[...] = jnp.zeros_like(row_ref)
    for h in range(heads):
        row_ref[h : h + 1, :] = rates_ref[h]
    total = row_ref[...]
    lanes = lane_ids(total.shape)
    step = 1
    while step < rows:
        total = total + jnp.where(lanes >= step, pltpu.roll(total, step, 1), 0.0)
        step *= 2
    row_ref[...] = total
    parts = jnp.concatenate(split3(total) + (jnp.zeros_like(total),), axis=0).astype(BF16)
    for ref, lanes in ((col_ref, HEAD_DIM), (wide_ref, LANES)):
        shape = (32, heads * lanes)
        picks = (row_ids(shape) % 8 == lane_ids(shape) // lanes).astype(F32).astype(BF16)
        ref[...] = lax.dot_general(parts, picks, CONTRACT_ROWS, preferred_element_type=F32)


def own_body(tp, x_hbm, gain_hbm, rates_hbm, *refs):
    weights = refs[:4]
    first, scaled, sq, row, col, wide_col, later, xbuf, gain, rates, wbuf, sems = refs[4:]
    rows, depth = xbuf.shape
    small = pltpu.make_async_copy(rates_hbm, rates, sems.at[8])
    small.start()
    load = pltpu.make_async_copy(x_hbm, xbuf, sems.at[6])
    load.start()
    gains = pltpu.make_async_copy(gain_hbm, gain, sems.at[7])
    gains.start()
    begin = pl.multiple_of(tp[0] * depth, depth)
    copies = fetch_weights(weights, wbuf, sems, begin)
    other = pl.multiple_of((1 - tp[0]) * depth, depth)
    more = fetch_weights(weights, later, sems.at[pl.ds(9, 4)], other)
    small.wait()
    decays(rates, row, col, wide_col)
    gains.wait()
    load.wait()
    for copy in copies:
        copy.wait()
    scale = gain[:, pl.ds(begin, depth)]
    for m in range(0, rows, CHUNK):
        here = slice(m, m + CHUNK)
        wide = xbuf[here, :].astype(F32)
        part = (wide * scale).astype(BF16)
        scaled[here, :] = part
        sq[here, :] = squares_of(wide)
        for n in range(0, first.shape[1], CHUNK):
            first[here, n : n + CHUNK] = dot(part, wbuf[:, n : n + CHUNK])
    for copy in more:
        copy.wait()


def own_half(tp, own, gain, rates, weights):
    rows, depth = own.shape
    widths = [w.shape[1] for w in weights]
    shapes = [
        ((rows, sum(widths)), F32),
        ((rows, depth), BF16),
        ((rows, LANES), F32),
        ((8, rows), F32),
        ((rows, widths[0]), F32),
        ((rows, 2 * widths[0]), F32),
        ((depth, sum(widths)), BF16),
    ]
    return call(
        own_body,
        [IN_HBM] * 7,
        [whole(s) for s, _ in shapes],
        [jax.ShapeDtypeStruct(s, t) for s, t in shapes],
        [
            pltpu.VMEM((rows, depth), BF16),
            pltpu.VMEM(gain.shape, F32),
            pltpu.VMEM(rates.shape, F32),
            pltpu.VMEM((depth, sum(widths)), BF16),
            pltpu.SemaphoreType.DMA((13,)),
        ],
        1,
        2 * rows * depth * sum(widths),
        24,
    )(tp, *[in_hbm(a) for a in (own, gain, rates) + weights])


def keys_body(tp, x, gain, part, sq, col, wbuf, *refs):
    k_out, v_out, akv_out, inv_out, scaled_out, pay_out, tail_out = refs
    rows, depth = x.shape
    width = k_out.shape[1]
    begin = pl.multiple_of((1 - tp[0]) * depth, depth)
    scale = gain[:, pl.ds(begin, depth)]
    low = lane_ids((HEAD_DIM, LANES)) < HEAD_DIM
    for m in range(0, rows, CHUNK):
        here = slice(m, m + CHUNK)
        wide = x[here, :].astype(F32)
        scaled = (wide * scale).astype(BF16)
        scaled_out[here, :] = scaled
        mean = jnp.sum(sq[here, :] + squares_of(wide), axis=1, keepdims=True) / (2 * depth)
        inverse = lax.rsqrt(mean + EPS)
        inv_out[here, :] = jnp.broadcast_to(inverse, (CHUNK, LANES))
        for n in range(0, part.shape[1], CHUNK):
            total = part[here, n : n + CHUNK] + dot(scaled, wbuf[:, n : n + CHUNK])
            value = (total * inverse).astype(BF16)
            for j in range(n, n + CHUNK, LANES):
                piece = value[:, j - n : j - n + LANES]
                if j < width:
                    k_out[here, j : j + LANES] = piece * jnp.asarray(SCALE, BF16)
                elif j < 2 * width:
                    v_out[here, j - width : j - width + LANES] = piece
                else:
                    akv_out[here, j - 2 * width : j - 2 * width + LANES] = piece
    logs = jnp.zeros((LOG_ROWS, LANES), F32)
    places = row_ids((LOG_ROWS, LANES))
    for p in range(PAIRS):
        lanes = slice(p * LANES, (p + 1) * LANES)
        last = col[rows - 1 : rows, lanes]
        faded = (k_out[:, lanes].astype(F32) * jnp.exp(last - col[:, lanes])).astype(BF16)
        state = lax.dot_general(faded, v_out[:, lanes], CONTRACT_ROWS, preferred_element_type=F32)
        packed = jnp.where(low, state[0:HEAD_DIM], state[HEAD_DIM:]).astype(BF16)
        pay_out[p * HEAD_DIM : (p + 1) * HEAD_DIM, :] = packed
        for i, part3 in enumerate(split3(last)):
            logs = logs + jnp.where(places == 3 * p + i, part3, 0.0)
    pay_out[STATE_ROWS:, :] = logs.astype(BF16)
    tail_out[...] = akv_out[rows - WINDOW : rows, :]


def keys_half(tp, peer, gain, part, sq, col, wbuf, width):
    rows, depth = peer.shape
    shapes = [
        ((rows, width), BF16),
        ((rows, width), BF16),
        ((rows, wbuf.shape[1] - 2 * width), BF16),
        ((rows, LANES), F32),
        ((rows, depth), BF16),
        ((PAY_ROWS, LANES), BF16),
        ((WINDOW, wbuf.shape[1] - 2 * width), BF16),
    ]
    return call(
        keys_body,
        [whole(a.shape) for a in (peer, gain, part, sq, col, wbuf)],
        [whole(s) for s, _ in shapes],
        [jax.ShapeDtypeStruct(s, t) for s, t in shapes],
        [],
        1,
        2 * rows * depth * wbuf.shape[1],
        20,
    )(tp, peer, gain, part, sq, col, wbuf)


def queries_body(tp, own, peer, inv, w0, w1, q_out, aq_out):
    rows, depth = own.shape
    width = q_out.shape[1]
    begin = pl.multiple_of(tp[0] * depth, depth)
    other = pl.multiple_of((1 - tp[0]) * depth, depth)
    weights = (w0, w1)
    for m in range(0, rows, CHUNK):
        here = slice(m, m + CHUNK)
        inverse = inv[here, 0:1]
        for n in range(0, 2 * width, CHUNK):
            total = dot(own[here, :], weight_columns(weights, begin, depth, n))
            total = total + dot(peer[here, :], weight_columns(weights, other, depth, n))
            value = (total * inverse).astype(BF16)
            for j in range(n, n + CHUNK, LANES):
                piece = value[:, j - n : j - n + LANES]
                if j < width:
                    q_out[here, j : j + LANES] = piece
                else:
                    aq_out[here, j - width : j - width + LANES] = piece * jnp.asarray(SCALE, BF16)


def queries(tp, own, peer, inv, w0, w1):
    rows, depth = own.shape
    shapes = [(rows, w0.shape[1]), (rows, w1.shape[1])]
    return call(
        queries_body,
        [whole(a.shape) for a in (own, peer, inv, w0, w1)],
        [whole(s) for s in shapes],
        [jax.ShapeDtypeStruct(s, BF16) for s in shapes],
        [],
        1,
        8 * rows * depth * w0.shape[1],
        20,
    )(tp, own, peer, inv, w0, w1)


def inner_body(q_ref, k_ref, v_ref, row_ref, col_ref, wide_ref, out_ref):
    rows = q_ref.shape[0]
    size = 256
    later = row_ids((size, size)) >= lane_ids((size, size))
    diagonal = diagonal_mask()
    masks = [half_mask(0, BF16), half_mask(1, BF16)]
    states = [None] * PAIRS
    for begin in range(0, rows, size):
        here = slice(begin, begin + size)
        last = slice(begin + size - 1, begin + size)
        for pair in range(PAIRS):
            lanes = slice(pair * LANES, (pair + 1) * LANES)
            q, k, v = q_ref[here, lanes], k_ref[here, lanes], v_ref[here, lanes]
            cum = col_ref[here, lanes]
            end = col_ref[last, lanes]
            start = col_ref[begin - 1 : begin, lanes] if begin else None
            both = jnp.concatenate([q * masks[0], q * masks[1]], axis=0)
            scores = lax.dot_general(both, k, CONTRACT_LANES, preferred_element_type=F32)
            weights = []
            for half in range(2):
                head = 2 * pair + half
                over = wide_ref[here, head * LANES : (head + 1) * LANES]
                over = jnp.concatenate([over] * (size // LANES), axis=1)
                fade = jnp.exp(jnp.where(later, over - row_ref[head : head + 1, here], -jnp.inf))
                part = scores[half * size : (half + 1) * size]
                weights.append((part * fade).astype(BF16))
            values = jnp.concatenate([v * masks[0], v * masks[1]], axis=0)
            out = dot(jnp.concatenate(weights, axis=1), values)
            if begin:
                faded = (q.astype(F32) * jnp.exp(cum - start)).astype(BF16)
                out = out + dot(faded, states[pair].astype(BF16))
            out_ref[here, lanes] = out
            if begin + size < rows:
                keyed = (k.astype(F32) * jnp.exp(end - cum)).astype(BF16)
                added = lax.dot_general(keyed, v, CONTRACT_ROWS, preferred_element_type=F32)
                added = jnp.where(diagonal, added, 0.0)
                states[pair] = states[pair] * jnp.exp(end - start) + added if begin else added


def inner(q, k, v, row, col, wide):
    args = (q, k, v, row, col, wide)
    return call(
        inner_body,
        [whole(a.shape) for a in args],
        whole(q.shape),
        jax.ShapeDtypeStruct(q.shape, F32),
        [],
        0,
        3 * 2**30,
        12,
    )(*args)


def logs_of(tile, p):
    return tile[3 * p : 3 * p + 1] + tile[3 * p + 1 : 3 * p + 2] + tile[3 * p + 2 : 3 * p + 3]


def state_of(ref, p):
    return ref[p * HEAD_DIM : (p + 1) * HEAD_DIM, :].astype(F32)


def log_tile(ref):
    return ref[STATE_ROWS:PAY_ROWS, :].astype(F32)


def write_logs(pay_out, rows):
    places = row_ids((LOG_ROWS, LANES))
    logs = jnp.zeros((LOG_ROWS, LANES), F32)
    for p, row in enumerate(rows):
        for i, part in enumerate(split3(row)):
            logs = logs + jnp.where(places == 3 * p + i, part, 0.0)
    pay_out[STATE_ROWS:, :] = logs.astype(BF16)


def line_body(place, *refs):
    y = place[0]
    sources, (before_out, log_out, pay_out) = refs[:4], refs[4:]
    tiles = [log_tile(r) for r in sources]
    spots = [(y - k + 4) % 4 for k in range(4)]
    lead = jnp.zeros((8, LANES), F32)
    totals = []
    for p in range(PAIRS):
        here = slice(p * HEAD_DIM, (p + 1) * HEAD_DIM)
        logs = [logs_of(t, p) for t in tiles]
        states = [state_of(r, p) for r in sources]
        total = before = between = None
        for k in range(4):
            after = jnp.zeros((1, LANES), F32)
            for j in range(4):
                if j != k:
                    after = after + jnp.where(spots[j] > spots[k], logs[j], 0.0)
            part = states[k] * jnp.exp(after)
            total = part if total is None else total + part
            if k > 0:
                part = jnp.where(k <= y, states[k], 0.0)
                part = part if between is None else part * jnp.exp(between)
                before = part if before is None else before + part
                rate = jnp.where(k <= y, logs[k], 0.0)
                between = rate if between is None else between + rate
        before_out[here, :] = before
        lead = lead + jnp.where(row_ids((8, LANES)) == p, between, 0.0)
        pay_out[here, :] = total.astype(BF16)
        totals.append(logs[0] + logs[1] + logs[2] + logs[3])
    log_out[...] = lead
    write_logs(pay_out, totals)


def column_body(place, own, back, ahead, before_out, log_out, pay_out):
    z = place[0]
    last = z == 7
    tiles = [log_tile(r) for r in (own, back, ahead)]
    lead = jnp.zeros((8, LANES), F32)
    totals = []
    for p in range(PAIRS):
        here = slice(p * HEAD_DIM, (p + 1) * HEAD_DIM)
        log, log_back, log_ahead = [logs_of(t, p) for t in tiles]
        before = jnp.where(z >= 1, state_of(back, p), 0.0)
        rate = jnp.where(z >= 1, log_back, 0.0)
        before_out[here, :] = before
        lead = lead + jnp.where(row_ids((8, LANES)) == p, rate, 0.0)
        inner_part = jnp.where(last, 0.0, state_of(own, p) + jnp.exp(log) * before)
        pay_out[here, :] = (state_of(ahead, p) + jnp.exp(log_ahead) * inner_part).astype(BF16)
        totals.append(log_ahead + jnp.where(last, 0.0, log + rate))
    log_out[...] = lead
    write_logs(pay_out, totals)


def scan_step(body, place, sources):
    return call(
        body,
        [whole(a.shape) for a in sources],
        [whole((STATE_ROWS, LANES)), whole((8, LANES)), whole((PAY_ROWS, LANES))],
        [
            jax.ShapeDtypeStruct((STATE_ROWS, LANES), F32),
            jax.ShapeDtypeStruct((8, LANES), F32),
            jax.ShapeDtypeStruct((PAY_ROWS, LANES), BF16),
        ],
        [],
        1,
        2**26,
        4,
    )(place, *sources)


def finish_body(side, row, q_ref, in_ref, col_ref, gain, *refs):
    line, line_log, column, column_log, three, six, out_ref = refs
    z = row[0]
    tile3, tile6 = log_tile(three), log_tile(six)
    diagonal = diagonal_mask()
    ones = jnp.where(diagonal, 1.0, 0.0).astype(BF16)
    for p in range(PAIRS):
        here = slice(p * HEAD_DIM, (p + 1) * HEAD_DIM)
        lanes = slice(p * LANES, (p + 1) * LANES)
        far = jnp.where(z >= 2, state_of(three, p), 0.0)
        rate = jnp.where(z >= 2, logs_of(tile3, p), 0.0)
        far = far + jnp.exp(rate) * jnp.where(z >= 5, state_of(six, p), 0.0)
        before = column[here, :] + jnp.exp(column_log[p : p + 1, :]) * far
        before = line[here, :] + jnp.exp(line_log[p : p + 1, :]) * before
        state = jnp.where(diagonal, jnp.concatenate([before, before], axis=0), 0.0).astype(BF16)
        carried = dot(q_ref[:, lanes], state) * jnp.exp(col_ref[:, lanes])
        retained = in_ref[:, lanes] + carried
        squares = retained * retained
        high = squares.astype(BF16)
        rest = (squares - high.astype(F32)).astype(BF16)
        mean = (dot(high, ones) + dot(rest, ones)) / HEAD_DIM
        out_ref[:, lanes] = (
            retained * lax.rsqrt(mean + EPS) * gain[lanes].reshape(1, LANES)
        ).astype(BF16)


def finish(mine, side, row, q, inside, col, gain, small):
    rows, width = q.shape
    spec = pl.BlockSpec((rows // 2, width), lambda i, t, z: (half_of(t, mine), 0))
    return call(
        finish_body,
        [spec, spec, spec, whole(gain.shape)] + [whole(s.shape) for s in small],
        whole((rows // 2, width)),
        jax.ShapeDtypeStruct((rows // 2, width), BF16),
        [],
        2,
        2**29,
        8,
    )(side, row, q, inside, col, gain, *small)


def half_of(side, mine):
    return side[0] if mine else 1 - side[0]


def window_body(mine, side, spot, q_ref, kv_ref, halo_ref, sink_ref, out_ref, ext):
    half, first = half_of(side, mine), spot[0]
    rows = q_ref.shape[0]
    begin = pl.multiple_of(half * rows, WINDOW)

    @pl.when(half == 0)
    def _():
        ext[0:WINDOW, :] = halo_ref[...]

    @pl.when(half == 1)
    def _():
        ext[0:WINDOW, :] = kv_ref[rows - WINDOW : rows, :]

    ext[WINDOW:, :] = kv_ref[pl.ds(begin, rows), :]
    masks = [half_mask(0, BF16), half_mask(1, BF16)]
    heads = q_ref.shape[1] // HEAD_DIM
    group = heads // 2
    band = (WINDOW, group * WINDOW)
    upper = row_ids(band) > lane_ids(band) % WINDOW
    empty = jnp.where((half == 0) & (first == 0), -jnp.inf, 0.0)
    levels = sink_ref[...].reshape(1, heads)
    levels = [jnp.broadcast_to(levels[:, h : h + 1], (1, WINDOW)) for h in range(heads)]
    sinks = [jnp.concatenate(levels[g * group : (g + 1) * group], axis=1) for g in range(2)]
    for block in range(rows // WINDOW):
        span = slice(block * WINDOW, (block + 2) * WINDOW)
        keys, values = ext[span, 0:LANES], ext[span, LANES:]
        here = slice(block * WINDOW, (block + 1) * WINDOW)
        outs = []
        for g in range(2):
            stack = []
            sink = sinks[g]
            for j in range(group):
                h = g * group + j
                q = q_ref[here, h // 2 * LANES : (h // 2 + 1) * LANES]
                if h % 2 != g:
                    q = pltpu.roll(q.astype(F32), HEAD_DIM, 1).astype(BF16)
                stack.append(q * masks[g])
            scores = lax.dot_general(
                keys, jnp.concatenate(stack, axis=0), CONTRACT_LANES, preferred_element_type=F32
            )
            back = scores[0:WINDOW] + empty if block == 0 else scores[0:WINDOW]
            scores = jnp.where(upper, back, scores[WINDOW:])
            highest = jnp.maximum(jnp.max(scores, axis=0, keepdims=True), sink)
            raised = jnp.exp(scores - highest)
            total = jnp.sum(raised, axis=0, keepdims=True) + jnp.exp(sink - highest)
            weights = jnp.concatenate(
                [jnp.where(upper, raised, 0.0), jnp.where(upper, 0.0, raised)], axis=0
            ).astype(BF16)
            out = lax.dot_general(values, weights, CONTRACT_ROWS, preferred_element_type=F32)
            out = out[g * HEAD_DIM : (g + 1) * HEAD_DIM] * (1.0 / total)
            outs += [out[:, j * WINDOW : (j + 1) * WINDOW] for j in range(group)]
        for p in range(heads // 2):
            both = jnp.concatenate([outs[2 * p], outs[2 * p + 1]], axis=0)
            out_ref[here, p * LANES : (p + 1) * LANES] = both.T.astype(BF16)


def window(mine, side, spot, q, kv, halo, sinks):
    rows, width = q.shape
    return call(
        functools.partial(window_body, mine),
        [
            pl.BlockSpec((rows // 2, width), lambda i, t, f: (half_of(t, mine), 0)),
            whole(kv.shape),
            whole(halo.shape),
            whole(sinks.shape),
        ],
        whole((rows // 2, width)),
        jax.ShapeDtypeStruct((rows // 2, width), BF16),
        [pltpu.VMEM((rows // 2 + WINDOW, kv.shape[1]), BF16)],
        2,
        2**30,
        8,
    )(side, spot, q, kv, halo, sinks)


def first_exit_body(a, b, wa, wb, out):
    rows = jnp.concatenate([a[...], b[...]], axis=1)
    for n in range(0, out.shape[1], CHUNK):
        here = slice(n, n + CHUNK)
        out[:, here] = dot(rows, jnp.concatenate([wa[:, here], wb[:, here]], axis=0))


def own_exit_body(a, w, more, out):
    for n in range(0, out.shape[1], CHUNK):
        here = slice(n, n + CHUNK)
        out[:, here] = more[:, here] + dot(a[...], w[:, here])


def last_exit_body(a, w, more, out, buffer, sems):
    copies = []
    for i, n in enumerate(range(0, out.shape[1], CHUNK)):
        here = slice(n, n + CHUNK)
        buffer[:, here] = (more[:, here] + dot(a[...], w[:, here])).astype(BF16)
        copy = pltpu.make_async_copy(buffer.at[:, here], out.at[:, here], sems.at[i])
        copy.start()
        copies.append(copy)
    for copy in copies:
        copy.wait()


def first_exit(a, b, wa, wb):
    args = (a, b, wa, wb)
    shape = (a.shape[0], wa.shape[1])
    return call(
        first_exit_body,
        [whole(x.shape) for x in args],
        whole(shape),
        jax.ShapeDtypeStruct(shape, F32),
        [],
        0,
        4 * a.shape[0] * a.shape[1] * wa.shape[1],
        12,
    )(*args)


def finish_exit_body(side, row, q_ref, in_ref, col_ref, gain, *refs):
    small, (w, more, out, rows) = refs[:6], refs[6:]
    finish_body(side, row, q_ref, in_ref, col_ref, gain, *small, rows)
    own_exit_body(rows, w, more, out)


def finish_exit(side, row, q, inside, col, gain, small, w, more):
    rows, width = q.shape
    spec = pl.BlockSpec((rows // 2, width), lambda i, t, z: (half_of(t, True), 0))
    rest = list(small) + [w, more]
    return call(
        finish_exit_body,
        [spec, spec, spec, whole(gain.shape)] + [whole(s.shape) for s in rest],
        whole(more.shape),
        jax.ShapeDtypeStruct(more.shape, F32),
        [pltpu.VMEM((rows // 2, width), BF16)],
        2,
        2**29,
        16,
    )(side, row, q, inside, col, gain, *rest)


def last_exit(a, w, more):
    args = (a, w, more)
    shape = (a.shape[0], w.shape[1])
    return call(
        last_exit_body,
        [whole(x.shape) for x in args],
        IN_HBM,
        jax.ShapeDtypeStruct(shape, BF16),
        [pltpu.VMEM(shape, BF16), pltpu.SemaphoreType.DMA((shape[1] // CHUNK,))],
        0,
        2 * a.shape[0] * a.shape[1] * w.shape[1],
        14,
    )(*args)


def turned(value, axis, by):
    peers = lax.axis_size(axis)
    return lax.ppermute(value, axis, [(i, (i + by) % peers) for i in range(peers)])


def shards(
    tokens,
    in_gain,
    ret_query,
    ret_key,
    ret_value,
    att_query,
    att_key,
    att_value,
    log_decay,
    ret_gain,
    sink_logit,
    retentive_exit_matrix,
    out_att,
):
    tp = lax.axis_index("tp").astype(jnp.int32)
    y = lax.axis_index("sp_1").astype(jnp.int32)
    z = lax.axis_index("sp_0").astype(jnp.int32)
    side, spot, row = tp.reshape(1), lax.axis_index(SP).astype(jnp.int32).reshape(1), z.reshape(1)
    side, spot, row, line_spot = lax.optimization_barrier((side, spot, row, y.reshape(1)))
    own = tokens[0]
    gain = in_gain[None]
    peer = turned(own, "tp", 1)
    early = (ret_key, ret_value, att_key, att_value)
    rates = log_decay.reshape(log_decay.shape[1], 1, log_decay.shape[2])
    first, scaled_own, squares, row_cum, col, wide_col, late = own_half(
        side, own, gain, rates, early
    )
    ret_k, ret_v, att_kv, inv, scaled, payload, tail = keys_half(
        side, peer, gain, first, squares, col, late, ret_key.shape[1]
    )
    sources = [payload] + [turned(payload, "sp_1", k) for k in (1, 2, 3)]
    peers = lax.axis_size(SP)
    halo = lax.ppermute(tail, SP, [(i, (i + 1) % peers) for i in range(peers)])
    ret_q, att_q = queries(side, scaled_own, scaled, inv, ret_query, att_query)
    sources, ret_q = lax.optimization_barrier((sources, ret_q))
    line, line_log, span = scan_step(line_body, line_spot, sources)
    sources = [span, turned(span, "sp_0", 1), turned(span, "sp_0", 7)]
    side, span = lax.optimization_barrier((side, span))
    theirs = window(False, side, spot, att_q, att_kv, halo, sink_logit)
    exit_own, out_own, sources[0] = lax.optimization_barrier(
        (retentive_exit_matrix, out_att, sources[0])
    )
    out_peer = turned(out_own, "tp", 1)
    exit_peer = turned(exit_own, "tp", 1)
    sources, theirs = lax.optimization_barrier((sources, theirs))
    att_got = turned(theirs, "tp", 1)
    column, column_log, span = scan_step(column_body, row, sources)
    sources = [turned(span, "sp_0", 3), turned(span, "sp_0", 6)]
    side, row, span = lax.optimization_barrier((side, row, span))
    att_mine = window(True, side, spot, att_q, att_kv, halo, sink_logit)
    ret_q, row = lax.optimization_barrier((ret_q, row))
    inside = inner(ret_q, ret_k, ret_v, row_cum, col, wide_col)
    partial = first_exit(att_mine, att_got, out_att, out_peer)
    sources, partial, inside = lax.optimization_barrier((sources, partial, inside))
    small = [line, line_log, column, column_log] + sources
    args = (side, row, ret_q, inside, col, ret_gain, small)
    ret_got = turned(finish(False, *args), "tp", 1)
    partial = finish_exit(*args, retentive_exit_matrix, partial)
    mixed = last_exit(ret_got, exit_peer, partial)
    return mixed[None]


def solution(mesh):
    finer = Mesh(
        mesh.devices.reshape(8, 4, mesh.shape["fs"], mesh.shape["tp"]), ("sp_0", "sp_1", "fs", "tp")
    )
    placed = (
        P("fs", SP, "tp"),
        P(),
        P(None, "tp"),
        P(None, "tp"),
        P(None, "tp"),
        P(None, "tp"),
        P(None, "tp"),
        P(None, "tp"),
        P("fs", "tp", SP),
        P("tp"),
        P("tp"),
        P("tp", None),
        P("tp", None),
    )
    return jax.shard_map(
        shards, mesh=finer, in_specs=placed, out_specs=P("fs", SP_TP, None), check_vma=False
    )
```

```python
import functools

import jax
import jax.numpy as jnp
from jax import lax
from jax.experimental import pallas as pl
from jax.experimental.pallas import tpu as pltpu
from jax.sharding import Mesh
from jax.sharding import PartitionSpec as P


HEAD_DIM = 64
WINDOW = 128
EPS = 1e-06
SP = ("sp_0", "sp_1")
SP_TP = ("sp_0", "sp_1", "tp")
F32 = jnp.float32
BF16 = jnp.bfloat16
CHUNK = 256
STATE_ROWS = 192
LOG_ROWS = 16
PAY_ROWS = STATE_ROWS + LOG_ROWS
PAIRS = 3
LANES = 128
CONTRACT_ROWS = (((0,), (0,)), ((), ()))
CONTRACT_LANES = (((1,), (1,)), ((), ()))


def dot(a, b):
    return jnp.dot(a, b, preferred_element_type=F32)


def lane_ids(shape):
    return lax.broadcasted_iota(jnp.int32, shape, len(shape) - 1)


def row_ids(shape):
    return lax.broadcasted_iota(jnp.int32, shape, 0)


def half_mask(half, dtype):
    lanes = lane_ids((1, LANES))
    inside = (lanes < HEAD_DIM) if half == 0 else (lanes >= HEAD_DIM)
    return jnp.where(inside, 1.0, 0.0).astype(dtype)


def diagonal_mask():
    return (row_ids((LANES, LANES)) < HEAD_DIM) == (lane_ids((LANES, LANES)) < HEAD_DIM)


def split3(x):
    high = x.astype(BF16).astype(F32)
    rest = x - high
    middle = rest.astype(BF16).astype(F32)
    return high, middle, rest - middle


def call(body, in_specs, out_specs, out_shape, scratch, scalars, flops, mib, grid=(1,)):
    return pl.pallas_call(
        body,
        out_shape=out_shape,
        grid_spec=pltpu.PrefetchScalarGridSpec(
            num_scalar_prefetch=scalars,
            grid=grid,
            in_specs=in_specs,
            out_specs=out_specs,
            scratch_shapes=scratch,
        ),
        compiler_params=pltpu.CompilerParams(
            dimension_semantics=("arbitrary",) * len(grid), vmem_limit_bytes=mib * 2**20
        ),
        cost_estimate=pl.CostEstimate(flops=flops, transcendentals=0, bytes_accessed=1 << 20),
    )


def whole(shape):
    return pl.BlockSpec(shape, lambda *_: (0,) * len(shape))


IN_HBM = pl.BlockSpec(memory_space=pltpu.HBM)
SCALE = HEAD_DIM**-0.5


def in_hbm(x):
    return pltpu.with_memory_space_constraint(x, pltpu.HBM)


def fetch_weights(weights, buffer, sems, begin):
    copies, start = [], 0
    depth = buffer.shape[0]
    for i, w in enumerate(weights):
        stop = start + w.shape[1]
        copy = pltpu.make_async_copy(
            w.at[pl.ds(begin, depth), :], buffer.at[:, start:stop], sems.at[i]
        )
        copy.start()
        copies.append(copy)
        start = stop
    return copies


def weight_columns(weights, begin, depth, start):
    pieces, left = [], 0
    for w in weights:
        for n in range(0, w.shape[1], LANES):
            if start <= left + n < start + CHUNK:
                pieces.append(w[pl.ds(begin, depth), n : n + LANES])
        left += w.shape[1]
    return jnp.concatenate(pieces, axis=1)


def squares_of(wide):
    squares = wide * wide
    total = squares[:, 0:LANES]
    for start in range(LANES, wide.shape[1], LANES):
        total = total + squares[:, start : start + LANES]
    return total


def decays(rates_ref, row_ref, col_ref, wide_ref):
    heads, _, rows = rates_ref.shape
    row_ref[...] = jnp.zeros_like(row_ref)
    for h in range(heads):
        row_ref[h : h + 1, :] = rates_ref[h]
    total = row_ref[...]
    lanes = lane_ids(total.shape)
    step = 1
    while step < rows:
        total = total + jnp.where(lanes >= step, pltpu.roll(total, step, 1), 0.0)
        step *= 2
    row_ref[...] = total
    parts = jnp.concatenate(split3(total) + (jnp.zeros_like(total),), axis=0).astype(BF16)
    for ref, lanes in ((col_ref, HEAD_DIM), (wide_ref, LANES)):
        shape = (32, heads * lanes)
        picks = (row_ids(shape) % 8 == lane_ids(shape) // lanes).astype(F32).astype(BF16)
        ref[...] = lax.dot_general(parts, picks, CONTRACT_ROWS, preferred_element_type=F32)


def own_body(tp, x_hbm, gain_hbm, rates_hbm, *refs):
    weights = refs[:4]
    first, scaled, sq, row, col, wide_col, later, xbuf, gain, rates, wbuf, sems = refs[4:]
    rows, depth = xbuf.shape
    small = pltpu.make_async_copy(rates_hbm, rates, sems.at[8])
    small.start()
    load = pltpu.make_async_copy(x_hbm, xbuf, sems.at[6])
    load.start()
    gains = pltpu.make_async_copy(gain_hbm, gain, sems.at[7])
    gains.start()
    begin = pl.multiple_of(tp[0] * depth, depth)
    copies = fetch_weights(weights, wbuf, sems, begin)
    other = pl.multiple_of((1 - tp[0]) * depth, depth)
    more = fetch_weights(weights, later, sems.at[pl.ds(9, 4)], other)
    small.wait()
    decays(rates, row, col, wide_col)
    gains.wait()
    load.wait()
    for copy in copies:
        copy.wait()
    scale = gain[:, pl.ds(begin, depth)]
    for m in range(0, rows, CHUNK):
        here = slice(m, m + CHUNK)
        wide = xbuf[here, :].astype(F32)
        part = (wide * scale).astype(BF16)
        scaled[here, :] = part
        sq[here, :] = squares_of(wide)
        for n in range(0, first.shape[1], CHUNK):
            first[here, n : n + CHUNK] = dot(part, wbuf[:, n : n + CHUNK])
    for copy in more:
        copy.wait()


def own_half(tp, own, gain, rates, weights):
    rows, depth = own.shape
    widths = [w.shape[1] for w in weights]
    shapes = [
        ((rows, sum(widths)), F32),
        ((rows, depth), BF16),
        ((rows, LANES), F32),
        ((8, rows), F32),
        ((rows, widths[0]), F32),
        ((rows, 2 * widths[0]), F32),
        ((depth, sum(widths)), BF16),
    ]
    return call(
        own_body,
        [IN_HBM] * 7,
        [whole(s) for s, _ in shapes],
        [jax.ShapeDtypeStruct(s, t) for s, t in shapes],
        [
            pltpu.VMEM((rows, depth), BF16),
            pltpu.VMEM(gain.shape, F32),
            pltpu.VMEM(rates.shape, F32),
            pltpu.VMEM((depth, sum(widths)), BF16),
            pltpu.SemaphoreType.DMA((13,)),
        ],
        1,
        2 * rows * depth * sum(widths),
        24,
    )(tp, *[in_hbm(a) for a in (own, gain, rates) + weights])


def keys_body(tp, x, gain, part, sq, col, wbuf, *refs):
    k_out, v_out, akv_out, inv_out, scaled_out, pay_out, tail_out = refs
    rows, depth = x.shape
    width = k_out.shape[1]
    begin = pl.multiple_of((1 - tp[0]) * depth, depth)
    scale = gain[:, pl.ds(begin, depth)]
    low = lane_ids((HEAD_DIM, LANES)) < HEAD_DIM
    for m in range(0, rows, CHUNK):
        here = slice(m, m + CHUNK)
        wide = x[here, :].astype(F32)
        scaled = (wide * scale).astype(BF16)
        scaled_out[here, :] = scaled
        mean = jnp.sum(sq[here, :] + squares_of(wide), axis=1, keepdims=True) / (2 * depth)
        inverse = lax.rsqrt(mean + EPS)
        inv_out[here, :] = jnp.broadcast_to(inverse, (CHUNK, LANES))
        for n in range(0, part.shape[1], CHUNK):
            total = part[here, n : n + CHUNK] + dot(scaled, wbuf[:, n : n + CHUNK])
            value = (total * inverse).astype(BF16)
            for j in range(n, n + CHUNK, LANES):
                piece = value[:, j - n : j - n + LANES]
                if j < width:
                    k_out[here, j : j + LANES] = piece * jnp.asarray(SCALE, BF16)
                elif j < 2 * width:
                    v_out[here, j - width : j - width + LANES] = piece
                else:
                    akv_out[here, j - 2 * width : j - 2 * width + LANES] = piece
    logs = jnp.zeros((LOG_ROWS, LANES), F32)
    places = row_ids((LOG_ROWS, LANES))
    for p in range(PAIRS):
        lanes = slice(p * LANES, (p + 1) * LANES)
        last = col[rows - 1 : rows, lanes]
        faded = (k_out[:, lanes].astype(F32) * jnp.exp(last - col[:, lanes])).astype(BF16)
        state = lax.dot_general(faded, v_out[:, lanes], CONTRACT_ROWS, preferred_element_type=F32)
        packed = jnp.where(low, state[0:HEAD_DIM], state[HEAD_DIM:]).astype(BF16)
        pay_out[p * HEAD_DIM : (p + 1) * HEAD_DIM, :] = packed
        for i, part3 in enumerate(split3(last)):
            logs = logs + jnp.where(places == 3 * p + i, part3, 0.0)
    pay_out[STATE_ROWS:, :] = logs.astype(BF16)
    tail_out[...] = akv_out[rows - WINDOW : rows, :]


def keys_half(tp, peer, gain, part, sq, col, wbuf, width):
    rows, depth = peer.shape
    shapes = [
        ((rows, width), BF16),
        ((rows, width), BF16),
        ((rows, wbuf.shape[1] - 2 * width), BF16),
        ((rows, LANES), F32),
        ((rows, depth), BF16),
        ((PAY_ROWS, LANES), BF16),
        ((WINDOW, wbuf.shape[1] - 2 * width), BF16),
    ]
    return call(
        keys_body,
        [whole(a.shape) for a in (peer, gain, part, sq, col, wbuf)],
        [whole(s) for s, _ in shapes],
        [jax.ShapeDtypeStruct(s, t) for s, t in shapes],
        [],
        1,
        2 * rows * depth * wbuf.shape[1],
        20,
    )(tp, peer, gain, part, sq, col, wbuf)


def queries_body(tp, own, peer, inv, w0, w1, q_out, aq_out):
    rows, depth = own.shape
    width = q_out.shape[1]
    begin = pl.multiple_of(tp[0] * depth, depth)
    other = pl.multiple_of((1 - tp[0]) * depth, depth)
    weights = (w0, w1)
    for m in range(0, rows, CHUNK):
        here = slice(m, m + CHUNK)
        inverse = inv[here, 0:1]
        for n in range(0, 2 * width, CHUNK):
            total = dot(own[here, :], weight_columns(weights, begin, depth, n))
            total = total + dot(peer[here, :], weight_columns(weights, other, depth, n))
            value = (total * inverse).astype(BF16)
            for j in range(n, n + CHUNK, LANES):
                piece = value[:, j - n : j - n + LANES]
                if j < width:
                    q_out[here, j : j + LANES] = piece
                else:
                    aq_out[here, j - width : j - width + LANES] = piece * jnp.asarray(SCALE, BF16)


def queries(tp, own, peer, inv, w0, w1):
    rows, depth = own.shape
    shapes = [(rows, w0.shape[1]), (rows, w1.shape[1])]
    return call(
        queries_body,
        [whole(a.shape) for a in (own, peer, inv, w0, w1)],
        [whole(s) for s in shapes],
        [jax.ShapeDtypeStruct(s, BF16) for s in shapes],
        [],
        1,
        8 * rows * depth * w0.shape[1],
        20,
    )(tp, own, peer, inv, w0, w1)


def inner_body(q_ref, k_ref, v_ref, row_ref, col_ref, wide_ref, out_ref):
    rows = q_ref.shape[0]
    size = 256
    later = row_ids((size, size)) >= lane_ids((size, size))
    diagonal = diagonal_mask()
    masks = [half_mask(0, BF16), half_mask(1, BF16)]
    states = [None] * PAIRS
    for begin in range(0, rows, size):
        here = slice(begin, begin + size)
        last = slice(begin + size - 1, begin + size)
        for pair in range(PAIRS):
            lanes = slice(pair * LANES, (pair + 1) * LANES)
            q, k, v = q_ref[here, lanes], k_ref[here, lanes], v_ref[here, lanes]
            cum = col_ref[here, lanes]
            end = col_ref[last, lanes]
            start = col_ref[begin - 1 : begin, lanes] if begin else None
            both = jnp.concatenate([q * masks[0], q * masks[1]], axis=0)
            scores = lax.dot_general(both, k, CONTRACT_LANES, preferred_element_type=F32)
            weights = []
            for half in range(2):
                head = 2 * pair + half
                over = wide_ref[here, head * LANES : (head + 1) * LANES]
                over = jnp.concatenate([over] * (size // LANES), axis=1)
                fade = jnp.exp(jnp.where(later, over - row_ref[head : head + 1, here], -jnp.inf))
                part = scores[half * size : (half + 1) * size]
                weights.append((part * fade).astype(BF16))
            values = jnp.concatenate([v * masks[0], v * masks[1]], axis=0)
            out = dot(jnp.concatenate(weights, axis=1), values)
            if begin:
                faded = (q.astype(F32) * jnp.exp(cum - start)).astype(BF16)
                out = out + dot(faded, states[pair].astype(BF16))
            out_ref[here, lanes] = out
            if begin + size < rows:
                keyed = (k.astype(F32) * jnp.exp(end - cum)).astype(BF16)
                added = lax.dot_general(keyed, v, CONTRACT_ROWS, preferred_element_type=F32)
                added = jnp.where(diagonal, added, 0.0)
                states[pair] = states[pair] * jnp.exp(end - start) + added if begin else added


def inner(q, k, v, row, col, wide):
    args = (q, k, v, row, col, wide)
    return call(
        inner_body,
        [whole(a.shape) for a in args],
        whole(q.shape),
        jax.ShapeDtypeStruct(q.shape, F32),
        [],
        0,
        3 * 2**30,
        12,
    )(*args)


def logs_of(tile, p):
    return tile[3 * p : 3 * p + 1] + tile[3 * p + 1 : 3 * p + 2] + tile[3 * p + 2 : 3 * p + 3]


def state_of(ref, p):
    return ref[p * HEAD_DIM : (p + 1) * HEAD_DIM, :].astype(F32)


def log_tile(ref):
    return ref[STATE_ROWS:PAY_ROWS, :].astype(F32)


def write_logs(pay_out, rows):
    places = row_ids((LOG_ROWS, LANES))
    logs = jnp.zeros((LOG_ROWS, LANES), F32)
    for p, row in enumerate(rows):
        for i, part in enumerate(split3(row)):
            logs = logs + jnp.where(places == 3 * p + i, part, 0.0)
    pay_out[STATE_ROWS:, :] = logs.astype(BF16)


def line_body(place, *refs):
    y = place[0]
    sources, (before_out, log_out, pay_out) = refs[:4], refs[4:]
    tiles = [log_tile(r) for r in sources]
    spots = [(y - k + 4) % 4 for k in range(4)]
    lead = jnp.zeros((8, LANES), F32)
    totals = []
    for p in range(PAIRS):
        here = slice(p * HEAD_DIM, (p + 1) * HEAD_DIM)
        logs = [logs_of(t, p) for t in tiles]
        states = [state_of(r, p) for r in sources]
        total = before = between = None
        for k in range(4):
            after = jnp.zeros((1, LANES), F32)
            for j in range(4):
                if j != k:
                    after = after + jnp.where(spots[j] > spots[k], logs[j], 0.0)
            part = states[k] * jnp.exp(after)
            total = part if total is None else total + part
            if k > 0:
                part = jnp.where(k <= y, states[k], 0.0)
                part = part if between is None else part * jnp.exp(between)
                before = part if before is None else before + part
                rate = jnp.where(k <= y, logs[k], 0.0)
                between = rate if between is None else between + rate
        before_out[here, :] = before
        lead = lead + jnp.where(row_ids((8, LANES)) == p, between, 0.0)
        pay_out[here, :] = total.astype(BF16)
        totals.append(logs[0] + logs[1] + logs[2] + logs[3])
    log_out[...] = lead
    write_logs(pay_out, totals)


def column_body(place, own, back, ahead, before_out, log_out, pay_out):
    z = place[0]
    last = z == 7
    tiles = [log_tile(r) for r in (own, back, ahead)]
    lead = jnp.zeros((8, LANES), F32)
    totals = []
    for p in range(PAIRS):
        here = slice(p * HEAD_DIM, (p + 1) * HEAD_DIM)
        log, log_back, log_ahead = [logs_of(t, p) for t in tiles]
        before = jnp.where(z >= 1, state_of(back, p), 0.0)
        rate = jnp.where(z >= 1, log_back, 0.0)
        before_out[here, :] = before
        lead = lead + jnp.where(row_ids((8, LANES)) == p, rate, 0.0)
        inner_part = jnp.where(last, 0.0, state_of(own, p) + jnp.exp(log) * before)
        pay_out[here, :] = (state_of(ahead, p) + jnp.exp(log_ahead) * inner_part).astype(BF16)
        totals.append(log_ahead + jnp.where(last, 0.0, log + rate))
    log_out[...] = lead
    write_logs(pay_out, totals)


def scan_step(body, place, sources):
    return call(
        body,
        [whole(a.shape) for a in sources],
        [whole((STATE_ROWS, LANES)), whole((8, LANES)), whole((PAY_ROWS, LANES))],
        [
            jax.ShapeDtypeStruct((STATE_ROWS, LANES), F32),
            jax.ShapeDtypeStruct((8, LANES), F32),
            jax.ShapeDtypeStruct((PAY_ROWS, LANES), BF16),
        ],
        [],
        1,
        2**26,
        4,
    )(place, *sources)


def finish_body(side, row, q_ref, in_ref, col_ref, gain, *refs):
    line, line_log, column, column_log, three, six, out_ref = refs
    z = row[0]
    tile3, tile6 = log_tile(three), log_tile(six)
    diagonal = diagonal_mask()
    ones = jnp.where(diagonal, 1.0, 0.0).astype(BF16)
    for p in range(PAIRS):
        here = slice(p * HEAD_DIM, (p + 1) * HEAD_DIM)
        lanes = slice(p * LANES, (p + 1) * LANES)
        far = jnp.where(z >= 2, state_of(three, p), 0.0)
        rate = jnp.where(z >= 2, logs_of(tile3, p), 0.0)
        far = far + jnp.exp(rate) * jnp.where(z >= 5, state_of(six, p), 0.0)
        before = column[here, :] + jnp.exp(column_log[p : p + 1, :]) * far
        before = line[here, :] + jnp.exp(line_log[p : p + 1, :]) * before
        state = jnp.where(diagonal, jnp.concatenate([before, before], axis=0), 0.0).astype(BF16)
        carried = dot(q_ref[:, lanes], state) * jnp.exp(col_ref[:, lanes])
        retained = in_ref[:, lanes] + carried
        squares = retained * retained
        high = squares.astype(BF16)
        rest = (squares - high.astype(F32)).astype(BF16)
        mean = (dot(high, ones) + dot(rest, ones)) / HEAD_DIM
        out_ref[:, lanes] = (
            retained * lax.rsqrt(mean + EPS) * gain[lanes].reshape(1, LANES)
        ).astype(BF16)


def finish(mine, side, row, q, inside, col, gain, small):
    rows, width = q.shape
    spec = pl.BlockSpec((rows // 2, width), lambda i, t, z: (half_of(t, mine), 0))
    return call(
        finish_body,
        [spec, spec, spec, whole(gain.shape)] + [whole(s.shape) for s in small],
        whole((rows // 2, width)),
        jax.ShapeDtypeStruct((rows // 2, width), BF16),
        [],
        2,
        2**29,
        8,
    )(side, row, q, inside, col, gain, *small)


def half_of(side, mine):
    return side[0] if mine else 1 - side[0]


def window_body(mine, side, spot, q_ref, kv_ref, halo_ref, sink_ref, out_ref, ext):
    half, first = half_of(side, mine), spot[0]
    rows = q_ref.shape[0]
    begin = pl.multiple_of(half * rows, WINDOW)

    @pl.when(half == 0)
    def _():
        ext[0:WINDOW, :] = halo_ref[...]

    @pl.when(half == 1)
    def _():
        ext[0:WINDOW, :] = kv_ref[rows - WINDOW : rows, :]

    ext[WINDOW:, :] = kv_ref[pl.ds(begin, rows), :]
    masks = [half_mask(0, BF16), half_mask(1, BF16)]
    heads = q_ref.shape[1] // HEAD_DIM
    group = heads // 2
    band = (WINDOW, group * WINDOW)
    upper = row_ids(band) > lane_ids(band) % WINDOW
    empty = jnp.where((half == 0) & (first == 0), -jnp.inf, 0.0)
    levels = sink_ref[...].reshape(1, heads)
    levels = [jnp.broadcast_to(levels[:, h : h + 1], (1, WINDOW)) for h in range(heads)]
    sinks = [jnp.concatenate(levels[g * group : (g + 1) * group], axis=1) for g in range(2)]
    for block in range(rows // WINDOW):
        span = slice(block * WINDOW, (block + 2) * WINDOW)
        keys, values = ext[span, 0:LANES], ext[span, LANES:]
        here = slice(block * WINDOW, (block + 1) * WINDOW)
        outs = []
        for g in range(2):
            stack = []
            sink = sinks[g]
            for j in range(group):
                h = g * group + j
                q = q_ref[here, h // 2 * LANES : (h // 2 + 1) * LANES]
                if h % 2 != g:
                    q = pltpu.roll(q.astype(F32), HEAD_DIM, 1).astype(BF16)
                stack.append(q * masks[g])
            scores = lax.dot_general(
                keys, jnp.concatenate(stack, axis=0), CONTRACT_LANES, preferred_element_type=F32
            )
            back = scores[0:WINDOW] + empty if block == 0 else scores[0:WINDOW]
            scores = jnp.where(upper, back, scores[WINDOW:])
            highest = jnp.maximum(jnp.max(scores, axis=0, keepdims=True), sink)
            raised = jnp.exp(scores - highest)
            total = jnp.sum(raised, axis=0, keepdims=True) + jnp.exp(sink - highest)
            weights = jnp.concatenate(
                [jnp.where(upper, raised, 0.0), jnp.where(upper, 0.0, raised)], axis=0
            ).astype(BF16)
            out = lax.dot_general(values, weights, CONTRACT_ROWS, preferred_element_type=F32)
            out = out[g * HEAD_DIM : (g + 1) * HEAD_DIM] * (1.0 / total)
            outs += [out[:, j * WINDOW : (j + 1) * WINDOW] for j in range(group)]
        for p in range(heads // 2):
            both = jnp.concatenate([outs[2 * p], outs[2 * p + 1]], axis=0)
            out_ref[here, p * LANES : (p + 1) * LANES] = both.T.astype(BF16)


def window(mine, side, spot, q, kv, halo, sinks):
    rows, width = q.shape
    return call(
        functools.partial(window_body, mine),
        [
            pl.BlockSpec((rows // 2, width), lambda i, t, f: (half_of(t, mine), 0)),
            whole(kv.shape),
            whole(halo.shape),
            whole(sinks.shape),
        ],
        whole((rows // 2, width)),
        jax.ShapeDtypeStruct((rows // 2, width), BF16),
        [pltpu.VMEM((rows // 2 + WINDOW, kv.shape[1]), BF16)],
        2,
        2**30,
        8,
    )(side, spot, q, kv, halo, sinks)


def first_exit_body(a, b, wa, wb, out):
    rows = jnp.concatenate([a[...], b[...]], axis=1)
    for n in range(0, out.shape[1], CHUNK):
        here = slice(n, n + CHUNK)
        out[:, here] = dot(rows, jnp.concatenate([wa[:, here], wb[:, here]], axis=0))


def own_exit_body(a, w, more, out):
    for n in range(0, out.shape[1], CHUNK):
        here = slice(n, n + CHUNK)
        out[:, here] = more[:, here] + dot(a[...], w[:, here])


def last_exit_body(a, w, more, out, buffer, sems):
    copies = []
    for i, n in enumerate(range(0, out.shape[1], CHUNK)):
        here = slice(n, n + CHUNK)
        buffer[:, here] = (more[:, here] + dot(a[...], w[:, here])).astype(BF16)
        copy = pltpu.make_async_copy(buffer.at[:, here], out.at[:, here], sems.at[i])
        copy.start()
        copies.append(copy)
    for copy in copies:
        copy.wait()


def first_exit(a, b, wa, wb):
    args = (a, b, wa, wb)
    shape = (a.shape[0], wa.shape[1])
    return call(
        first_exit_body,
        [whole(x.shape) for x in args],
        whole(shape),
        jax.ShapeDtypeStruct(shape, F32),
        [],
        0,
        4 * a.shape[0] * a.shape[1] * wa.shape[1],
        12,
    )(*args)


def finish_exit_body(side, row, q_ref, in_ref, col_ref, gain, *refs):
    small, (w, more, out, rows) = refs[:6], refs[6:]
    finish_body(side, row, q_ref, in_ref, col_ref, gain, *small, rows)
    own_exit_body(rows, w, more, out)


def finish_exit(side, row, q, inside, col, gain, small, w, more):
    rows, width = q.shape
    spec = pl.BlockSpec((rows // 2, width), lambda i, t, z: (half_of(t, True), 0))
    rest = list(small) + [w, more]
    return call(
        finish_exit_body,
        [spec, spec, spec, whole(gain.shape)] + [whole(s.shape) for s in rest],
        whole(more.shape),
        jax.ShapeDtypeStruct(more.shape, F32),
        [pltpu.VMEM((rows // 2, width), BF16)],
        2,
        2**29,
        16,
    )(side, row, q, inside, col, gain, *rest)


def last_exit(a, w, more):
    args = (a, w, more)
    shape = (a.shape[0], w.shape[1])
    return call(
        last_exit_body,
        [whole(x.shape) for x in args],
        IN_HBM,
        jax.ShapeDtypeStruct(shape, BF16),
        [pltpu.VMEM(shape, BF16), pltpu.SemaphoreType.DMA((shape[1] // CHUNK,))],
        0,
        2 * a.shape[0] * a.shape[1] * w.shape[1],
        14,
    )(*args)


def turned(value, axis, by):
    peers = lax.axis_size(axis)
    return lax.ppermute(value, axis, [(i, (i + by) % peers) for i in range(peers)])


def shards(
    tokens,
    in_gain,
    ret_query,
    ret_key,
    ret_value,
    att_query,
    att_key,
    att_value,
    log_decay,
    ret_gain,
    sink_logit,
    retentive_exit_matrix,
    out_att,
):
    tp = lax.axis_index("tp").astype(jnp.int32)
    y = lax.axis_index("sp_1").astype(jnp.int32)
    z = lax.axis_index("sp_0").astype(jnp.int32)
    side, spot, row = tp.reshape(1), lax.axis_index(SP).astype(jnp.int32).reshape(1), z.reshape(1)
    side, spot, row, line_spot = lax.optimization_barrier((side, spot, row, y.reshape(1)))
    own = tokens[0]
    gain = in_gain[None]
    peer = turned(own, "tp", 1)
    early = (ret_key, ret_value, att_key, att_value)
    rates = log_decay.reshape(log_decay.shape[1], 1, log_decay.shape[2])
    first, scaled_own, squares, row_cum, col, wide_col, late = own_half(
        side, own, gain, rates, early
    )
    ret_k, ret_v, att_kv, inv, scaled, payload, tail = keys_half(
        side, peer, gain, first, squares, col, late, ret_key.shape[1]
    )
    hops = {}
    for k in (1, 2, 3):
        hops[k] = turned(payload, "sp_1", k)
    sources = [payload] + [hops[k] for k in (1, 2, 3)]
    peers = lax.axis_size(SP)
    halo = lax.ppermute(tail, SP, [(i, (i + 1) % peers) for i in range(peers)])
    ret_q, att_q = queries(side, scaled_own, scaled, inv, ret_query, att_query)
    sources, ret_q = lax.optimization_barrier((sources, ret_q))
    line, line_log, span = scan_step(line_body, line_spot, sources)
    sources = [span, turned(span, "sp_0", 1), turned(span, "sp_0", 7)]
    side, span = lax.optimization_barrier((side, span))
    theirs = window(False, side, spot, att_q, att_kv, halo, sink_logit)
    exit_own, out_own, sources[0] = lax.optimization_barrier(
        (retentive_exit_matrix, out_att, sources[0])
    )
    out_peer = turned(out_own, "tp", 1)
    exit_peer = turned(exit_own, "tp", 1)
    att_got = turned(theirs, "tp", 1)
    sources, theirs = lax.optimization_barrier((sources, theirs))
    column, column_log, span = scan_step(column_body, row, sources)
    three = turned(span, "sp_0", 3)
    six = turned(span, "sp_0", 6)
    sources = [three, six]
    side, row, span = lax.optimization_barrier((side, row, span))
    att_mine = window(True, side, spot, att_q, att_kv, halo, sink_logit)
    ret_q, row = lax.optimization_barrier((ret_q, row))
    inside = inner(ret_q, ret_k, ret_v, row_cum, col, wide_col)
    partial = first_exit(att_mine, att_got, out_att, out_peer)
    sources, partial, inside = lax.optimization_barrier((sources, partial, inside))
    small = [line, line_log, column, column_log] + sources
    args = (side, row, ret_q, inside, col, ret_gain, small)
    ret_got = turned(finish(False, *args), "tp", 1)
    partial = finish_exit(*args, retentive_exit_matrix, partial)
    mixed = last_exit(ret_got, exit_peer, partial)
    return mixed[None]


def solution(mesh):
    finer = Mesh(
        mesh.devices.reshape(8, 4, mesh.shape["fs"], mesh.shape["tp"]), ("sp_0", "sp_1", "fs", "tp")
    )
    placed = (
        P("fs", SP, "tp"),
        P(),
        P(None, "tp"),
        P(None, "tp"),
        P(None, "tp"),
        P(None, "tp"),
        P(None, "tp"),
        P(None, "tp"),
        P("fs", "tp", SP),
        P("tp"),
        P("tp"),
        P("tp", None),
        P("tp", None),
    )
    return jax.shard_map(
        shards, mesh=finer, in_specs=placed, out_specs=P("fs", SP_TP, None), check_vma=False
    )
```
